32 devices in a mesh: sp: 8 (over z, y), tp: 4 (over x, core).
Axes of the slice: x: 2, y: 2, z: 4, core: 2. Of those that a mesh axis runs over, the one named last changes fastest.
Arguments:
- latent: bfloat16 [3072, 2048], P(('sp', 'tp')), may hold values from -6 to 6
- context: bfloat16 [512, 2048], P('sp'), may hold values from -6 to 6
- cond_latent: float32 [2048], replicated, may hold values from -6 to 6
- cond_context: float32 [2048], replicated, may hold values from -12 to 12
- shift_weight: bfloat16 [2048, 2048], P('sp', 'tp'), may hold values from -0.125 to 0.125
- scale_weight: bfloat16 [2048, 2048], P('sp', 'tp'), may hold values from -0.125 to 0.125
- gate_weight: bfloat16 [2048, 2048], P('sp', 'tp'), may hold values from -0.125 to 0.125
- query_weight: bfloat16 [2, 2048, 1024], P(None, None, 'tp'), may hold values from -1.3258252 to 1.3258252
- key_weight: bfloat16 [2, 2048, 1024], P(None, None, 'tp'), may hold values from -1.3258252 to 1.3258252
- value_weight: bfloat16 [2048, 2048], P(None, 'tp'), may hold values from -0.125 to 0.125
- out_weight: bfloat16 [2048, 2048], P('tp'), may hold values from -0.125 to 0.125
- lambda_heads: float32 [16], P('tp'), may hold values from 0.3 to 0.8
- out_gain: float32 [2048], P('tp'), may hold values from 0.1 to 1.9
Outputs:
- result: bfloat16 [3072, 2048], P(('sp', 'tp'))
The draws below stay inside these ranges and needn't reach their ends.
All inputs are finite; a program needn't handle non-finite values.
Results may differ from the reference program's by a relative error of at most 0.02.
The reference program's roundings to bfloat16 on the way count: a program that leaves them out, or rounds other values in their place, can miss the bound.
Values may be sent and summed in bfloat16 or wider, within the bound.
A program may use at most 128 MiB of HBM per device.

```python
import math
import jax
import jax.numpy as jnp
from jax import lax

D = 2048
HEADS = 16
HEAD_DIM = 64
GRID_W = 64
CTX = 512
VALUE_DIM = 128
TOKENS = 3072
N_TP = 4


def projection(key, salt_value):
    entries = jax.random.truncated_normal(jax.random.fold_in(key, salt_value), -6.0, 6.0, (2, D, HEADS, HEAD_DIM), jnp.float32)
    scaled = entries * D ** (-0.5)
    return scaled.reshape(2, D, HEADS * HEAD_DIM).astype(jnp.bfloat16)


def draw_query_weight(key, part):
    return projection(key, 11)


def draw_key_weight(key, part):
    return projection(key, 23)


def level_of(own_key, extent, shards, low, top_value):
    gain = 1.0
    for dim, shards_of in shards:
        steps = jax.random.uniform(jax.random.fold_in(jax.random.fold_in(own_key, 6), dim), (shards_of,), jnp.float32, low / len(shards), top_value / len(shards))
        gain = gain * jnp.repeat(jnp.exp(steps), extent[dim] // shards_of).reshape((-1,) + (1,) * (len(extent) - 1 - dim))
    return gain


def gaussian(stream_key, extent, spread, reach, cuts=(), held_as=jnp.bfloat16):
    values = spread * jax.random.normal(stream_key, extent, jnp.float32)
    if cuts:
        values = values * level_of(stream_key, extent, cuts, -0.22, 0.18)
    return jnp.clip(values, -reach, reach).astype(held_as)


def setup_inputs(seed: int = 0) -> dict:
    streams_of = jax.random.split(jax.random.key(seed), 14)
    latent = gaussian(streams_of[0], (TOKENS, D), 1.0, 6.0, ((0, 32),))
    context = gaussian(streams_of[1], (CTX, D), 1.0, 6.0, ((0, 8),))
    cond_latent = gaussian(streams_of[2], (D,), 1.0, 6.0, (), jnp.float32)
    cond_context = gaussian(streams_of[3], (D,), 2.0, 12.0, (), jnp.float32)
    shift_weight = gaussian(streams_of[4], (D, D), D ** -0.5, 0.125, ((0, 8), (1, 4)))
    scale_weight = gaussian(streams_of[5], (D, D), D ** -0.5, 0.125, ((0, 8), (1, 4)))
    gate_weight = gaussian(streams_of[6], (D, D), D ** -0.5, 0.125, ((0, 8), (1, 4)))
    query_weight = draw_query_weight(jax.random.fold_in(streams_of[13], 71), 0)
    key_weight = draw_key_weight(jax.random.fold_in(streams_of[13], 71), 0)
    value_weight = gaussian(streams_of[9], (D, HEADS * VALUE_DIM), D ** -0.5, 0.125, ((1, 4),))
    out_weight = gaussian(streams_of[10], (HEADS * VALUE_DIM, D), (HEADS * VALUE_DIM) ** -0.5, 0.125, ((0, 4),))
    lambda_heads = jnp.clip(0.3 + 0.5 * jax.random.uniform(streams_of[11], (HEADS,), jnp.float32) ** level_of(streams_of[11], (HEADS,), ((0, 4),), -0.2, 0.2), 0.3, 0.8)
    out_gain = jnp.clip(1.0 + 0.18 * jax.random.normal(streams_of[12], (HEADS * VALUE_DIM,), jnp.float32), 0.1, 1.9)
    return dict(latent=latent, context=context, cond_latent=cond_latent, cond_context=cond_context, shift_weight=shift_weight, scale_weight=scale_weight, gate_weight=gate_weight, query_weight=query_weight, key_weight=key_weight, value_weight=value_weight, out_weight=out_weight, lambda_heads=lambda_heads, out_gain=out_gain)


norm_eps = 1e-06
rope_theta = 10000.0

def rms_scale(matrix):
    return matrix * lax.rsqrt(lax.optimization_barrier(jnp.mean(matrix * matrix, axis=-1, keepdims=True)) + norm_eps)

def modulated(activations, shift, scale):
    return (rms_scale(activations.astype(jnp.float32)) * (1.0 + scale) + shift).astype(jnp.bfloat16)

def rotate(vectors, positions, grid_width):
    quarter = vectors.shape[-1] // 4
    inverse = rope_theta ** (-jnp.arange(quarter, dtype=jnp.float32) / quarter)
    grid_row = (positions // grid_width).astype(jnp.float32)
    grid_col = (positions % grid_width).astype(jnp.float32)
    angles = jnp.concatenate([grid_row[:, None] * inverse, grid_col[:, None] * inverse], axis=-1)
    cos_table = jnp.cos(angles)[:, None, :]
    sin_table = jnp.sin(angles)[:, None, :]
    former = vectors[..., :2 * quarter]
    latter = vectors[..., 2 * quarter:]
    return jnp.concatenate([former * cos_table - latter * sin_table, latter * cos_table + former * sin_table], axis=-1)

def reference(latent, context, cond_latent, cond_context, shift_weight, scale_weight, gate_weight, query_weight, key_weight, value_weight, out_weight, lambda_heads, out_gain):
    conditions = jax.nn.silu(jnp.stack([cond_latent, cond_context])).astype(jnp.bfloat16)
    shifts = jnp.dot(conditions, shift_weight, preferred_element_type=jnp.float32)
    scales = jnp.dot(conditions, scale_weight, preferred_element_type=jnp.float32)
    gate_vector = jnp.dot(conditions[:1], gate_weight, preferred_element_type=jnp.float32)[0]
    hidden = modulated(latent, shifts[0], scales[0])
    context_hidden = modulated(context, shifts[1], scales[1])
    positions = jnp.arange(TOKENS, dtype=jnp.int32)

    def latent_heads(weight):
        product = jnp.dot(hidden, weight, preferred_element_type=jnp.float32).reshape(TOKENS, HEADS, HEAD_DIM)
        return rotate(product, positions, GRID_W).astype(jnp.bfloat16)

    def context_heads(weight):
        product = jnp.dot(context_hidden, weight, preferred_element_type=jnp.float32)
        return product.reshape(CTX, HEADS, HEAD_DIM).astype(jnp.bfloat16)
    queries = jnp.stack([latent_heads(query_weight[0]), latent_heads(query_weight[1])])
    key_rows = jnp.stack([jnp.concatenate([context_heads(key_weight[which_map]), latent_heads(key_weight[which_map])], axis=0) for which_map in (0, 1)])
    value_rows = jnp.concatenate([jnp.dot(context_hidden, value_weight, preferred_element_type=jnp.float32).astype(jnp.bfloat16), jnp.dot(hidden, value_weight, preferred_element_type=jnp.float32).astype(jnp.bfloat16)], axis=0)
    queries, key_rows, value_rows = lax.optimization_barrier((queries, key_rows, value_rows))
    queries = queries.transpose(2, 0, 1, 3)
    key_rows = key_rows.transpose(2, 0, 1, 3)
    value_rows = value_rows.reshape(CTX + TOKENS, HEADS, VALUE_DIM).transpose(1, 0, 2)
    query_block = math.gcd(TOKENS, 512)

    def one_head(operands):
        head_queries, head_keys, head_values, head_lambda = operands
        key_float = head_keys.astype(jnp.float32)
        value_float = head_values.astype(jnp.float32)
        blocks = head_queries.reshape(2, TOKENS // query_block, query_block, HEAD_DIM).transpose(1, 0, 2, 3)

        def one_block(block_queries):
            scores = jnp.einsum('mqd,mkd->mqk', block_queries.astype(jnp.float32), key_float) * HEAD_DIM ** (-0.5)
            weights = jnp.exp(scores - lax.optimization_barrier(jnp.max(scores, axis=-1, keepdims=True)))
            totals = lax.optimization_barrier(jnp.sum(weights, axis=-1, keepdims=True))
            rounded = lax.optimization_barrier(weights.astype(jnp.bfloat16)).astype(jnp.float32)
            numerator = jnp.einsum('mqk,ke->mqe', rounded, value_float)
            return numerator[0] / totals[0] - head_lambda * (numerator[1] / totals[1])
        return lax.map(one_block, blocks).reshape(TOKENS, VALUE_DIM)
    mixed = lax.map(one_head, (queries, key_rows, value_rows, lambda_heads))
    normed = rms_scale(mixed) * out_gain.reshape(HEADS, 1, VALUE_DIM)
    heads_out = normed.transpose(1, 0, 2).reshape(TOKENS, HEADS * VALUE_DIM).astype(jnp.bfloat16)
    group_width = HEADS // N_TP * VALUE_DIM
    summed = jnp.zeros((TOKENS, D), jnp.float32)
    for group_index in range(N_TP):
        lower = group_index * group_width
        group_term = jnp.dot(heads_out[:, lower:lower + group_width], out_weight[lower:lower + group_width], preferred_element_type=jnp.float32)
        summed = summed + lax.optimization_barrier(group_term.astype(jnp.bfloat16)).astype(jnp.float32)
    return (latent.astype(jnp.float32) + gate_vector * summed).astype(jnp.bfloat16)
```

```python
import functools

import jax
import jax.numpy as jnp
import numpy as np
from jax import lax
from jax.experimental import pallas as pl
from jax.experimental.pallas import tpu as pltpu
from jax.sharding import PartitionSpec as P

HEAD_DIM = 64
GRID_W = 64
VALUE_DIM = 128
LANES = 128

norm_eps = 1e-06
rope_theta = 10000.0
f32 = jnp.float32
bf16 = jnp.bfloat16
MESH = pl.DeviceIdType.MESH


def pick(total, limit, unit):
    best = unit
    for size in range(unit, limit + 1, unit):
        if total % size == 0:
            best = size
    return best


def body(
    n_sp,
    n_tp,
    lat,
    ctx,
    cond_l,
    cond_c,
    shift_w,
    scale_w,
    gate_w,
    lane_table,
    lam,
    gain,
    wq_hbm,
    wk_hbm,
    wv_hbm,
    wo_hbm,
    out,
    wq,
    wk,
    wv,
    wo,
    mod_part,
    mod_recv,
    mod_all,
    raw,
    hidden,
    cos_t,
    sin_t,
    q_send,
    kv_send,
    kvc_send,
    q_buf,
    kv_buf,
    scores,
    o_send,
    heads,
    pair_send,
    pair_recv,
    fin_send,
    fin_recv,
    own_sum,
    w_sem,
    loc_sem,
    mod1_s,
    mod1_r,
    mod2_s,
    mod2_r,
    raw_s,
    raw_r,
    fwd_s,
    fwd_r,
    q_s,
    q_r,
    kv_s,
    kv_r,
    kvc_s,
    kvc_r,
    rel_s,
    rel_r,
    relc_s,
    relc_r,
    o_s,
    o_r,
    pair_s,
    pair_r,
    fin_s,
    fin_r,
):
    own, width = lat.shape
    ctx_rows = ctx.shape[0]
    tok = own * n_tp
    mod_cols = shift_w.shape[1]
    groups = q_send.shape[0]
    ranks = n_sp // groups
    chips = n_tp // 2
    sp_i = lax.axis_index("sp")
    tp_i = lax.axis_index("tp")
    g_i = sp_i // ranks
    r_i = sp_i % ranks
    chip_i = tp_i // 2
    core_i = tp_i % 2
    partner = chip_i * 2 + (1 - core_i)
    pending = []

    def send(src, dst, s_sem, r_sem, **where):
        copy = pltpu.make_async_remote_copy(
            src_ref=src, dst_ref=dst, send_sem=s_sem, recv_sem=r_sem,
            device_id=where, device_id_type=MESH,
        )
        copy.start()
        pending.append(copy)

    def arrived(ref, s_sem, r_sem, **where):
        pltpu.make_async_remote_copy(
            src_ref=ref, dst_ref=ref, send_sem=s_sem, recv_sem=r_sem,
            device_id=where, device_id_type=MESH,
        ).wait_recv()

    loads = [
        pltpu.make_async_copy(src, dst, w_sem.at[i])
        for i, (src, dst) in enumerate(
            ((wk_hbm, wk), (wv_hbm, wv), (wq_hbm, wq), (wo_hbm, wo))
        )
    ]
    for load in loads:
        load.start()

    barrier = pltpu.get_barrier_semaphore()
    for k in range(1, n_sp):
        pl.semaphore_signal(
            barrier, inc=1, device_id={"sp": (sp_i + k) % n_sp}, device_id_type=MESH
        )
    for k in range(1, n_tp):
        pl.semaphore_signal(
            barrier, inc=1, device_id={"tp": (tp_i + k) % n_tp}, device_id_type=MESH
        )

    def silu(v):
        return (v / (1.0 + jnp.exp(-v))).astype(bf16).astype(f32)

    c0 = silu(cond_l[sp_i])
    c1 = silu(cond_c[sp_i])
    row = lax.broadcasted_iota(jnp.int32, (8, c0.shape[-1]), 0)

    def placed_rows(at0, at1):
        zero = jnp.zeros(row.shape, f32)
        rows = jnp.where(row == at0, jnp.broadcast_to(c0, row.shape), zero)
        if at1 is not None:
            rows = jnp.where(row == at1, jnp.broadcast_to(c1, row.shape), rows)
        return rows.astype(bf16)

    mod_part[...] = (
        jnp.dot(placed_rows(0, 1), shift_w[...], preferred_element_type=f32)
        + jnp.dot(placed_rows(2, 3), scale_w[...], preferred_element_type=f32)
        + jnp.dot(placed_rows(4, None), gate_w[...], preferred_element_type=f32)
    )
    pl.semaphore_wait(barrier, n_sp + n_tp - 2)

    for k in range(1, n_sp):
        send(
            mod_part, mod_recv.at[sp_i], mod1_s.at[k], mod1_r.at[sp_i], sp=(sp_i + k) % n_sp
        )
    pieces = raw_s.shape[1]
    piece_rows = own // pieces

    def raw_piece(slot, i):
        return raw.at[slot, pl.ds(i * piece_rows, piece_rows)]

    def send_raw(i):
        for k in range(1, chips):
            send(
                lat.at[pl.ds(i * piece_rows, piece_rows)], raw_piece(tp_i, i),
                raw_s.at[k, i], raw_r.at[chip_i, i],
                tp=((chip_i + k) % chips) * 2 + core_i,
            )

    def relay_raw(i):
        for k in range(1, chips):
            src_chip = (chip_i + chips - k) % chips
            slot = src_chip * 2 + core_i
            arrived(raw_piece(slot, i), raw_s.at[k, i], raw_r.at[src_chip, i], tp=slot)
            send(
                raw_piece(slot, i), raw_piece(slot, i), fwd_s.at[k, i], fwd_r.at[src_chip, i],
                tp=partner,
            )

    early = max(pieces - 1, 1)
    for i in range(early):
        send_raw(i)
    send(lat, raw.at[tp_i], fwd_s.at[0, 0], fwd_r.at[chip_i, 0], tp=partner)
    raw[tp_i] = lat[...]
    mod_recv[sp_i] = mod_part[...]

    tok_row = lax.broadcasted_iota(jnp.int32, (tok, LANES), 0) + sp_i * tok
    grid_row = (tok_row // GRID_W).astype(f32)
    grid_col = (tok_row % GRID_W).astype(f32)
    angles = grid_row * lane_table[0:1, :] + grid_col * lane_table[1:2, :]
    cos_t[...] = jnp.cos(angles)
    sin_t[...] = jnp.sin(angles) * lane_table[2:3, :]

    for k in range(1, n_sp):
        src = (sp_i + n_sp - k) % n_sp
        arrived(mod_recv.at[src], mod1_s.at[k], mod1_r.at[src], sp=src)
    total = mod_recv[0]
    for s in range(1, n_sp):
        total = total + mod_recv[s]
    mod_part2 = mod_all.at[tp_i]
    mod_part2[...] = total
    for k in range(1, n_tp):
        send(
            mod_part2, mod_all.at[tp_i], mod2_s.at[k], mod2_r.at[tp_i], tp=(tp_i + k) % n_tp
        )
    for i in range(early, pieces):
        send_raw(i)
    for i in range(early):
        relay_raw(i)
    for k in range(1, n_tp):
        src = (tp_i + n_tp - k) % n_tp
        arrived(mod_all.at[src], mod2_s.at[k], mod2_r.at[src], tp=src)

    def modulate(x, which, start):
        at = pl.ds(start if isinstance(start, int) else pl.multiple_of(start, 16), x.shape[0])
        factor = lax.rsqrt(jnp.mean(x * x, axis=-1, keepdims=True) + norm_eps)
        for t in range(n_tp):
            cols = slice(t * mod_cols, (t + 1) * mod_cols)
            shift = mod_all[t, which : which + 1, :]
            scale = mod_all[t, which + 2 : which + 3, :]
            hidden[at, cols] = (
                (x[:, cols] * factor) * (1.0 + scale) + shift
            ).astype(bf16)

    half = 2 * own
    lane = lax.broadcasted_iota(jnp.int32, (half, LANES), 1)
    first_quarter = lane % HEAD_DIM < HEAD_DIM // 2
    low_half = lane < HEAD_DIM
    ctx_half = lax.broadcasted_iota(jnp.int32, (ctx_rows, LANES), 1) < HEAD_DIM

    def rope(u, rows):
        swapped = jnp.where(
            first_quarter,
            pltpu.roll(u, LANES - HEAD_DIM // 2, 1),
            pltpu.roll(u, HEAD_DIM // 2, 1),
        )
        return u * cos_t[rows, :] + swapped * sin_t[rows, :]

    def pair_up(a, b, low):
        return (
            jnp.where(low, a, pltpu.roll(b, HEAD_DIM, 1)).astype(bf16),
            jnp.where(low, pltpu.roll(a, HEAD_DIM, 1), b).astype(bf16),
        )

    def lat_slot(s, chip=None):
        if chip is None:
            return kv_buf.at[pl.ds(pl.multiple_of(s * tok, 16), tok)]
        return kv_buf.at[pl.ds(pl.multiple_of(s * tok + chip * half, 16), half)]

    def ctx_slot(s):
        return kv_buf.at[pl.ds(pl.multiple_of(n_sp * tok + s * ctx_rows, 16), ctx_rows)]

    order = list(range(1, groups))
    for c in range(chips):
        chip = (chip_i + c) % chips
        rows = pl.ds(pl.multiple_of(chip * half, 16), half)
        if c == 0:
            modulate(ctx[...].astype(f32), 1, half)
            modulate(raw[tp_i].astype(f32), 0, core_i * own)
            arrived(raw.at[partner], fwd_s.at[0, 0], fwd_r.at[chip_i, 0], tp=partner)
            modulate(raw[partner].astype(f32), 0, (1 - core_i) * own)
            for i in range(early, pieces):
                relay_raw(i)
            count = half + ctx_rows
        else:
            slot = chip * 2 + core_i
            modulate(raw[slot].astype(f32), 0, core_i * own)
            slot = chip * 2 + (1 - core_i)
            for i in range(pieces):
                arrived(
                    raw_piece(slot, i), fwd_s.at[chips - c, i], fwd_r.at[chip, i], tp=partner
                )
            modulate(raw[slot].astype(f32), 0, (1 - core_i) * own)
            count = half
        if c == 0:
            loads[0].wait()
        keys = [jnp.dot(hidden[:count, :], wk[m], preferred_element_type=f32) for m in (0, 1)]
        for p in range(groups // 2):
            slab = slice(p * LANES, (p + 1) * LANES)
            a, b = pair_up(
                rope(keys[0][:half, slab], rows), rope(keys[1][:half, slab], rows), low_half
            )
            kv_send[2 * p, rows, :LANES] = a
            kv_send[2 * p + 1, rows, :LANES] = b
            if c == 0:
                a, b = pair_up(keys[0][half:, slab], keys[1][half:, slab], ctx_half)
                kvc_send[2 * p, :, :LANES] = a
                kvc_send[2 * p + 1, :, :LANES] = b
        if c == 0:
            loads[1].wait()
        vals = jnp.dot(hidden[:count, :], wv[...], preferred_element_type=f32).astype(bf16)
        for j in range(groups):
            slab = slice(j * LANES, (j + 1) * LANES)
            kv_send[j, rows, LANES:] = vals[:half, slab]
            if c == 0:
                kvc_send[j, :, LANES:] = vals[half:, slab]
        for k in order:
            g = (g_i + k) % groups
            to = g * ranks + r_i
            send(
                kv_send.at[g, rows], lat_slot(sp_i, chip), kv_s.at[k, c], kv_r.at[g_i, c], sp=to
            )
            if c == 0:
                send(kvc_send.at[g], ctx_slot(sp_i), kvc_s.at[k], kvc_r.at[g_i], sp=to)
        for e in range(1, ranks):
            to = g_i * ranks + (r_i + e) % ranks
            send(
                kv_send.at[g_i, rows], lat_slot(sp_i, chip), rel_s.at[0, c, e],
                rel_r.at[g_i, c, r_i], sp=to,
            )
            if c == 0:
                send(
                    kvc_send.at[g_i], ctx_slot(sp_i), relc_s.at[0, e], relc_r.at[g_i, r_i], sp=to
                )
        if c == 0:
            loads[2].wait()
        queries = [
            jnp.dot(hidden[:half, :], wq[m], preferred_element_type=f32) for m in (0, 1)
        ]
        for p in range(groups // 2):
            slab = slice(p * LANES, (p + 1) * LANES)
            a, b = pair_up(
                rope(queries[0][:, slab], rows), rope(queries[1][:, slab], rows), low_half
            )
            q_send[2 * p, rows, :] = a
            q_send[2 * p + 1, rows, :] = b
    for k in order:
        g = (g_i + k) % groups
        send(q_send.at[g], q_buf.at[g_i], q_s.at[k], q_r.at[g_i], sp=g * ranks + r_i)
    local = [
        pltpu.make_async_copy(kv_send.at[g_i], lat_slot(sp_i), loc_sem.at[0]),
        pltpu.make_async_copy(kvc_send.at[g_i], ctx_slot(sp_i), loc_sem.at[1]),
        pltpu.make_async_copy(q_send.at[g_i], q_buf.at[g_i], loc_sem.at[2]),
    ]
    for copy in local:
        copy.start()

    for c in range(chips):
        chip = (chip_i + c) % chips
        for k in order:
            g = (g_i + groups - k) % groups
            s = g * ranks + r_i
            arrived(lat_slot(s, chip), kv_s.at[k, c], kv_r.at[g, c], sp=s)
            for e in range(1, ranks):
                to = g_i * ranks + (r_i + e) % ranks
                send(
                    lat_slot(s, chip), lat_slot(s, chip), rel_s.at[k, c, e],
                    rel_r.at[g, c, r_i], sp=to,
                )
            if c == 0:
                arrived(ctx_slot(s), kvc_s.at[k], kvc_r.at[g], sp=s)
                for e in range(1, ranks):
                    to = g_i * ranks + (r_i + e) % ranks
                    send(
                        ctx_slot(s), ctx_slot(s), relc_s.at[k, e], relc_r.at[g, r_i], sp=to
                    )
    for copy in local:
        copy.wait()
    for e in range(1, ranks):
        r = (r_i + ranks - e) % ranks
        to = g_i * ranks + r
        for k in range(groups):
            g = (g_i + groups - k) % groups
            s = g * ranks + r
            for c in range(chips):
                chip = (chip_i + c) % chips
                arrived(lat_slot(s, chip), rel_s.at[k, c, e], rel_r.at[g, c, r], sp=to)
            arrived(ctx_slot(s), relc_s.at[k, e], relc_r.at[g, r], sp=to)

    key_total = kv_buf.shape[0]
    q_tile = scores.shape[0] // 2
    block = pick(key_total, 512, LANES)
    coef = HEAD_DIM ** (-0.5) * 1.4426950408889634
    q_low = lax.broadcasted_iota(jnp.int32, (q_tile, LANES), 1) < HEAD_DIM
    head_lam = lam[g_i]
    tiles = tok // q_tile
    head_gain = gain[g_i]

    def attend(g, start):
        q = q_buf[g, pl.ds(start, q_tile), :]
        zero = jnp.zeros_like(q)
        q2 = jnp.concatenate([jnp.where(q_low, q, zero), jnp.where(q_low, zero, q)], axis=0)
        peak = None
        for b in range(key_total // block):
            rows = slice(b * block, (b + 1) * block)
            s = lax.dot_general(
                q2, kv_buf[rows, :LANES], (((1,), (1,)), ((), ())), preferred_element_type=f32
            )
            scores[:, rows] = s
            for c in range(block // LANES):
                piece = s[:, c * LANES : (c + 1) * LANES]
                peak = piece if peak is None else jnp.maximum(peak, piece)
        top = jnp.max(peak, axis=-1, keepdims=True) * coef
        sums = None
        acc = None
        for b in range(key_total // block):
            rows = slice(b * block, (b + 1) * block)
            w = jnp.exp2(scores[:, rows] * coef - top)
            for c in range(block // LANES):
                piece = w[:, c * LANES : (c + 1) * LANES]
                sums = piece if sums is None else sums + piece
            part = jnp.dot(w.astype(bf16), kv_buf[rows, LANES:], preferred_element_type=f32)
            acc = part if acc is None else acc + part
        mean_v = acc / jnp.sum(sums, axis=-1, keepdims=True)
        mixed = mean_v[:q_tile] - head_lam * mean_v[q_tile:]
        factor = lax.rsqrt(jnp.mean(mixed * mixed, axis=-1, keepdims=True) + norm_eps)
        o_send[g, pl.ds(start, q_tile), :] = (mixed * factor * head_gain).astype(bf16)

    def o_copy(k, i):
        g = (g_i + groups - k) % groups
        rows = pl.ds(pl.multiple_of(i * q_tile, 16), q_tile)
        return pltpu.make_async_remote_copy(
            src_ref=o_send.at[g, rows], dst_ref=heads.at[g_i, rows], send_sem=o_s.at[k, i],
            recv_sem=o_r.at[g_i, i], device_id={"sp": g * ranks + r_i}, device_id_type=MESH,
        )

    @pl.loop(0, groups)
    def _(k):
        g = (g_i + groups - k) % groups

        @pl.when(k > 0)
        def _():
            arrived(q_buf.at[g], q_s.at[k], q_r.at[g], sp=g * ranks + r_i)

        @pl.loop(0, tiles)
        def _(i):
            attend(g, pl.multiple_of(i * q_tile, q_tile))

            @pl.when(k > 0)
            def _():
                o_copy(k, i).start()

    heads[g_i] = o_send[g_i]
    loads[3].wait()
    for k in order:
        src = (g_i + k) % groups
        for i in range(tiles):
            rows = pl.ds(i * q_tile, q_tile)
            arrived(heads.at[src, rows], o_s.at[k, i], o_r.at[src, i], sp=src * ranks + r_i)

    parts = pair_send.shape[1]
    part_cols = width // parts

    def head_rows(chunk):
        start = pl.multiple_of(chunk * own, 16)
        return jnp.concatenate(
            [heads[h, pl.ds(start, own), :] for h in range(groups)], axis=-1
        )

    def term(left, p):
        cols = slice(p * part_cols, (p + 1) * part_cols)
        return jnp.dot(left, wo[:, cols], preferred_element_type=f32).astype(bf16)

    def to_partner(k):
        chip = (chip_i + 1 + k) % chips
        left = head_rows(chip * 2 + (1 - core_i))
        for p in range(parts):
            pair_send[k, p] = term(left, p)
            send(
                pair_send.at[k, p], pair_recv.at[k, p], pair_s.at[k, p], pair_r.at[k, p],
                tp=partner,
            )

    def with_partner(k):
        chip = (chip_i + 1 + k) % chips
        left = head_rows(chip * 2 + core_i)
        for p in range(parts):
            mine = term(left, p).astype(f32)
            arrived(pair_recv.at[k, p], pair_s.at[k, p], pair_r.at[k, p], tp=partner)
            both = mine + pair_recv[k, p].astype(f32)
            if k < chips - 1:
                fin_send[k, p] = both.astype(bf16)
                send(
                    fin_send.at[k, p], fin_recv.at[k, p], fin_s.at[k, p], fin_r.at[k, p],
                    tp=chip * 2 + core_i,
                )
            else:
                own_sum[p] = both

    for k in range(chips - 1):
        to_partner(k)
    for k in range(chips - 1):
        with_partner(k)
    to_partner(chips - 1)
    with_partner(chips - 1)
    for p in range(parts):
        summed = own_sum[p]
        for k in range(chips - 1):
            src_chip = (chip_i + chips - 1 - k) % chips
            arrived(
                fin_recv.at[k, p], fin_s.at[k, p], fin_r.at[k, p], tp=src_chip * 2 + core_i
            )
            summed = summed + fin_recv[k, p].astype(f32)
        cols = slice(p * part_cols, (p + 1) * part_cols)
        per = mod_cols // part_cols
        if per >= 1:
            low = (p % per) * part_cols
            gate = mod_all[p // per, 4:5, low : low + part_cols]
        else:
            span = part_cols // mod_cols
            gate = jnp.concatenate(
                [mod_all[p * span + q, 4:5, :] for q in range(span)], axis=-1
            )
        out[:, cols] = (lat[:, cols].astype(f32) + gate * summed).astype(bf16)
    for copy in pending:
        copy.wait_send()
    for k in order:
        for i in range(tiles):
            o_copy(k, i).wait_send()


def split_body(
    n_sp,
    n_tp,
    lat,
    ctx,
    cond_l,
    cond_c,
    shift_w,
    scale_w,
    gate_w,
    lane_table,
    lam,
    gain,
    wq_hbm,
    wk_hbm,
    wv_hbm,
    wo_hbm,
    out,
    w,
    wo,
    mod_part,
    mod_recv,
    mod_half,
    mod_far,
    mod_all,
    par_own,
    par_recv,
    raw,
    far_ctx,
    hidden,
    cos_t,
    sin_t,
    kv_send,
    kvc_send,
    q_send,
    kv_buf,
    q_buf,
    vals_t,
    gain_t,
    peak_s,
    sum_s,
    acc_s,
    o_send,
    heads,
    mine,
    pair_send,
    pair_recv,
    fin_send,
    fin_recv,
    own_sum,
    w_sem,
    par_sem,
    mod1_s,
    mod1_r,
    modf_sem,
    mod2_s,
    mod2_r,
    z_s,
    z_r,
    x_s,
    x_r,
    d_s,
    d_r,
    kv_s,
    kv_r,
    kvc_s,
    kvc_r,
    q_s,
    q_r,
    rel_s,
    rel_r,
    relc_s,
    relc_r,
    o_s,
    o_r,
    pair_s,
    pair_r,
    fin_s,
    fin_r,
):
    own, width = lat.shape
    ctx_rows = ctx.shape[0]
    tok = own * n_tp
    mod_cols = shift_w.shape[1]
    pieces = z_s.shape[0] - 1
    rows_p = own // pieces
    ctx_p = ctx_rows // n_tp
    pair_rows = 2 * rows_p
    chunk_rows = 2 * pair_rows
    set_rows = tok + ctx_rows
    keys = 4 * set_rows
    q_tile = 4 * pair_rows
    sp_i = lax.axis_index("sp")
    tp_i = lax.axis_index("tp")
    z_i = sp_i // 2
    y_i = sp_i % 2
    half_i = z_i // 2
    zl_i = z_i % 2
    src_i = zl_i * 2 + y_i
    x_i = tp_i // 2
    c_i = tp_i % 2
    slot_i = c_i * 2 + x_i
    mirror = (sp_i + 4) % n_sp
    partner = x_i * 2 + (1 - c_i)
    across = (1 - x_i) * 2 + c_i
    owns_head = c_i == y_i
    pending = []
    when_remote = []

    def remote(src, dst, s_sem, r_sem, **where):
        return pltpu.make_async_remote_copy(
            src_ref=src, dst_ref=dst, send_sem=s_sem, recv_sem=r_sem,
            device_id=where, device_id_type=MESH,
        )

    def send(src, dst, s_sem, r_sem, **where):
        copy = remote(src, dst, s_sem, r_sem, **where)
        copy.start()
        pending.append(copy)

    def send_or_keep(src, dst, s_sem, r_sem, **where):
        copy = remote(src, dst, s_sem, r_sem, **where)

        @pl.when(owns_head)
        def _():
            pltpu.make_async_copy(src, dst, r_sem).start()

        @pl.when(jnp.logical_not(owns_head))
        def _():
            copy.start()

        when_remote.append(copy)

    def arrived(ref, r_sem):
        pltpu.make_async_copy(ref, ref, r_sem).wait()

    def sp_at(half, zl, y):
        return (half * 2 + zl) * 2 + y

    head_cols = 2 * HEAD_DIM
    val_cols = 2 * VALUE_DIM

    def part_cols_of(start, size):
        return pl.ds(pl.multiple_of(start, LANES), size)

    loads = []
    for m in (0, 1):
        loads.append(
            (wk_hbm.at[m, :, part_cols_of(half_i * head_cols, head_cols)],
             w.at[:, pl.ds(m * head_cols, head_cols)])
        )
    loads.append(
        (wv_hbm.at[:, part_cols_of(half_i * val_cols, val_cols)],
         w.at[:, pl.ds(2 * head_cols, val_cols)])
    )
    for m in (0, 1):
        loads.append(
            (wq_hbm.at[m, :, part_cols_of(half_i * head_cols, head_cols)],
             w.at[:, pl.ds(2 * head_cols + val_cols + m * head_cols, head_cols)])
        )
    loads.append((wo_hbm, wo))
    loads = [pltpu.make_async_copy(a, b, w_sem.at[i]) for i, (a, b) in enumerate(loads)]
    for load in loads:
        load.start()

    barrier = pltpu.get_barrier_semaphore()
    for k in range(1, n_sp):
        for tp in (tp_i, partner):
            pl.semaphore_signal(
                barrier, inc=1, device_id={"sp": (sp_i + k) % n_sp, "tp": tp},
                device_id_type=MESH,
            )
    for k in range(1, n_tp):
        pl.semaphore_signal(
            barrier, inc=1, device_id={"tp": (tp_i + k) % n_tp}, device_id_type=MESH
        )

    def silu(v):
        return (v / (1.0 + jnp.exp(-v))).astype(bf16).astype(f32)

    c0 = silu(cond_l[sp_i])
    c1 = silu(cond_c[sp_i])
    row = lax.broadcasted_iota(jnp.int32, (8, c0.shape[-1]), 0)

    def placed_rows(at0, at1):
        zero = jnp.zeros(row.shape, f32)
        rows = jnp.where(row == at0, jnp.broadcast_to(c0, row.shape), zero)
        if at1 is not None:
            rows = jnp.where(row == at1, jnp.broadcast_to(c1, row.shape), rows)
        return rows.astype(bf16)

    mod_part[...] = (
        jnp.dot(placed_rows(0, 1), shift_w[...], preferred_element_type=f32)
        + jnp.dot(placed_rows(2, 3), scale_w[...], preferred_element_type=f32)
        + jnp.dot(placed_rows(4, None), gate_w[...], preferred_element_type=f32)
    )
    par_own[0:1, :] = gain[z_i]
    par_own[1:2, :] = jnp.full((1, VALUE_DIM), lam[z_i], f32)
    pl.semaphore_wait(barrier, 2 * (n_sp - 1) + n_tp - 1)

    mates = [(dz, dy) for dz in (0, 1) for dy in (0, 1) if dz or dy]
    for e, (dz, dy) in enumerate(mates):
        send(
            mod_part, mod_recv.at[src_i], mod1_s.at[e], mod1_r.at[src_i],
            sp=sp_at(half_i, (zl_i + dz) % 2, (y_i + dy) % 2),
        )

    def piece(s, slot, p):
        if p == pieces:
            return far_ctx.at[pl.ds(slot * ctx_p, ctx_p)]
        return raw.at[s, slot, pl.ds(p * rows_p, rows_p)]

    def send_far(p):
        src = (
            ctx.at[pl.ds(pl.multiple_of(tp_i * ctx_p, ctx_p), ctx_p)]
            if p == pieces
            else lat.at[pl.ds(p * rows_p, rows_p)]
        )
        send(src, piece(1, slot_i, p), z_s.at[p], z_r.at[p], sp=mirror)

    def spread_x(s, p):
        src = piece(s, slot_i, p)
        if s == 0:
            src = lat.at[pl.ds(p * rows_p, rows_p)]
        send(src, piece(s, slot_i, p), x_s.at[s, p], x_r.at[s, p], tp=across)

    def spread_d(s, p):
        src = piece(s, slot_i, p)
        if s == 0:
            src = lat.at[pl.ds(p * rows_p, rows_p)]
        send(src, piece(s, slot_i, p), d_s.at[s, p, 0], d_r.at[s, p, 0], tp=partner)

    def from_far(p):
        arrived(piece(1, slot_i, p), z_r.at[p])
        spread_x(1, p)
        spread_d(1, p)

    def from_across(s, p):
        slot = c_i * 2 + (1 - x_i)
        arrived(piece(s, slot, p), x_r.at[s, p])
        send(piece(s, slot, p), piece(s, slot, p), d_s.at[s, p, 1], d_r.at[s, p, 1], tp=partner)

    def from_partner(s, p):
        arrived(piece(s, (1 - c_i) * 2 + x_i, p), d_r.at[s, p, 0])
        arrived(piece(s, (1 - c_i) * 2 + (1 - x_i), p), d_r.at[s, p, 1])

    send_far(pieces)
    for p in range(pieces):
        spread_d(0, p)
    for p in range(pieces - 1):
        spread_x(0, p)
    send(par_own, par_recv, par_sem.at[0], par_sem.at[1], tp=partner)
    raw[0, slot_i] = lat[...]
    mod_recv[src_i] = mod_part[...]

    def fill_rope(s):
        place = lax.broadcasted_iota(jnp.int32, (chunk_rows, LANES), 0)
        core = place // pair_rows
        chip = (place // rows_p) % 2
        home = sp_i if s == 0 else mirror
        for p in range(pieces):
            tok_row = home * tok + (chip * 2 + core) * own + p * rows_p + place % rows_p
            grid_row = (tok_row // GRID_W).astype(f32)
            grid_col = (tok_row % GRID_W).astype(f32)
            angles = grid_row * lane_table[0:1, :] + grid_col * lane_table[1:2, :]
            cos_t[s, p] = jnp.cos(angles)
            sin_t[s, p] = jnp.sin(angles) * lane_table[2:3, :]

    fill_rope(0)

    for dz, dy in mates:
        src = (zl_i + dz) % 2 * 2 + (y_i + dy) % 2
        arrived(mod_recv.at[src], mod1_r.at[src])
    total = mod_recv[0]
    for k in range(1, 4):
        total = total + mod_recv[k]
    mod_half[...] = total
    send(mod_half, mod_far, modf_sem.at[0], modf_sem.at[1], sp=mirror)
    for p in range(pieces):
        send_far(p)

    fill_rope(1)

    arrived(mod_far, modf_sem.at[1])
    mod_all[tp_i] = total + mod_far[...]
    for k in range(1, n_tp):
        send(
            mod_all.at[tp_i], mod_all.at[tp_i], mod2_s.at[k], mod2_r.at[tp_i],
            tp=(tp_i + k) % n_tp,
        )
    spread_x(0, pieces - 1)
    from_far(pieces)
    for p in range(pieces - 1):
        from_across(0, p)
    for k in range(1, n_tp):
        src = (tp_i + n_tp - k) % n_tp
        arrived(mod_all.at[src], mod2_r.at[src])

    def modulate(x, which, start):
        at = pl.ds(start, x.shape[0])
        factor = lax.rsqrt(jnp.mean(x * x, axis=-1, keepdims=True) + norm_eps)
        for t in range(n_tp):
            cols = slice(t * mod_cols, (t + 1) * mod_cols)
            shift = mod_all[t, which : which + 1, :]
            scale = mod_all[t, which + 2 : which + 3, :]
            hidden[at, cols] = (
                (x[:, cols] * factor) * (1.0 + scale) + shift
            ).astype(bf16)

    lane = lax.broadcasted_iota(jnp.int32, (chunk_rows, LANES), 1)
    first_quarter = lane % HEAD_DIM < HEAD_DIM // 2
    low_half = lane < HEAD_DIM
    ctx_half = lax.broadcasted_iota(jnp.int32, (ctx_rows, LANES), 1) < HEAD_DIM

    def rope(u, s, p):
        swapped = jnp.where(
            first_quarter,
            pltpu.roll(u, LANES - HEAD_DIM // 2, 1),
            pltpu.roll(u, HEAD_DIM // 2, 1),
        )
        return u * cos_t[s, p] + swapped * sin_t[s, p]

    def pair_up(a, b, low):
        return (
            jnp.where(low, a, pltpu.roll(b, HEAD_DIM, 1)).astype(bf16),
            jnp.where(low, pltpu.roll(a, HEAD_DIM, 1), b).astype(bf16),
        )

    def kv_at(s, src, core, p):
        start = (s * 4 + src) * set_rows + core * (tok // 2) + p * pair_rows
        return kv_buf.at[pl.ds(pl.multiple_of(start, 16), pair_rows)]

    def kvc_at(s, src, core):
        start = (s * 4 + src) * set_rows + tok + core * (ctx_rows // 2)
        return kv_buf.at[pl.ds(pl.multiple_of(start, 16), ctx_rows // 2)]

    def q_at(s, src, p):
        start = ((s * pieces + p) * 4 + src) * pair_rows
        return pl.ds(pl.multiple_of(start, 16), pair_rows)

    def chunk(s, p, with_ctx):
        from_partner(s, p)
        for slot in range(4):
            modulate(
                raw[s, slot, p * rows_p : (p + 1) * rows_p, :].astype(f32), 0, slot * rows_p
            )
        count = chunk_rows
        if with_ctx:
            if s == 1:
                from_partner(1, pieces)
                modulate(far_ctx[...].astype(f32), 1, chunk_rows)
            else:
                modulate(ctx[...].astype(f32), 1, chunk_rows)
            count = chunk_rows + ctx_rows
        if s == 0 and p == 0:
            for load in loads[:5]:
                load.wait()
        kv_cols = 2 * head_cols + val_cols
        kv = jnp.dot(hidden[:count, :], w[:, :kv_cols], preferred_element_type=f32)
        slabs = [kv[:, m * LANES : (m + 1) * LANES] for m in (0, 1)]
        pair = pair_up(
            rope(slabs[0][:chunk_rows], s, p), rope(slabs[1][:chunk_rows], s, p), low_half
        )
        if with_ctx:
            pair_c = pair_up(slabs[0][chunk_rows:], slabs[1][chunk_rows:], ctx_half)
        for j in (0, 1):
            vals = kv[:, (2 + j) * LANES : (3 + j) * LANES].astype(bf16)
            for core in (0, 1):
                rows = slice(core * pair_rows, (core + 1) * pair_rows)
                kv_send[s, j, core, p, :, :LANES] = pair[j][rows]
                kv_send[s, j, core, p, :, LANES:] = vals[rows]
            if with_ctx:
                kvc_send[s, j, :, :LANES] = pair_c[j]
                kvc_send[s, j, :, LANES:] = vals[chunk_rows:]
        for dj in (1, 0):
            j = (zl_i + dj) % 2
            for dc in (0, 1):
                core = (c_i + dc) % 2
                put = send if dj or dc else send_or_keep
                where = dict(sp=sp_at(half_i, j, c_i), tp=x_i * 2 + core)
                put(
                    kv_send.at[s, j, core, p], kv_at(s, src_i, core, p),
                    kv_s.at[s, p, dj, dc], kv_r.at[s, src_i, p], **where,
                )
                if with_ctx:
                    half = pl.ds(pl.multiple_of(core * (ctx_rows // 2), 16), ctx_rows // 2)
                    put(
                        kvc_send.at[s, j, half], kvc_at(s, src_i, core),
                        kvc_s.at[s, dj, dc], kvc_r.at[s, src_i], **where,
                    )
        q = jnp.dot(hidden[:chunk_rows, :], w[:, kv_cols:], preferred_element_type=f32)
        pair = pair_up(rope(q[:, :LANES], s, p), rope(q[:, LANES:], s, p), low_half)
        for j in (0, 1):
            for core in (0, 1):
                q_send[s, j, core, p] = pair[j][core * pair_rows : (core + 1) * pair_rows]
        for dj in (1, 0):
            j = (zl_i + dj) % 2
            for dc in (0, 1):
                core = (c_i + dc) % 2
                put = send if dj or dc else send_or_keep
                put(
                    q_send.at[s, j, core, p], q_buf.at[q_at(s, src_i, p)],
                    q_s.at[s, p, dj, dc], q_r.at[s, src_i, p],
                    sp=sp_at(half_i, j, c_i), tp=x_i * 2 + core,
                )

    def relay(s, p, with_ctx):
        for src in range(4):
            arrived(kv_at(s, src, c_i, p), kv_r.at[s, src, p])
            send(
                kv_at(s, src, c_i, p), kv_at(s, src, c_i, p),
                rel_s.at[s, src, p], rel_r.at[s, src, p], tp=partner,
            )
            if with_ctx:
                arrived(kvc_at(s, src, c_i), kvc_r.at[s, src])
                send(
                    kvc_at(s, src, c_i), kvc_at(s, src, c_i),
                    relc_s.at[s, src], relc_r.at[s, src], tp=partner,
                )

    def wait_keys(s):
        for src in range(4):
            for p in range(pieces):
                arrived(kv_at(s, src, 1 - c_i, p), rel_r.at[s, src, p])
            arrived(kvc_at(s, src, 1 - c_i), relc_r.at[s, src])
        step = 2 * LANES
        for b in range(keys // step):
            at = s * keys + b * step
            vals_t[s, :, b * step : (b + 1) * step] = kv_buf[at : at + step, LANES:].T

    def wait_queries(s, p):
        for src in range(4):
            arrived(q_buf.at[q_at(s, src, p)], q_r.at[s, src, p])

    coef = HEAD_DIM ** (-0.5) * 1.4426950408889634
    q_low = lax.broadcasted_iota(jnp.int32, (q_tile, LANES), 1) < HEAD_DIM
    cols = 2 * q_tile

    def item(tile, s, first, last):
        q = q_buf[tile * q_tile : (tile + 1) * q_tile, :]
        zero = jnp.zeros_like(q)
        q2 = jnp.concatenate([jnp.where(q_low, q, zero), jnp.where(q_low, zero, q)], axis=0)
        scores = lax.dot_general(
            kv_buf[s * keys : (s + 1) * keys, :LANES], q2, (((1,), (1,)), ((), ())),
            preferred_element_type=f32,
        )
        peak = jnp.max(scores, axis=0, keepdims=True)
        if not first:
            old = peak_s[tile]
            peak = jnp.maximum(old, peak)
        weights = jnp.exp2(scores * coef - peak * coef)
        sums = jnp.sum(weights.reshape(keys // 8, 8, cols), axis=0)
        acc = jnp.dot(vals_t[s], weights.astype(bf16), preferred_element_type=f32)
        if not first:
            fade = jnp.exp2((old - peak) * coef)
            sums = sums + sum_s[tile] * fade
            acc = acc + acc_s[tile] * fade
        if not last:
            peak_s[tile] = peak
            sum_s[tile] = sums
            acc_s[tile] = acc
            return
        mean_v = acc / jnp.sum(sums, axis=0, keepdims=True)
        mixed = mean_v[:, :q_tile] - gain_t[VALUE_DIM : VALUE_DIM + 1, :] * mean_v[:, q_tile:]
        factor = lax.rsqrt(jnp.mean(mixed * mixed, axis=0, keepdims=True) + norm_eps)
        o_send[tile * q_tile : (tile + 1) * q_tile, :] = (
            mixed * factor * gain_t[:VALUE_DIM, :]
        ).T.astype(bf16)

    def give_back(s, p):
        half = half_i if s == 0 else 1 - half_i
        for dz, dy in mates + [(0, 0)]:
            zl = (zl_i + dz) % 2
            y = (y_i + dy) % 2
            put = send if s or dz or dy else send_or_keep
            put(
                o_send.at[q_at(s, zl * 2 + y, p)], heads.at[z_i, c_i, p],
                o_s.at[s, p, dz * 2 + dy], o_r.at[z_i, c_i, p],
                sp=sp_at(half, zl, y), tp=x_i * 2 + y_i,
            )

    parts = pair_send.shape[1]
    part_cols = width // parts

    def project(p):
        for h in range(4):
            for core in (0, 1):
                arrived(heads.at[h, core, p], o_r.at[h, core, p])
        left = jnp.concatenate(
            [
                jnp.concatenate([heads[h, core, p] for h in range(4)], axis=-1)
                for core in (1 - c_i, c_i)
            ],
            axis=0,
        )
        for k in range(parts):
            at = slice(k * part_cols, (k + 1) * part_cols)
            terms = jnp.dot(left, wo[:, at], preferred_element_type=f32).astype(bf16)
            pair_send[p, k] = terms[:pair_rows]
            mine[p, k] = terms[pair_rows:]
            send(
                pair_send.at[p, k], pair_recv.at[p, k], pair_s.at[p, k], pair_r.at[p, k],
                tp=partner,
            )

    def combine(p):
        here = pl.ds(pl.multiple_of(x_i * rows_p, rows_p), rows_p)
        there = pl.ds(pl.multiple_of((1 - x_i) * rows_p, rows_p), rows_p)
        for k in range(parts):
            arrived(pair_recv.at[p, k], pair_r.at[p, k])
            both = mine[p, k, there, :].astype(f32) + pair_recv[p, k, there, :].astype(f32)
            fin_send[p, k] = both.astype(bf16)
            send(
                fin_send.at[p, k], fin_recv.at[p, k], fin_s.at[p, k], fin_r.at[p, k], tp=across
            )
            own_sum[p, k] = mine[p, k, here, :].astype(f32) + pair_recv[p, k, here, :].astype(f32)

    def finish(p):
        rows = slice(p * rows_p, (p + 1) * rows_p)
        for k in range(parts):
            arrived(fin_recv.at[p, k], fin_r.at[p, k])
            summed = own_sum[p, k] + fin_recv[p, k].astype(f32)
            done = 0
            while done < part_cols:
                col = k * part_cols + done
                size = min(mod_cols - col % mod_cols, part_cols - done)
                at = slice(col, col + size)
                low = col % mod_cols
                gate = mod_all[col // mod_cols, 4:5, low : low + size]
                out[rows, at] = (
                    lat[rows, at].astype(f32) + gate * summed[:, done : done + size]
                ).astype(bf16)
                done += size

    last = pieces - 1
    for p in range(last):
        chunk(0, p, p == 0)
        if p == 0:
            from_across(1, pieces)
    from_far(0)
    from_across(0, last)
    chunk(0, last, False)
    arrived(par_recv, par_sem.at[1])
    params = jnp.where(owns_head, par_own[...], par_recv[...])
    gain_row = jnp.broadcast_to(params[0:1, :], (VALUE_DIM, VALUE_DIM)).T
    lam_row = jnp.broadcast_to(params[1:2, :], (8, VALUE_DIM))
    for k in range(q_tile // VALUE_DIM):
        gain_t[:VALUE_DIM, k * VALUE_DIM : (k + 1) * VALUE_DIM] = gain_row
        gain_t[VALUE_DIM:, k * VALUE_DIM : (k + 1) * VALUE_DIM] = lam_row
    from_across(1, 0)
    chunk(1, 0, True)
    for p in range(last):
        relay(0, p, p == 0)
    for p in range(1, last):
        from_far(p)
        from_across(1, p)
        chunk(1, p, False)
    relay(0, last, False)
    wait_keys(0)
    for p in range(pieces):
        wait_queries(0, p)
    item(0, 0, True, False)
    from_far(last)
    item(1, 0, True, False)
    from_across(1, last)
    chunk(1, last, False)
    item(2, 0, True, False)
    for p in range(last):
        relay(1, p, p == 0)
    for p in range(last):
        wait_queries(1, p)
        item(pieces + p, 0, True, False)
    relay(1, last, False)
    wait_keys(1)
    wait_queries(1, last)
    for p in range(pieces):
        if p == last:
            item(pieces + p, 0, True, False)
        item(pieces + p, 1, False, True)
        give_back(1, p)
        if p > 0:
            project(p - 1)
        item(p, 1, False, True)
        give_back(0, p)
        if p == 0:
            loads[5].wait()
        else:
            combine(p - 1)
    project(last)
    for p in range(last):
        finish(p)
    combine(last)
    finish(last)
    for copy in pending:
        copy.wait_send()

    @pl.when(jnp.logical_not(owns_head))
    def _():
        for copy in when_remote:
            copy.wait_send()


def split_scratch(n_sp, n_tp, own, width, ctx_rows, mod_cols, groups):
    tok = own * n_tp
    pieces = 3
    rows_p = own // pieces
    pair_rows = 2 * rows_p
    q_tile = 4 * pair_rows
    keys = 4 * (tok + ctx_rows)
    parts = 2
    part_cols = width // parts
    dma = pltpu.SemaphoreType.DMA
    return [
        pltpu.VMEM((width, 4 * 2 * HEAD_DIM + 2 * VALUE_DIM), bf16),
        pltpu.VMEM((groups * VALUE_DIM, width), bf16),
        pltpu.VMEM((8, mod_cols), f32),
        pltpu.VMEM((4, 8, mod_cols), f32),
        pltpu.VMEM((8, mod_cols), f32),
        pltpu.VMEM((8, mod_cols), f32),
        pltpu.VMEM((n_tp, 8, mod_cols), f32),
        pltpu.VMEM((8, VALUE_DIM), f32),
        pltpu.VMEM((8, VALUE_DIM), f32),
        pltpu.VMEM((2, 4, own, width), bf16),
        pltpu.VMEM((ctx_rows, width), bf16),
        pltpu.VMEM((2 * pair_rows + ctx_rows, width), bf16),
        pltpu.VMEM((2, pieces, 2 * pair_rows, LANES), f32),
        pltpu.VMEM((2, pieces, 2 * pair_rows, LANES), f32),
        pltpu.VMEM((2, 2, 2, pieces, pair_rows, 2 * LANES), bf16),
        pltpu.VMEM((2, 2, ctx_rows, 2 * LANES), bf16),
        pltpu.VMEM((2, 2, 2, pieces, pair_rows, LANES), bf16),
        pltpu.VMEM((2 * keys, 2 * LANES), bf16),
        pltpu.VMEM((2 * pieces * q_tile, LANES), bf16),
        pltpu.VMEM((2, VALUE_DIM, keys), bf16),
        pltpu.VMEM((VALUE_DIM + 8, q_tile), f32),
        pltpu.VMEM((2 * pieces, 1, 2 * q_tile), f32),
        pltpu.VMEM((2 * pieces, 8, 2 * q_tile), f32),
        pltpu.VMEM((2 * pieces, VALUE_DIM, 2 * q_tile), f32),
        pltpu.VMEM((2 * pieces * q_tile, LANES), bf16),
        pltpu.VMEM((4, 2, pieces, pair_rows, LANES), bf16),
        pltpu.VMEM((pieces, parts, pair_rows, part_cols), bf16),
        pltpu.VMEM((pieces, parts, pair_rows, part_cols), bf16),
        pltpu.VMEM((pieces, parts, pair_rows, part_cols), bf16),
        pltpu.VMEM((pieces, parts, rows_p, part_cols), bf16),
        pltpu.VMEM((pieces, parts, rows_p, part_cols), bf16),
        pltpu.VMEM((pieces, parts, rows_p, part_cols), f32),
        dma((6,)),
        dma((2,)),
        dma((3,)),
        dma((4,)),
        dma((2,)),
        dma((n_tp,)),
        dma((n_tp,)),
        dma((pieces + 1,)),
        dma((pieces + 1,)),
        dma((2, pieces + 1)),
        dma((2, pieces + 1)),
        dma((2, pieces + 1, 2)),
        dma((2, pieces + 1, 2)),
        dma((2, pieces, 2, 2)),
        dma((2, 4, pieces)),
        dma((2, 2, 2)),
        dma((2, 4)),
        dma((2, pieces, 2, 2)),
        dma((2, 4, pieces)),
        dma((2, 4, pieces)),
        dma((2, 4, pieces)),
        dma((2, 4)),
        dma((2, 4)),
        dma((2, pieces, 4)),
        dma((4, 2, pieces)),
        dma((pieces, parts)),
        dma((pieces, parts)),
        dma((pieces, parts)),
        dma((pieces, parts)),
    ]


def local(
    n_sp,
    n_tp,
    latent,
    context,
    cond_latent,
    cond_context,
    shift_weight,
    scale_weight,
    gate_weight,
    query_weight,
    key_weight,
    value_weight,
    out_weight,
    lambda_heads,
    out_gain,
):
    own, width = latent.shape
    ctx_rows = context.shape[0]
    tok = own * n_tp
    groups = lambda_heads.shape[0]
    ranks = n_sp // groups
    chips = n_tp // 2
    mod_rows, mod_cols = shift_weight.shape
    keys = n_sp * (tok + ctx_rows)
    q_tile = pick(tok, 128, 16)
    pieces = 3 if own % 48 == 0 else 1
    parts = 4 if width % (4 * LANES) == 0 else 1

    quarter = HEAD_DIM // 4
    inverse = np.float32(rope_theta) ** (-np.arange(quarter, dtype=np.float32) / quarter)
    zeros = np.zeros((quarter,), np.float32)
    repeat = LANES // (2 * quarter)
    half = np.ones((2 * quarter,), np.float32)
    lane_table = np.zeros((8, LANES), np.float32)
    lane_table[0] = np.tile(np.concatenate([inverse, zeros]), repeat)
    lane_table[1] = np.tile(np.concatenate([zeros, inverse]), repeat)
    lane_table[2] = np.tile(np.concatenate([-half, half]), repeat // 2)
    gain = out_gain.reshape(groups, 1, VALUE_DIM)
    vmem = pl.BlockSpec(memory_space=pltpu.VMEM)
    hbm = pl.BlockSpec(memory_space=pl.ANY)
    dma = pltpu.SemaphoreType.DMA
    scratch = [
        pltpu.VMEM(query_weight.shape, bf16),
        pltpu.VMEM(key_weight.shape, bf16),
        pltpu.VMEM(value_weight.shape, bf16),
        pltpu.VMEM(out_weight.shape, bf16),
        pltpu.VMEM((8, mod_cols), f32),
        pltpu.VMEM((n_sp, 8, mod_cols), f32),
        pltpu.VMEM((n_tp, 8, mod_cols), f32),
        pltpu.VMEM((n_tp, own, width), bf16),
        pltpu.VMEM((2 * own + ctx_rows, width), bf16),
        pltpu.VMEM((tok, LANES), f32),
        pltpu.VMEM((tok, LANES), f32),
        pltpu.VMEM((groups, tok, LANES), bf16),
        pltpu.VMEM((groups, tok, 2 * LANES), bf16),
        pltpu.VMEM((groups, ctx_rows, 2 * LANES), bf16),
        pltpu.VMEM((groups, tok, LANES), bf16),
        pltpu.VMEM((keys, 2 * LANES), bf16),
        pltpu.VMEM((2 * q_tile, keys), f32),
        pltpu.VMEM((groups, tok, LANES), bf16),
        pltpu.VMEM((groups, tok, LANES), bf16),
        pltpu.VMEM((chips, parts, own, width // parts), bf16),
        pltpu.VMEM((chips, parts, own, width // parts), bf16),
        pltpu.VMEM((max(chips - 1, 1), parts, own, width // parts), bf16),
        pltpu.VMEM((max(chips - 1, 1), parts, own, width // parts), bf16),
        pltpu.VMEM((parts, own, width // parts), f32),
        dma((4,)),
        dma((3,)),
        dma((n_sp,)),
        dma((n_sp,)),
        dma((n_tp,)),
        dma((n_tp,)),
        dma((chips, pieces)),
        dma((chips, pieces)),
        dma((chips, pieces)),
        dma((chips, pieces)),
        dma((groups,)),
        dma((groups,)),
        dma((groups, chips)),
        dma((groups, chips)),
        dma((groups,)),
        dma((groups,)),
        dma((groups, chips, ranks)),
        dma((groups, chips, ranks)),
        dma((groups, ranks)),
        dma((groups, ranks)),
        dma((groups, tok // q_tile)),
        dma((groups, tok // q_tile)),
        dma((chips, parts)),
        dma((chips, parts)),
        dma((chips, parts)),
        dma((chips, parts)),
    ]
    kernel = body
    fits = own % 48 == 0 and ctx_rows % (16 * n_tp) == 0 and own * 8 // 3 % LANES == 0
    if (n_sp, n_tp, groups) == (8, 4, 4) and fits and (tok + ctx_rows) % 64 == 0:
        kernel = split_body
        scratch = split_scratch(n_sp, n_tp, own, width, ctx_rows, mod_cols, groups)
    return pl.pallas_call(
        functools.partial(kernel, n_sp, n_tp),
        out_shape=jax.ShapeDtypeStruct((own, width), bf16),
        in_specs=[vmem] * 8 + [pl.BlockSpec(memory_space=pltpu.SMEM), vmem] + [hbm] * 4,
        out_specs=vmem,
        scratch_shapes=scratch,
        compiler_params=pltpu.CompilerParams(
            collective_id=0, has_side_effects=True, vmem_limit_bytes=60 * 1024 * 1024
        ),
        name="diff_attention",
    )(
        latent,
        context,
        cond_latent.reshape(n_sp, 1, mod_rows),
        cond_context.reshape(n_sp, 1, mod_rows),
        shift_weight,
        scale_weight,
        gate_weight,
        jnp.asarray(lane_table),
        lambda_heads,
        gain,
        query_weight,
        key_weight,
        value_weight,
        out_weight,
    )


def solution(mesh):
    placed = (
        P(("sp", "tp"), None),
        P("sp", None),
        P(),
        P(),
        P("sp", "tp"),
        P("sp", "tp"),
        P("sp", "tp"),
        P(None, None, "tp"),
        P(None, None, "tp"),
        P(None, "tp"),
        P("tp", None),
        P("tp"),
        P("tp"),
    )
    return jax.shard_map(
        functools.partial(local, mesh.shape["sp"], mesh.shape["tp"]),
        mesh=mesh,
        in_specs=placed,
        out_specs=P(("sp", "tp"), None),
        check_vma=False,
    )
```

```python
import functools

import jax
import jax.numpy as jnp
import numpy as np
from jax import lax
from jax.experimental import pallas as pl
from jax.experimental.pallas import tpu as pltpu
from jax.sharding import PartitionSpec as P

HEAD_DIM = 64
GRID_W = 64
VALUE_DIM = 128
LANES = 128

norm_eps = 1e-06
rope_theta = 10000.0
f32 = jnp.float32
bf16 = jnp.bfloat16
MESH = pl.DeviceIdType.MESH


def pick(total, limit, unit):
    best = unit
    for size in range(unit, limit + 1, unit):
        if total % size == 0:
            best = size
    return best


def body(
    n_sp,
    n_tp,
    lat,
    ctx,
    cond_l,
    cond_c,
    shift_w,
    scale_w,
    gate_w,
    lane_table,
    lam,
    gain,
    wq_hbm,
    wk_hbm,
    wv_hbm,
    wo_hbm,
    out,
    wq,
    wk,
    wv,
    wo,
    mod_part,
    mod_recv,
    mod_all,
    raw,
    hidden,
    cos_t,
    sin_t,
    q_send,
    kv_send,
    kvc_send,
    q_buf,
    kv_buf,
    scores,
    o_send,
    heads,
    pair_send,
    pair_recv,
    fin_send,
    fin_recv,
    own_sum,
    w_sem,
    loc_sem,
    mod1_s,
    mod1_r,
    mod2_s,
    mod2_r,
    raw_s,
    raw_r,
    fwd_s,
    fwd_r,
    q_s,
    q_r,
    kv_s,
    kv_r,
    kvc_s,
    kvc_r,
    rel_s,
    rel_r,
    relc_s,
    relc_r,
    o_s,
    o_r,
    pair_s,
    pair_r,
    fin_s,
    fin_r,
):
    own, width = lat.shape
    ctx_rows = ctx.shape[0]
    tok = own * n_tp
    mod_cols = shift_w.shape[1]
    groups = q_send.shape[0]
    ranks = n_sp // groups
    chips = n_tp // 2
    sp_i = lax.axis_index("sp")
    tp_i = lax.axis_index("tp")
    g_i = sp_i // ranks
    r_i = sp_i % ranks
    chip_i = tp_i // 2
    core_i = tp_i % 2
    partner = chip_i * 2 + (1 - core_i)
    pending = []

    def send(src, dst, s_sem, r_sem, **where):
        copy = pltpu.make_async_remote_copy(
            src_ref=src, dst_ref=dst, send_sem=s_sem, recv_sem=r_sem,
            device_id=where, device_id_type=MESH,
        )
        copy.start()
        pending.append(copy)

    def arrived(ref, s_sem, r_sem, **where):
        pltpu.make_async_remote_copy(
            src_ref=ref, dst_ref=ref, send_sem=s_sem, recv_sem=r_sem,
            device_id=where, device_id_type=MESH,
        ).wait_recv()

    loads = [
        pltpu.make_async_copy(src, dst, w_sem.at[i])
        for i, (src, dst) in enumerate(
            ((wk_hbm, wk), (wv_hbm, wv), (wq_hbm, wq), (wo_hbm, wo))
        )
    ]
    for load in loads:
        load.start()

    barrier = pltpu.get_barrier_semaphore()
    for k in range(1, n_sp):
        pl.semaphore_signal(
            barrier, inc=1, device_id={"sp": (sp_i + k) % n_sp}, device_id_type=MESH
        )
    for k in range(1, n_tp):
        pl.semaphore_signal(
            barrier, inc=1, device_id={"tp": (tp_i + k) % n_tp}, device_id_type=MESH
        )

    def silu(v):
        return (v / (1.0 + jnp.exp(-v))).astype(bf16).astype(f32)

    c0 = silu(cond_l[sp_i])
    c1 = silu(cond_c[sp_i])
    row = lax.broadcasted_iota(jnp.int32, (8, c0.shape[-1]), 0)

    def placed_rows(at0, at1):
        zero = jnp.zeros(row.shape, f32)
        rows = jnp.where(row == at0, jnp.broadcast_to(c0, row.shape), zero)
        if at1 is not None:
            rows = jnp.where(row == at1, jnp.broadcast_to(c1, row.shape), rows)
        return rows.astype(bf16)

    mod_part[...] = (
        jnp.dot(placed_rows(0, 1), shift_w[...], preferred_element_type=f32)
        + jnp.dot(placed_rows(2, 3), scale_w[...], preferred_element_type=f32)
        + jnp.dot(placed_rows(4, None), gate_w[...], preferred_element_type=f32)
    )
    pl.semaphore_wait(barrier, n_sp + n_tp - 2)

    for k in range(1, n_sp):
        send(
            mod_part, mod_recv.at[sp_i], mod1_s.at[k], mod1_r.at[sp_i], sp=(sp_i + k) % n_sp
        )
    pieces = raw_s.shape[1]
    piece_rows = own // pieces

    def raw_piece(slot, i):
        return raw.at[slot, pl.ds(i * piece_rows, piece_rows)]

    def send_raw(i):
        for k in range(1, chips):
            send(
                lat.at[pl.ds(i * piece_rows, piece_rows)], raw_piece(tp_i, i),
                raw_s.at[k, i], raw_r.at[chip_i, i],
                tp=((chip_i + k) % chips) * 2 + core_i,
            )

    def relay_raw(i):
        for k in range(1, chips):
            src_chip = (chip_i + chips - k) % chips
            slot = src_chip * 2 + core_i
            arrived(raw_piece(slot, i), raw_s.at[k, i], raw_r.at[src_chip, i], tp=slot)
            send(
                raw_piece(slot, i), raw_piece(slot, i), fwd_s.at[k, i], fwd_r.at[src_chip, i],
                tp=partner,
            )

    early = max(pieces - 1, 1)
    for i in range(early):
        send_raw(i)
    send(lat, raw.at[tp_i], fwd_s.at[0, 0], fwd_r.at[chip_i, 0], tp=partner)
    raw[tp_i] = lat[...]
    mod_recv[sp_i] = mod_part[...]

    tok_row = lax.broadcasted_iota(jnp.int32, (tok, LANES), 0) + sp_i * tok
    grid_row = (tok_row // GRID_W).astype(f32)
    grid_col = (tok_row % GRID_W).astype(f32)
    angles = grid_row * lane_table[0:1, :] + grid_col * lane_table[1:2, :]
    cos_t[...] = jnp.cos(angles)
    sin_t[...] = jnp.sin(angles) * lane_table[2:3, :]

    for k in range(1, n_sp):
        src = (sp_i + n_sp - k) % n_sp
        arrived(mod_recv.at[src], mod1_s.at[k], mod1_r.at[src], sp=src)
    total = mod_recv[0]
    for s in range(1, n_sp):
        total = total + mod_recv[s]
    mod_part2 = mod_all.at[tp_i]
    mod_part2[...] = total
    for k in range(1, n_tp):
        send(
            mod_part2, mod_all.at[tp_i], mod2_s.at[k], mod2_r.at[tp_i], tp=(tp_i + k) % n_tp
        )
    for i in range(early, pieces):
        send_raw(i)
    for i in range(early):
        relay_raw(i)
    for k in range(1, n_tp):
        src = (tp_i + n_tp - k) % n_tp
        arrived(mod_all.at[src], mod2_s.at[k], mod2_r.at[src], tp=src)

    def modulate(x, which, start):
        at = pl.ds(start if isinstance(start, int) else pl.multiple_of(start, 16), x.shape[0])
        factor = lax.rsqrt(jnp.mean(x * x, axis=-1, keepdims=True) + norm_eps)
        for t in range(n_tp):
            cols = slice(t * mod_cols, (t + 1) * mod_cols)
            shift = mod_all[t, which : which + 1, :]
            scale = mod_all[t, which + 2 : which + 3, :]
            hidden[at, cols] = (
                (x[:, cols] * factor) * (1.0 + scale) + shift
            ).astype(bf16)

    half = 2 * own
    lane = lax.broadcasted_iota(jnp.int32, (half, LANES), 1)
    first_quarter = lane % HEAD_DIM < HEAD_DIM // 2
    low_half = lane < HEAD_DIM
    ctx_half = lax.broadcasted_iota(jnp.int32, (ctx_rows, LANES), 1) < HEAD_DIM

    def rope(u, rows):
        swapped = jnp.where(
            first_quarter,
            pltpu.roll(u, LANES - HEAD_DIM // 2, 1),
            pltpu.roll(u, HEAD_DIM // 2, 1),
        )
        return u * cos_t[rows, :] + swapped * sin_t[rows, :]

    def pair_up(a, b, low):
        return (
            jnp.where(low, a, pltpu.roll(b, HEAD_DIM, 1)).astype(bf16),
            jnp.where(low, pltpu.roll(a, HEAD_DIM, 1), b).astype(bf16),
        )

    def lat_slot(s, chip=None):
        if chip is None:
            return kv_buf.at[pl.ds(pl.multiple_of(s * tok, 16), tok)]
        return kv_buf.at[pl.ds(pl.multiple_of(s * tok + chip * half, 16), half)]

    def ctx_slot(s):
        return kv_buf.at[pl.ds(pl.multiple_of(n_sp * tok + s * ctx_rows, 16), ctx_rows)]

    order = list(range(1, groups))
    for c in range(chips):
        chip = (chip_i + c) % chips
        rows = pl.ds(pl.multiple_of(chip * half, 16), half)
        if c == 0:
            modulate(ctx[...].astype(f32), 1, half)
            modulate(raw[tp_i].astype(f32), 0, core_i * own)
            arrived(raw.at[partner], fwd_s.at[0, 0], fwd_r.at[chip_i, 0], tp=partner)
            modulate(raw[partner].astype(f32), 0, (1 - core_i) * own)
            for i in range(early, pieces):
                relay_raw(i)
            count = half + ctx_rows
        else:
            slot = chip * 2 + core_i
            modulate(raw[slot].astype(f32), 0, core_i * own)
            slot = chip * 2 + (1 - core_i)
            for i in range(pieces):
                arrived(
                    raw_piece(slot, i), fwd_s.at[chips - c, i], fwd_r.at[chip, i], tp=partner
                )
            modulate(raw[slot].astype(f32), 0, (1 - core_i) * own)
            count = half
        if c == 0:
            loads[0].wait()
        keys = [jnp.dot(hidden[:count, :], wk[m], preferred_element_type=f32) for m in (0, 1)]
        for p in range(groups // 2):
            slab = slice(p * LANES, (p + 1) * LANES)
            a, b = pair_up(
                rope(keys[0][:half, slab], rows), rope(keys[1][:half, slab], rows), low_half
            )
            kv_send[2 * p, rows, :LANES] = a
            kv_send[2 * p + 1, rows, :LANES] = b
            if c == 0:
                a, b = pair_up(keys[0][half:, slab], keys[1][half:, slab], ctx_half)
                kvc_send[2 * p, :, :LANES] = a
                kvc_send[2 * p + 1, :, :LANES] = b
        if c == 0:
            loads[1].wait()
        vals = jnp.dot(hidden[:count, :], wv[...], preferred_element_type=f32).astype(bf16)
        for j in range(groups):
            slab = slice(j * LANES, (j + 1) * LANES)
            kv_send[j, rows, LANES:] = vals[:half, slab]
            if c == 0:
                kvc_send[j, :, LANES:] = vals[half:, slab]
        for k in order:
            g = (g_i + k) % groups
            to = g * ranks + r_i
            send(
                kv_send.at[g, rows], lat_slot(sp_i, chip), kv_s.at[k, c], kv_r.at[g_i, c], sp=to
            )
            if c == 0:
                send(kvc_send.at[g], ctx_slot(sp_i), kvc_s.at[k], kvc_r.at[g_i], sp=to)
        for e in range(1, ranks):
            to = g_i * ranks + (r_i + e) % ranks
            send(
                kv_send.at[g_i, rows], lat_slot(sp_i, chip), rel_s.at[0, c, e],
                rel_r.at[g_i, c, r_i], sp=to,
            )
            if c == 0:
                send(
                    kvc_send.at[g_i], ctx_slot(sp_i), relc_s.at[0, e], relc_r.at[g_i, r_i], sp=to
                )
        if c == 0:
            loads[2].wait()
        queries = [
            jnp.dot(hidden[:half, :], wq[m], preferred_element_type=f32) for m in (0, 1)
        ]
        for p in range(groups // 2):
            slab = slice(p * LANES, (p + 1) * LANES)
            a, b = pair_up(
                rope(queries[0][:, slab], rows), rope(queries[1][:, slab], rows), low_half
            )
            q_send[2 * p, rows, :] = a
            q_send[2 * p + 1, rows, :] = b
    for k in order:
        g = (g_i + k) % groups
        send(q_send.at[g], q_buf.at[g_i], q_s.at[k], q_r.at[g_i], sp=g * ranks + r_i)
    local = [
        pltpu.make_async_copy(kv_send.at[g_i], lat_slot(sp_i), loc_sem.at[0]),
        pltpu.make_async_copy(kvc_send.at[g_i], ctx_slot(sp_i), loc_sem.at[1]),
        pltpu.make_async_copy(q_send.at[g_i], q_buf.at[g_i], loc_sem.at[2]),
    ]
    for copy in local:
        copy.start()

    for c in range(chips):
        chip = (chip_i + c) % chips
        for k in order:
            g = (g_i + groups - k) % groups
            s = g * ranks + r_i
            arrived(lat_slot(s, chip), kv_s.at[k, c], kv_r.at[g, c], sp=s)
            for e in range(1, ranks):
                to = g_i * ranks + (r_i + e) % ranks
                send(
                    lat_slot(s, chip), lat_slot(s, chip), rel_s.at[k, c, e],
                    rel_r.at[g, c, r_i], sp=to,
                )
            if c == 0:
                arrived(ctx_slot(s), kvc_s.at[k], kvc_r.at[g], sp=s)
                for e in range(1, ranks):
                    to = g_i * ranks + (r_i + e) % ranks
                    send(
                        ctx_slot(s), ctx_slot(s), relc_s.at[k, e], relc_r.at[g, r_i], sp=to
                    )
    for copy in local:
        copy.wait()
    for e in range(1, ranks):
        r = (r_i + ranks - e) % ranks
        to = g_i * ranks + r
        for k in range(groups):
            g = (g_i + groups - k) % groups
            s = g * ranks + r
            for c in range(chips):
                chip = (chip_i + c) % chips
                arrived(lat_slot(s, chip), rel_s.at[k, c, e], rel_r.at[g, c, r], sp=to)
            arrived(ctx_slot(s), relc_s.at[k, e], relc_r.at[g, r], sp=to)

    key_total = kv_buf.shape[0]
    q_tile = scores.shape[0] // 2
    block = pick(key_total, 512, LANES)
    coef = HEAD_DIM ** (-0.5) * 1.4426950408889634
    q_low = lax.broadcasted_iota(jnp.int32, (q_tile, LANES), 1) < HEAD_DIM
    head_lam = lam[g_i]
    tiles = tok // q_tile
    head_gain = gain[g_i]

    def attend(g, start):
        q = q_buf[g, pl.ds(start, q_tile), :]
        zero = jnp.zeros_like(q)
        q2 = jnp.concatenate([jnp.where(q_low, q, zero), jnp.where(q_low, zero, q)], axis=0)
        peak = None
        for b in range(key_total // block):
            rows = slice(b * block, (b + 1) * block)
            s = lax.dot_general(
                q2, kv_buf[rows, :LANES], (((1,), (1,)), ((), ())), preferred_element_type=f32
            )
            scores[:, rows] = s
            for c in range(block // LANES):
                piece = s[:, c * LANES : (c + 1) * LANES]
                peak = piece if peak is None else jnp.maximum(peak, piece)
        top = jnp.max(peak, axis=-1, keepdims=True) * coef
        sums = None
        acc = None
        for b in range(key_total // block):
            rows = slice(b * block, (b + 1) * block)
            w = jnp.exp2(scores[:, rows] * coef - top)
            for c in range(block // LANES):
                piece = w[:, c * LANES : (c + 1) * LANES]
                sums = piece if sums is None else sums + piece
            part = jnp.dot(w.astype(bf16), kv_buf[rows, LANES:], preferred_element_type=f32)
            acc = part if acc is None else acc + part
        mean_v = acc / jnp.sum(sums, axis=-1, keepdims=True)
        mixed = mean_v[:q_tile] - head_lam * mean_v[q_tile:]
        factor = lax.rsqrt(jnp.mean(mixed * mixed, axis=-1, keepdims=True) + norm_eps)
        o_send[g, pl.ds(start, q_tile), :] = (mixed * factor * head_gain).astype(bf16)

    def o_copy(k, i):
        g = (g_i + groups - k) % groups
        rows = pl.ds(pl.multiple_of(i * q_tile, 16), q_tile)
        return pltpu.make_async_remote_copy(
            src_ref=o_send.at[g, rows], dst_ref=heads.at[g_i, rows], send_sem=o_s.at[k, i],
            recv_sem=o_r.at[g_i, i], device_id={"sp": g * ranks + r_i}, device_id_type=MESH,
        )

    @pl.loop(0, groups)
    def _(k):
        g = (g_i + groups - k) % groups

        @pl.when(k > 0)
        def _():
            arrived(q_buf.at[g], q_s.at[k], q_r.at[g], sp=g * ranks + r_i)

        @pl.loop(0, tiles)
        def _(i):
            attend(g, pl.multiple_of(i * q_tile, q_tile))

            @pl.when(k > 0)
            def _():
                o_copy(k, i).start()

    heads[g_i] = o_send[g_i]
    loads[3].wait()
    for k in order:
        src = (g_i + k) % groups
        for i in range(tiles):
            rows = pl.ds(i * q_tile, q_tile)
            arrived(heads.at[src, rows], o_s.at[k, i], o_r.at[src, i], sp=src * ranks + r_i)

    parts = pair_send.shape[1]
    part_cols = width // parts

    def head_rows(chunk):
        start = pl.multiple_of(chunk * own, 16)
        return jnp.concatenate(
            [heads[h, pl.ds(start, own), :] for h in range(groups)], axis=-1
        )

    def term(left, p):
        cols = slice(p * part_cols, (p + 1) * part_cols)
        return jnp.dot(left, wo[:, cols], preferred_element_type=f32).astype(bf16)

    def to_partner(k):
        chip = (chip_i + 1 + k) % chips
        left = head_rows(chip * 2 + (1 - core_i))
        for p in range(parts):
            pair_send[k, p] = term(left, p)
            send(
                pair_send.at[k, p], pair_recv.at[k, p], pair_s.at[k, p], pair_r.at[k, p],
                tp=partner,
            )

    def with_partner(k):
        chip = (chip_i + 1 + k) % chips
        left = head_rows(chip * 2 + core_i)
        for p in range(parts):
            mine = term(left, p).astype(f32)
            arrived(pair_recv.at[k, p], pair_s.at[k, p], pair_r.at[k, p], tp=partner)
            both = mine + pair_recv[k, p].astype(f32)
            if k < chips - 1:
                fin_send[k, p] = both.astype(bf16)
                send(
                    fin_send.at[k, p], fin_recv.at[k, p], fin_s.at[k, p], fin_r.at[k, p],
                    tp=chip * 2 + core_i,
                )
            else:
                own_sum[p] = both

    for k in range(chips - 1):
        to_partner(k)
    for k in range(chips - 1):
        with_partner(k)
    to_partner(chips - 1)
    with_partner(chips - 1)
    for p in range(parts):
        summed = own_sum[p]
        for k in range(chips - 1):
            src_chip = (chip_i + chips - 1 - k) % chips
            arrived(
                fin_recv.at[k, p], fin_s.at[k, p], fin_r.at[k, p], tp=src_chip * 2 + core_i
            )
            summed = summed + fin_recv[k, p].astype(f32)
        cols = slice(p * part_cols, (p + 1) * part_cols)
        per = mod_cols // part_cols
        if per >= 1:
            low = (p % per) * part_cols
            gate = mod_all[p // per, 4:5, low : low + part_cols]
        else:
            span = part_cols // mod_cols
            gate = jnp.concatenate(
                [mod_all[p * span + q, 4:5, :] for q in range(span)], axis=-1
            )
        out[:, cols] = (lat[:, cols].astype(f32) + gate * summed).astype(bf16)
    for copy in pending:
        copy.wait_send()
    for k in order:
        for i in range(tiles):
            o_copy(k, i).wait_send()


def split_body(
    n_sp,
    n_tp,
    lat,
    ctx,
    cond_l,
    cond_c,
    shift_w,
    scale_w,
    gate_w,
    lane_table,
    lam,
    gain,
    wq_hbm,
    wk_hbm,
    wv_hbm,
    wo_hbm,
    out,
    w,
    wo,
    mod_part,
    mod_recv,
    mod_all,
    gate_part,
    gate_recv,
    gate_all,
    par_own,
    par_recv,
    raw,
    far_ctx,
    hidden,
    cos_t,
    sin_t,
    kv_send,
    kvc_send,
    q_send,
    kv_buf,
    q_buf,
    vals_t,
    gain_t,
    peak_s,
    sum_s,
    acc_s,
    o_send,
    heads,
    mine,
    pair_send,
    pair_recv,
    fin_send,
    fin_recv,
    own_sum,
    w_sem,
    par_sem,
    mod_sem,
    gate_sem,
    raw_s,
    z_r,
    x_r,
    d_r,
    kv_s,
    kv_r,
    rel_r,
    q_s,
    q_r,
    o_s,
    o_r,
    pair_s,
    pair_r,
    fin_s,
    fin_r,
):
    own, width = lat.shape
    ctx_rows = ctx.shape[0]
    tok = own * n_tp
    mod_cols = shift_w.shape[1]
    pieces = z_r.shape[0] - 1
    rows_p = own // pieces
    ctx_p = ctx_rows // n_tp
    pair_rows = 2 * rows_p
    chunk_rows = 2 * pair_rows
    set_rows = tok + ctx_rows
    keys = 4 * set_rows
    q_tile = 4 * pair_rows
    sp_i = lax.axis_index("sp")
    tp_i = lax.axis_index("tp")
    z_i = sp_i // 2
    y_i = sp_i % 2
    half_i = z_i // 2
    zl_i = z_i % 2
    src_i = zl_i * 2 + y_i
    x_i = tp_i // 2
    c_i = tp_i % 2
    slot_i = c_i * 2 + x_i
    mirror = (sp_i + 4) % n_sp
    partner = x_i * 2 + (1 - c_i)
    across = (1 - x_i) * 2 + c_i
    owns_head = c_i == y_i

    def remote(src, dst, s_sem, r_sem, **where):
        return pltpu.make_async_remote_copy(
            src_ref=src, dst_ref=dst, send_sem=s_sem, recv_sem=r_sem,
            device_id=where, device_id_type=MESH,
        )

    def send(src, dst, s_sem, r_sem, **where):
        remote(src, dst, s_sem, r_sem, **where).start()

    def send_or_keep(src, dst, s_sem, r_sem, **where):
        copy = remote(src, dst, s_sem, r_sem, **where)

        @pl.when(owns_head)
        def _():
            pltpu.make_async_copy(src, dst, r_sem).start()

        @pl.when(jnp.logical_not(owns_head))
        def _():
            copy.start()

    def arrived(ref, r_sem):
        pltpu.make_async_copy(ref, ref, r_sem).wait()

    def sp_at(half, zl, y):
        return (half * 2 + zl) * 2 + y

    head_cols = 2 * HEAD_DIM
    val_cols = 2 * VALUE_DIM

    def part_cols_of(start, size):
        return pl.ds(pl.multiple_of(start, LANES), size)

    loads = []
    for m in (0, 1):
        loads.append(
            (wk_hbm.at[m, :, part_cols_of(half_i * head_cols, head_cols)],
             w.at[:, pl.ds(m * head_cols, head_cols)])
        )
    loads.append(
        (wv_hbm.at[:, part_cols_of(half_i * val_cols, val_cols)],
         w.at[:, pl.ds(2 * head_cols, val_cols)])
    )
    for m in (0, 1):
        loads.append(
            (wq_hbm.at[m, :, part_cols_of(half_i * head_cols, head_cols)],
             w.at[:, pl.ds(2 * head_cols + val_cols + m * head_cols, head_cols)])
        )
    loads = [pltpu.make_async_copy(a, b, w_sem.at[0]) for a, b in loads]
    loads.append(pltpu.make_async_copy(wo_hbm, wo, w_sem.at[1]))
    for load in loads:
        load.start()

    barrier = pltpu.get_barrier_semaphore()
    for k in range(1, n_sp):
        for tp in (tp_i, partner):
            pl.semaphore_signal(
                barrier, inc=1, device_id={"sp": (sp_i + k) % n_sp, "tp": tp},
                device_id_type=MESH,
            )
    for k in range(1, n_tp):
        pl.semaphore_signal(
            barrier, inc=1, device_id={"tp": (tp_i + k) % n_tp}, device_id_type=MESH
        )

    def silu(v):
        return (v / (1.0 + jnp.exp(-v))).astype(bf16).astype(f32)

    c0 = silu(cond_l[sp_i])
    c1 = silu(cond_c[sp_i])
    row = lax.broadcasted_iota(jnp.int32, (8, c0.shape[-1]), 0)

    def placed_rows(at0, at1):
        zero = jnp.zeros(row.shape, f32)
        rows = jnp.where(row == at0, jnp.broadcast_to(c0, row.shape), zero)
        if at1 is not None:
            rows = jnp.where(row == at1, jnp.broadcast_to(c1, row.shape), rows)
        return rows.astype(bf16)

    half_cols = mod_cols // 2
    mod_total = None
    for k in (0, 1):
        at = slice(k * half_cols, (k + 1) * half_cols)
        for first, weight in ((4 * k, shift_w), (4 * k + 2, scale_w)):
            term = jnp.dot(
                placed_rows(first, first + 1), weight[:, at], preferred_element_type=f32
            )
            mod_total = term if mod_total is None else mod_total + term
    mod_part[...] = mod_total
    par_own[0:1, :] = gain[z_i]
    par_own[1:2, :] = jnp.full((1, VALUE_DIM), lam[z_i], f32)
    pl.semaphore_wait(barrier, 2 * (n_sp - 1) + n_tp - 1)

    def to_all_sp(src, dst, sems):
        for k in range(1, n_sp):
            send(src, dst.at[sp_i], sems.at[0], sems.at[1], sp=(sp_i + k) % n_sp)

    def to_all_tp(ref, sems):
        for k in range(1, n_tp):
            send(ref.at[tp_i], ref.at[tp_i], sems.at[2], sems.at[3], tp=(tp_i + k) % n_tp)

    def sum_sp(ref, sems):
        arrived(ref.at[pl.ds(0, n_sp - 1)], sems.at[1])
        total = ref[0]
        for k in range(1, n_sp):
            total = total + ref[k]
        return total

    mates = [(0, 1), (1, 0), (1, 1)]
    to_all_sp(mod_part, mod_recv, mod_sem)

    def piece(s, slot, p):
        if p == pieces:
            return far_ctx.at[pl.ds(pl.multiple_of(slot * ctx_p, 16), ctx_p)]
        start = ((s * pieces + p) * 4 + slot) * rows_p
        return raw.at[pl.ds(pl.multiple_of(start, 16), rows_p)]

    def piece_pair(s, core, p):
        if p == pieces:
            return far_ctx.at[pl.ds(pl.multiple_of(core * 2 * ctx_p, 16), 2 * ctx_p)]
        start = ((s * pieces + p) * 4 + core * 2) * rows_p
        return raw.at[pl.ds(pl.multiple_of(start, 16), pair_rows)]

    def send_far(p):
        src = (
            ctx.at[pl.ds(pl.multiple_of(tp_i * ctx_p, ctx_p), ctx_p)]
            if p == pieces
            else lat.at[pl.ds(p * rows_p, rows_p)]
        )
        send(src, piece(1, slot_i, p), raw_s.at[0], z_r.at[p], sp=mirror)

    def spread_x(s, p):
        src = piece(s, slot_i, p)
        if s == 0:
            src = lat.at[pl.ds(p * rows_p, rows_p)]
        send(src, piece(s, slot_i, p), raw_s.at[0], x_r.at[s, p], tp=across)

    def spread_d(s, p):
        src = piece(s, slot_i, p)
        if s == 0:
            src = lat.at[pl.ds(p * rows_p, rows_p)]
        send(src, piece(s, slot_i, p), raw_s.at[0], d_r.at[s, p], tp=partner)

    def from_far(p):
        arrived(piece(1, slot_i, p), z_r.at[p])
        spread_x(1, p)
        spread_d(1, p)

    def from_across(s, p):
        slot = c_i * 2 + (1 - x_i)
        arrived(piece(s, slot, p), x_r.at[s, p])
        send(piece(s, slot, p), piece(s, slot, p), raw_s.at[0], d_r.at[s, p], tp=partner)

    def from_partner(s, p):
        arrived(piece_pair(s, 1 - c_i, p), d_r.at[s, p])

    spread_x(0, 0)
    for p in range(pieces):
        spread_d(0, p)
    send(par_own, par_recv, par_sem.at[0], par_sem.at[1], tp=partner)
    for p in range(pieces):
        piece(0, slot_i, p)[...] = lat[p * rows_p : (p + 1) * rows_p, :]
    mod_recv[sp_i] = mod_part[...]

    def fill_rope(s):
        place = lax.broadcasted_iota(jnp.int32, (chunk_rows, LANES), 0)
        core = place // pair_rows
        chip = (place // rows_p) % 2
        home = sp_i if s == 0 else mirror
        for p in range(pieces):
            tok_row = home * tok + (chip * 2 + core) * own + p * rows_p + place % rows_p
            grid_row = (tok_row // GRID_W).astype(f32)
            grid_col = (tok_row % GRID_W).astype(f32)
            angles = grid_row * lane_table[0:1, :] + grid_col * lane_table[1:2, :]
            cos_t[s, p] = jnp.cos(angles)
            sin_t[s, p] = jnp.sin(angles) * lane_table[2:3, :]

    fill_rope(0)
    fill_rope(1)
    gate_total = None
    gate_cols = mod_cols // 4
    for k in range(4):
        term = jnp.dot(
            placed_rows(k, None), gate_w[:, k * gate_cols : (k + 1) * gate_cols],
            preferred_element_type=f32,
        )
        gate_total = term if gate_total is None else gate_total + term
    gate_part[...] = gate_total
    gate_recv[sp_i] = gate_total

    mod_all[tp_i] = sum_sp(mod_recv, mod_sem)
    to_all_tp(mod_all, mod_sem)
    outer = zl_i != half_i

    @pl.when(outer)
    def _():
        send_far(pieces)
        for p in range(pieces):
            send_far(p)

    for p in range(1, pieces):
        spread_x(0, p)
    to_all_sp(gate_part, gate_recv, gate_sem)
    from_across(0, 0)
    arrived(mod_all.at[pl.ds(0, n_tp - 1)], mod_sem.at[3])

    def modulate(x, which, start):
        at = pl.ds(start, x.shape[0])
        factor = lax.rsqrt(jnp.mean(x * x, axis=-1, keepdims=True) + norm_eps)
        for t in range(n_tp):
            for k in (0, 1):
                start = t * mod_cols + k * half_cols
                cols = slice(start, start + half_cols)
                shift = mod_all[t, 4 * k + which : 4 * k + which + 1, :]
                scale = mod_all[t, 4 * k + which + 2 : 4 * k + which + 3, :]
                hidden[at, cols] = (
                    (x[:, cols] * factor) * (1.0 + scale) + shift
                ).astype(bf16)

    lane = lax.broadcasted_iota(jnp.int32, (chunk_rows, LANES), 1)
    first_quarter = lane % HEAD_DIM < HEAD_DIM // 2
    low_half = lane < HEAD_DIM
    ctx_half = lax.broadcasted_iota(jnp.int32, (ctx_rows, LANES), 1) < HEAD_DIM

    def rope(u, s, p):
        swapped = jnp.where(
            first_quarter,
            pltpu.roll(u, LANES - HEAD_DIM // 2, 1),
            pltpu.roll(u, HEAD_DIM // 2, 1),
        )
        return u * cos_t[s, p] + swapped * sin_t[s, p]

    def pair_up(a, b, low):
        return (
            jnp.where(low, a, pltpu.roll(b, HEAD_DIM, 1)).astype(bf16),
            jnp.where(low, pltpu.roll(a, HEAD_DIM, 1), b).astype(bf16),
        )

    core_keys = keys // 2

    def kv_at(s, src, core, p):
        start = s * keys + core * core_keys + (p * 4 + src) * pair_rows
        return kv_buf.at[pl.ds(pl.multiple_of(start, 16), pair_rows)]

    def kvc_at(s, src, core):
        start = s * keys + core * core_keys + 2 * tok + src * (ctx_rows // 2)
        return kv_buf.at[pl.ds(pl.multiple_of(start, 16), ctx_rows // 2)]

    def kv_block(s, core, p):
        start = s * keys + core * core_keys + p * 4 * pair_rows
        size = 2 * ctx_rows if p == pieces else 4 * pair_rows
        return kv_buf.at[pl.ds(pl.multiple_of(start, 16), size)]

    def q_at(s, src, p):
        start = ((s * pieces + p) * 4 + src) * pair_rows
        return pl.ds(pl.multiple_of(start, 16), pair_rows)

    kv_cols = 2 * head_cols + val_cols

    def chunk(s, ps, with_ctx):
        for i, p in enumerate(ps):
            from_partner(s, p)
            start = (s * pieces + p) * chunk_rows
            modulate(raw[start : start + chunk_rows, :].astype(f32), 0, i * chunk_rows)
        lat_count = len(ps) * chunk_rows
        count = lat_count
        if with_ctx:
            if s == 1:
                from_partner(1, pieces)
                modulate(far_ctx[...].astype(f32), 1, lat_count)
            else:
                modulate(ctx[...].astype(f32), 1, lat_count)
            count = lat_count + ctx_rows
        if s == 0 and ps[0] == 0:
            arrived(w, w_sem.at[0])
        kv = jnp.dot(hidden[:count, :], w[:, :kv_cols], preferred_element_type=f32)
        slabs = [kv[:, m * LANES : (m + 1) * LANES] for m in (0, 1)]
        vals = [kv[:, (2 + j) * LANES : (3 + j) * LANES].astype(bf16) for j in (0, 1)]
        for i, p in enumerate(ps):
            at = slice(i * chunk_rows, (i + 1) * chunk_rows)
            pair = pair_up(rope(slabs[0][at], s, p), rope(slabs[1][at], s, p), low_half)
            for j in (0, 1):
                for core in (0, 1):
                    rows = slice(core * pair_rows, (core + 1) * pair_rows)
                    kv_send[s, j, core, p, :, :LANES] = pair[j][rows]
                    kv_send[s, j, core, p, :, LANES:] = vals[j][at][rows]
        if with_ctx:
            pair = pair_up(slabs[0][lat_count:], slabs[1][lat_count:], ctx_half)
            for j in (0, 1):
                kvc_send[s, j, :, :LANES] = pair[j]
                kvc_send[s, j, :, LANES:] = vals[j][lat_count:]
        for dj in (1, 0):
            j = (zl_i + dj) % 2
            for dc in (0, 1):
                core = (c_i + dc) % 2
                put = send if dj or dc else send_or_keep
                s_sem = kv_s.at[0] if dj or dc else kv_s.at[1]
                where = dict(sp=sp_at(half_i, j, c_i), tp=x_i * 2 + core)
                for p in ps:
                    put(
                        kv_send.at[s, j, core, p], kv_at(s, src_i, core, p),
                        s_sem, kv_r.at[s, p], **where,
                    )
                if with_ctx:
                    half = pl.ds(pl.multiple_of(core * (ctx_rows // 2), 16), ctx_rows // 2)
                    put(
                        kvc_send.at[s, j, half], kvc_at(s, src_i, core),
                        s_sem, kv_r.at[s, pieces], **where,
                    )
        q = jnp.dot(hidden[:lat_count, :], w[:, kv_cols:], preferred_element_type=f32)
        for i, p in enumerate(ps):
            at = slice(i * chunk_rows, (i + 1) * chunk_rows)
            pair = pair_up(rope(q[at, :LANES], s, p), rope(q[at, LANES:], s, p), low_half)
            for j in (0, 1):
                for core in (0, 1):
                    q_send[s, j, core, p] = pair[j][core * pair_rows : (core + 1) * pair_rows]
        for dj in (1, 0):
            j = (zl_i + dj) % 2
            for dc in (0, 1):
                core = (c_i + dc) % 2
                put = send if dj or dc else send_or_keep
                s_sem = q_s.at[0] if dj or dc else q_s.at[1]
                for p in ps:
                    put(
                        q_send.at[s, j, core, p], q_buf.at[q_at(s, src_i, p)],
                        s_sem, q_r.at[s, p],
                        sp=sp_at(half_i, j, c_i), tp=x_i * 2 + core,
                    )

    def relay(s, p):
        block = kv_block(s, c_i, p)
        arrived(block, kv_r.at[s, p])
        send(block, block, kv_s.at[0], rel_r.at[s], tp=partner)

    def wait_keys(s):
        start = s * keys + (1 - c_i) * core_keys
        arrived(kv_buf.at[pl.ds(pl.multiple_of(start, 16), core_keys)], rel_r.at[s])
        step = 2 * LANES
        for b in range(keys // step):
            at = s * keys + b * step
            vals_t[s, :, b * step : (b + 1) * step] = kv_buf[at : at + step, LANES:].T

    def wait_queries(s, p):
        arrived(
            q_buf.at[pl.ds((s * pieces + p) * 4 * pair_rows, 4 * pair_rows)], q_r.at[s, p]
        )

    coef = HEAD_DIM ** (-0.5) * 1.4426950408889634
    q_low = lax.broadcasted_iota(jnp.int32, (q_tile, LANES), 1) < HEAD_DIM
    cols = 2 * q_tile

    def item(tile, s, first, last):
        q = q_buf[tile * q_tile : (tile + 1) * q_tile, :]
        zero = jnp.zeros_like(q)
        q2 = jnp.concatenate([jnp.where(q_low, q, zero), jnp.where(q_low, zero, q)], axis=0)
        scores = lax.dot_general(
            kv_buf[s * keys : (s + 1) * keys, :LANES], q2, (((1,), (1,)), ((), ())),
            preferred_element_type=f32,
        )
        peak = jnp.max(scores, axis=0, keepdims=True)
        if not first:
            old = peak_s[tile]
            peak = jnp.maximum(old, peak)
        weights = jnp.exp2(scores * coef - peak * coef)
        sums = jnp.sum(weights.reshape(keys // 8, 8, cols), axis=0)
        acc = jnp.dot(vals_t[s], weights.astype(bf16), preferred_element_type=f32)
        if not first:
            fade = jnp.exp2((old - peak) * coef)
            sums = sums + sum_s[tile] * fade
            acc = acc + acc_s[tile] * fade
        if not last:
            peak_s[tile] = peak
            sum_s[tile] = sums
            acc_s[tile] = acc
            return
        mean_v = acc / jnp.sum(sums, axis=0, keepdims=True)
        mixed = mean_v[:, :q_tile] - gain_t[VALUE_DIM : VALUE_DIM + 1, :] * mean_v[:, q_tile:]
        factor = lax.rsqrt(jnp.mean(mixed * mixed, axis=0, keepdims=True) + norm_eps)
        o_send[tile * q_tile : (tile + 1) * q_tile, :] = (
            mixed * factor * gain_t[:VALUE_DIM, :]
        ).T.astype(bf16)

    def head_row(p, core, h):
        return ((p * 2 + core) * 4 + h) * pair_rows

    def give_back(s, p):
        half = half_i if s == 0 else 1 - half_i
        for dz, dy in mates + [(0, 0)]:
            zl = (zl_i + dz) % 2
            y = (y_i + dy) % 2
            put = send if s or dz or dy else send_or_keep
            put(
                o_send.at[q_at(s, zl * 2 + y, p)],
                heads.at[pl.ds(pl.multiple_of(head_row(p, c_i, z_i), 16), pair_rows)],
                o_s.at[0] if s or dz or dy else o_s.at[1], o_r.at[p],
                sp=sp_at(half, zl, y), tp=x_i * 2 + y_i,
            )

    parts = pair_send.shape[1]
    part_cols = width // parts

    def project(p):
        arrived(heads.at[pl.ds(head_row(p, 0, 0), 8 * pair_rows)], o_r.at[p])
        left = jnp.concatenate(
            [
                jnp.concatenate(
                    [
                        heads[pl.ds(pl.multiple_of(head_row(p, core, h), 16), pair_rows), :]
                        for h in range(4)
                    ],
                    axis=-1,
                )
                for core in (1 - c_i, c_i)
            ],
            axis=0,
        )
        for k in range(parts):
            at = slice(k * part_cols, (k + 1) * part_cols)
            terms = jnp.dot(left, wo[:, at], preferred_element_type=f32).astype(bf16)
            pair_send[p, k] = terms[:pair_rows]
            mine[p, k] = terms[pair_rows:]
            send(
                pair_send.at[p, k], pair_recv.at[p, k], pair_s.at[0], pair_r.at[p, k],
                tp=partner,
            )

    def combine(p):
        here = pl.ds(pl.multiple_of(x_i * rows_p, rows_p), rows_p)
        there = pl.ds(pl.multiple_of((1 - x_i) * rows_p, rows_p), rows_p)
        for k in range(parts):
            arrived(pair_recv.at[p, k], pair_r.at[p, k])
            both = mine[p, k, there, :].astype(f32) + pair_recv[p, k, there, :].astype(f32)
            fin_send[p, k] = both.astype(bf16)
            send(
                fin_send.at[p, k], fin_recv.at[p, k], fin_s.at[0], fin_r.at[p, k], tp=across
            )
            own_sum[p, k] = mine[p, k, here, :].astype(f32) + pair_recv[p, k, here, :].astype(f32)

    def finish(p):
        rows = slice(p * rows_p, (p + 1) * rows_p)
        for k in range(parts):
            arrived(fin_recv.at[p, k], fin_r.at[p, k])
            summed = own_sum[p, k] + fin_recv[p, k].astype(f32)
            for col in range(0, part_cols, gate_cols):
                at = slice(k * part_cols + col, k * part_cols + col + gate_cols)
                block = (k * part_cols + col) // gate_cols
                gate = gate_all[block // 4, block % 4 : block % 4 + 1, :]
                out[rows, at] = (
                    lat[rows, at].astype(f32) + gate * summed[:, col : col + gate_cols]
                ).astype(bf16)

    last = pieces - 1
    chunk(0, [0], True)
    @pl.when(jnp.logical_not(outer))
    def _():
        send_far(pieces)
        send_far(0)

    for p in range(1, pieces):
        from_across(0, p)
    chunk(0, list(range(1, pieces)), False)

    @pl.when(jnp.logical_not(outer))
    def _():
        for p in range(1, pieces):
            send_far(p)

    arrived(par_recv, par_sem.at[1])
    params = jnp.where(owns_head, par_own[...], par_recv[...])
    gain_row = jnp.broadcast_to(params[0:1, :], (VALUE_DIM, VALUE_DIM)).T
    lam_row = jnp.broadcast_to(params[1:2, :], (8, VALUE_DIM))
    for k in range(q_tile // VALUE_DIM):
        gain_t[:VALUE_DIM, k * VALUE_DIM : (k + 1) * VALUE_DIM] = gain_row
        gain_t[VALUE_DIM:, k * VALUE_DIM : (k + 1) * VALUE_DIM] = lam_row
    relay(0, 0)
    relay(0, pieces)
    for p in range(1, pieces):
        relay(0, p)
    from_far(pieces)
    from_far(0)
    from_across(1, pieces)
    wait_keys(0)
    for p in range(pieces):
        wait_queries(0, p)
    item(0, 0, True, False)
    from_across(1, 0)
    from_far(1)
    chunk(1, [0], True)
    item(1, 0, True, False)
    from_across(1, 1)
    for p in range(2, pieces):
        from_far(p)
    chunk(1, [1], False)
    relay(1, 0)
    relay(1, pieces)
    item(2, 0, True, False)
    gate_all[tp_i] = sum_sp(gate_recv, gate_sem)
    to_all_tp(gate_all, gate_sem)
    wait_queries(1, 0)
    item(pieces, 0, True, False)
    for p in range(2, pieces):
        from_across(1, p)
        chunk(1, [p], False)
    for p in range(1, last):
        relay(1, p)
    wait_queries(1, 1)
    item(pieces + 1, 0, True, False)
    relay(1, last)
    wait_keys(1)
    wait_queries(1, last)
    for p in range(pieces):
        if p == last:
            item(pieces + p, 0, True, False)
        item(pieces + p, 1, False, True)
        give_back(1, p)
        if p > 0:
            project(p - 1)
        item(p, 1, False, True)
        give_back(0, p)
        if p == 0:
            arrived(wo, w_sem.at[1])
        else:
            combine(p - 1)
    project(last)
    combine(last)
    arrived(gate_all.at[pl.ds(0, n_tp - 1)], gate_sem.at[3])
    for p in range(pieces):
        finish(p)
    def sent(ref, s_sem):
        pltpu.make_async_copy(ref, ref, s_sem).wait()

    far_rows = own + ctx_p
    sent(raw.at[pl.ds(0, 3 * own + 4 * far_rows)], raw_s.at[0])
    for sems, ref, tp_ref in (
        (mod_sem, mod_recv, mod_all), (gate_sem, gate_recv, gate_all),
    ):
        sent(ref.at[pl.ds(0, n_sp - 1)], sems.at[0])
        sent(tp_ref.at[pl.ds(0, n_tp - 1)], sems.at[2])
    sent(par_own, par_sem.at[0])
    sent(kv_buf.at[pl.ds(0, 3 * set_rows + 2 * core_keys)], kv_s.at[0])
    sent(q_buf.at[pl.ds(0, 3 * tok)], q_s.at[0])
    sent(o_send.at[pl.ds(0, 7 * pieces * pair_rows)], o_s.at[0])
    sent(pair_send, pair_s.at[0])
    sent(fin_send, fin_s.at[0])

    @pl.when(jnp.logical_not(owns_head))
    def _():
        sent(kv_buf.at[pl.ds(0, set_rows)], kv_s.at[1])
        sent(q_buf.at[pl.ds(0, tok)], q_s.at[1])
        sent(o_send.at[pl.ds(0, pieces * pair_rows)], o_s.at[1])


def split_scratch(n_sp, n_tp, own, width, ctx_rows, mod_cols, groups):
    tok = own * n_tp
    pieces = 3
    rows_p = own // pieces
    pair_rows = 2 * rows_p
    q_tile = 4 * pair_rows
    keys = 4 * (tok + ctx_rows)
    parts = 2
    part_cols = width // parts
    dma = pltpu.SemaphoreType.DMA
    return [
        pltpu.VMEM((width, 4 * 2 * HEAD_DIM + 2 * VALUE_DIM), bf16),
        pltpu.VMEM((groups * VALUE_DIM, width), bf16),
        pltpu.VMEM((8, mod_cols // 2), f32),
        pltpu.VMEM((n_sp, 8, mod_cols // 2), f32),
        pltpu.VMEM((n_tp, 8, mod_cols // 2), f32),
        pltpu.VMEM((8, mod_cols // 4), f32),
        pltpu.VMEM((n_sp, 8, mod_cols // 4), f32),
        pltpu.VMEM((n_tp, 8, mod_cols // 4), f32),
        pltpu.VMEM((8, VALUE_DIM), f32),
        pltpu.VMEM((8, VALUE_DIM), f32),
        pltpu.VMEM((8 * own, width), bf16),
        pltpu.VMEM((ctx_rows, width), bf16),
        pltpu.VMEM((4 * pair_rows + ctx_rows, width), bf16),
        pltpu.VMEM((2, pieces, 2 * pair_rows, LANES), f32),
        pltpu.VMEM((2, pieces, 2 * pair_rows, LANES), f32),
        pltpu.VMEM((2, 2, 2, pieces, pair_rows, 2 * LANES), bf16),
        pltpu.VMEM((2, 2, ctx_rows, 2 * LANES), bf16),
        pltpu.VMEM((2, 2, 2, pieces, pair_rows, LANES), bf16),
        pltpu.VMEM((2 * keys, 2 * LANES), bf16),
        pltpu.VMEM((2 * pieces * q_tile, LANES), bf16),
        pltpu.VMEM((2, VALUE_DIM, keys), bf16),
        pltpu.VMEM((VALUE_DIM + 8, q_tile), f32),
        pltpu.VMEM((2 * pieces, 1, 2 * q_tile), f32),
        pltpu.VMEM((2 * pieces, 8, 2 * q_tile), f32),
        pltpu.VMEM((2 * pieces, VALUE_DIM, 2 * q_tile), f32),
        pltpu.VMEM((2 * pieces * q_tile, LANES), bf16),
        pltpu.VMEM((8 * pieces * pair_rows, LANES), bf16),
        pltpu.VMEM((pieces, parts, pair_rows, part_cols), bf16),
        pltpu.VMEM((pieces, parts, pair_rows, part_cols), bf16),
        pltpu.VMEM((pieces, parts, pair_rows, part_cols), bf16),
        pltpu.VMEM((pieces, parts, rows_p, part_cols), bf16),
        pltpu.VMEM((pieces, parts, rows_p, part_cols), bf16),
        pltpu.VMEM((pieces, parts, rows_p, part_cols), f32),
        dma((2,)),
        dma((2,)),
        dma((4,)),
        dma((4,)),
        dma((1,)),
        dma((pieces + 1,)),
        dma((2, pieces + 1)),
        dma((2, pieces + 1)),
        dma((2,)),
        dma((2, pieces + 1)),
        dma((2,)),
        dma((2,)),
        dma((2, pieces)),
        dma((2,)),
        dma((pieces,)),
        dma((1,)),
        dma((pieces, parts)),
        dma((1,)),
        dma((pieces, parts)),
    ]


def local(
    n_sp,
    n_tp,
    latent,
    context,
    cond_latent,
    cond_context,
    shift_weight,
    scale_weight,
    gate_weight,
    query_weight,
    key_weight,
    value_weight,
    out_weight,
    lambda_heads,
    out_gain,
):
    own, width = latent.shape
    ctx_rows = context.shape[0]
    tok = own * n_tp
    groups = lambda_heads.shape[0]
    ranks = n_sp // groups
    chips = n_tp // 2
    mod_rows, mod_cols = shift_weight.shape
    keys = n_sp * (tok + ctx_rows)
    q_tile = pick(tok, 128, 16)
    pieces = 3 if own % 48 == 0 else 1
    parts = 4 if width % (4 * LANES) == 0 else 1

    quarter = HEAD_DIM // 4
    inverse = np.float32(rope_theta) ** (-np.arange(quarter, dtype=np.float32) / quarter)
    zeros = np.zeros((quarter,), np.float32)
    repeat = LANES // (2 * quarter)
    half = np.ones((2 * quarter,), np.float32)
    lane_table = np.zeros((8, LANES), np.float32)
    lane_table[0] = np.tile(np.concatenate([inverse, zeros]), repeat)
    lane_table[1] = np.tile(np.concatenate([zeros, inverse]), repeat)
    lane_table[2] = np.tile(np.concatenate([-half, half]), repeat // 2)
    gain = out_gain.reshape(groups, 1, VALUE_DIM)
    vmem = pl.BlockSpec(memory_space=pltpu.VMEM)
    hbm = pl.BlockSpec(memory_space=pl.ANY)
    dma = pltpu.SemaphoreType.DMA
    scratch = [
        pltpu.VMEM(query_weight.shape, bf16),
        pltpu.VMEM(key_weight.shape, bf16),
        pltpu.VMEM(value_weight.shape, bf16),
        pltpu.VMEM(out_weight.shape, bf16),
        pltpu.VMEM((8, mod_cols), f32),
        pltpu.VMEM((n_sp, 8, mod_cols), f32),
        pltpu.VMEM((n_tp, 8, mod_cols), f32),
        pltpu.VMEM((n_tp, own, width), bf16),
        pltpu.VMEM((2 * own + ctx_rows, width), bf16),
        pltpu.VMEM((tok, LANES), f32),
        pltpu.VMEM((tok, LANES), f32),
        pltpu.VMEM((groups, tok, LANES), bf16),
        pltpu.VMEM((groups, tok, 2 * LANES), bf16),
        pltpu.VMEM((groups, ctx_rows, 2 * LANES), bf16),
        pltpu.VMEM((groups, tok, LANES), bf16),
        pltpu.VMEM((keys, 2 * LANES), bf16),
        pltpu.VMEM((2 * q_tile, keys), f32),
        pltpu.VMEM((groups, tok, LANES), bf16),
        pltpu.VMEM((groups, tok, LANES), bf16),
        pltpu.VMEM((chips, parts, own, width // parts), bf16),
        pltpu.VMEM((chips, parts, own, width // parts), bf16),
        pltpu.VMEM((max(chips - 1, 1), parts, own, width // parts), bf16),
        pltpu.VMEM((max(chips - 1, 1), parts, own, width // parts), bf16),
        pltpu.VMEM((parts, own, width // parts), f32),
        dma((4,)),
        dma((3,)),
        dma((n_sp,)),
        dma((n_sp,)),
        dma((n_tp,)),
        dma((n_tp,)),
        dma((chips, pieces)),
        dma((chips, pieces)),
        dma((chips, pieces)),
        dma((chips, pieces)),
        dma((groups,)),
        dma((groups,)),
        dma((groups, chips)),
        dma((groups, chips)),
        dma((groups,)),
        dma((groups,)),
        dma((groups, chips, ranks)),
        dma((groups, chips, ranks)),
        dma((groups, ranks)),
        dma((groups, ranks)),
        dma((groups, tok // q_tile)),
        dma((groups, tok // q_tile)),
        dma((chips, parts)),
        dma((chips, parts)),
        dma((chips, parts)),
        dma((chips, parts)),
    ]
    kernel = body
    fits = own % 48 == 0 and ctx_rows % (16 * n_tp) == 0 and own * 8 // 3 % LANES == 0
    if (n_sp, n_tp, groups) == (8, 4, 4) and fits and (tok + ctx_rows) % 64 == 0:
        kernel = split_body
        scratch = split_scratch(n_sp, n_tp, own, width, ctx_rows, mod_cols, groups)
    return pl.pallas_call(
        functools.partial(kernel, n_sp, n_tp),
        out_shape=jax.ShapeDtypeStruct((own, width), bf16),
        in_specs=[vmem] * 8 + [pl.BlockSpec(memory_space=pltpu.SMEM), vmem] + [hbm] * 4,
        out_specs=vmem,
        scratch_shapes=scratch,
        compiler_params=pltpu.CompilerParams(
            collective_id=0, has_side_effects=True, vmem_limit_bytes=60 * 1024 * 1024
        ),
        name="diff_attention",
    )(
        latent,
        context,
        cond_latent.reshape(n_sp, 1, mod_rows),
        cond_context.reshape(n_sp, 1, mod_rows),
        shift_weight,
        scale_weight,
        gate_weight,
        jnp.asarray(lane_table),
        lambda_heads,
        gain,
        query_weight,
        key_weight,
        value_weight,
        out_weight,
    )


def solution(mesh):
    placed = (
        P(("sp", "tp"), None),
        P("sp", None),
        P(),
        P(),
        P("sp", "tp"),
        P("sp", "tp"),
        P("sp", "tp"),
        P(None, None, "tp"),
        P(None, None, "tp"),
        P(None, "tp"),
        P("tp", None),
        P("tp"),
        P("tp"),
    )
    return jax.shard_map(
        functools.partial(local, mesh.shape["sp"], mesh.shape["tp"]),
        mesh=mesh,
        in_specs=placed,
        out_specs=P(("sp", "tp"), None),
        check_vma=False,
    )
```

```python
import functools

import jax
import jax.numpy as jnp
import numpy as np
from jax import lax
from jax.experimental import pallas as pl
from jax.experimental.pallas import tpu as pltpu
from jax.sharding import PartitionSpec as P

HEAD_DIM = 64
GRID_W = 64
VALUE_DIM = 128
LANES = 128

norm_eps = 1e-06
rope_theta = 10000.0
f32 = jnp.float32
bf16 = jnp.bfloat16
MESH = pl.DeviceIdType.MESH


def pick(total, limit, unit):
    best = unit
    for size in range(unit, limit + 1, unit):
        if total % size == 0:
            best = size
    return best


def body(
    n_sp,
    n_tp,
    lat,
    ctx,
    cond_l,
    cond_c,
    shift_w,
    scale_w,
    gate_w,
    lane_table,
    lam,
    gain,
    wq_hbm,
    wk_hbm,
    wv_hbm,
    wo_hbm,
    out,
    wq,
    wk,
    wv,
    wo,
    mod_part,
    mod_recv,
    mod_all,
    raw,
    hidden,
    cos_t,
    sin_t,
    q_send,
    kv_send,
    kvc_send,
    q_buf,
    kv_buf,
    scores,
    o_send,
    heads,
    pair_send,
    pair_recv,
    fin_send,
    fin_recv,
    own_sum,
    w_sem,
    loc_sem,
    mod1_s,
    mod1_r,
    mod2_s,
    mod2_r,
    raw_s,
    raw_r,
    fwd_s,
    fwd_r,
    q_s,
    q_r,
    kv_s,
    kv_r,
    kvc_s,
    kvc_r,
    rel_s,
    rel_r,
    relc_s,
    relc_r,
    o_s,
    o_r,
    pair_s,
    pair_r,
    fin_s,
    fin_r,
):
    own, width = lat.shape
    ctx_rows = ctx.shape[0]
    tok = own * n_tp
    mod_cols = shift_w.shape[1]
    groups = q_send.shape[0]
    ranks = n_sp // groups
    chips = n_tp // 2
    sp_i = lax.axis_index("sp")
    tp_i = lax.axis_index("tp")
    g_i = sp_i // ranks
    r_i = sp_i % ranks
    chip_i = tp_i // 2
    core_i = tp_i % 2
    partner = chip_i * 2 + (1 - core_i)
    pending = []

    def send(src, dst, s_sem, r_sem, **where):
        copy = pltpu.make_async_remote_copy(
            src_ref=src, dst_ref=dst, send_sem=s_sem, recv_sem=r_sem,
            device_id=where, device_id_type=MESH,
        )
        copy.start()
        pending.append(copy)

    def arrived(ref, s_sem, r_sem, **where):
        pltpu.make_async_remote_copy(
            src_ref=ref, dst_ref=ref, send_sem=s_sem, recv_sem=r_sem,
            device_id=where, device_id_type=MESH,
        ).wait_recv()

    loads = [
        pltpu.make_async_copy(src, dst, w_sem.at[i])
        for i, (src, dst) in enumerate(
            ((wk_hbm, wk), (wv_hbm, wv), (wq_hbm, wq), (wo_hbm, wo))
        )
    ]
    for load in loads:
        load.start()

    barrier = pltpu.get_barrier_semaphore()
    for k in range(1, n_sp):
        pl.semaphore_signal(
            barrier, inc=1, device_id={"sp": (sp_i + k) % n_sp}, device_id_type=MESH
        )
    for k in range(1, n_tp):
        pl.semaphore_signal(
            barrier, inc=1, device_id={"tp": (tp_i + k) % n_tp}, device_id_type=MESH
        )

    def silu(v):
        return (v / (1.0 + jnp.exp(-v))).astype(bf16).astype(f32)

    c0 = silu(cond_l[sp_i])
    c1 = silu(cond_c[sp_i])
    row = lax.broadcasted_iota(jnp.int32, (8, c0.shape[-1]), 0)

    def placed_rows(at0, at1):
        zero = jnp.zeros(row.shape, f32)
        rows = jnp.where(row == at0, jnp.broadcast_to(c0, row.shape), zero)
        if at1 is not None:
            rows = jnp.where(row == at1, jnp.broadcast_to(c1, row.shape), rows)
        return rows.astype(bf16)

    mod_part[...] = (
        jnp.dot(placed_rows(0, 1), shift_w[...], preferred_element_type=f32)
        + jnp.dot(placed_rows(2, 3), scale_w[...], preferred_element_type=f32)
        + jnp.dot(placed_rows(4, None), gate_w[...], preferred_element_type=f32)
    )
    pl.semaphore_wait(barrier, n_sp + n_tp - 2)

    for k in range(1, n_sp):
        send(
            mod_part, mod_recv.at[sp_i], mod1_s.at[k], mod1_r.at[sp_i], sp=(sp_i + k) % n_sp
        )
    pieces = raw_s.shape[1]
    piece_rows = own // pieces

    def raw_piece(slot, i):
        return raw.at[slot, pl.ds(i * piece_rows, piece_rows)]

    def send_raw(i):
        for k in range(1, chips):
            send(
                lat.at[pl.ds(i * piece_rows, piece_rows)], raw_piece(tp_i, i),
                raw_s.at[k, i], raw_r.at[chip_i, i],
                tp=((chip_i + k) % chips) * 2 + core_i,
            )

    def relay_raw(i):
        for k in range(1, chips):
            src_chip = (chip_i + chips - k) % chips
            slot = src_chip * 2 + core_i
            arrived(raw_piece(slot, i), raw_s.at[k, i], raw_r.at[src_chip, i], tp=slot)
            send(
                raw_piece(slot, i), raw_piece(slot, i), fwd_s.at[k, i], fwd_r.at[src_chip, i],
                tp=partner,
            )

    early = max(pieces - 1, 1)
    for i in range(early):
        send_raw(i)
    send(lat, raw.at[tp_i], fwd_s.at[0, 0], fwd_r.at[chip_i, 0], tp=partner)
    raw[tp_i] = lat[...]
    mod_recv[sp_i] = mod_part[...]

    tok_row = lax.broadcasted_iota(jnp.int32, (tok, LANES), 0) + sp_i * tok
    grid_row = (tok_row // GRID_W).astype(f32)
    grid_col = (tok_row % GRID_W).astype(f32)
    angles = grid_row * lane_table[0:1, :] + grid_col * lane_table[1:2, :]
    cos_t[...] = jnp.cos(angles)
    sin_t[...] = jnp.sin(angles) * lane_table[2:3, :]

    for k in range(1, n_sp):
        src = (sp_i + n_sp - k) % n_sp
        arrived(mod_recv.at[src], mod1_s.at[k], mod1_r.at[src], sp=src)
    total = mod_recv[0]
    for s in range(1, n_sp):
        total = total + mod_recv[s]
    mod_part2 = mod_all.at[tp_i]
    mod_part2[...] = total
    for k in range(1, n_tp):
        send(
            mod_part2, mod_all.at[tp_i], mod2_s.at[k], mod2_r.at[tp_i], tp=(tp_i + k) % n_tp
        )
    for i in range(early, pieces):
        send_raw(i)
    for i in range(early):
        relay_raw(i)
    for k in range(1, n_tp):
        src = (tp_i + n_tp - k) % n_tp
        arrived(mod_all.at[src], mod2_s.at[k], mod2_r.at[src], tp=src)

    def modulate(x, which, start):
        at = pl.ds(start if isinstance(start, int) else pl.multiple_of(start, 16), x.shape[0])
        factor = lax.rsqrt(jnp.mean(x * x, axis=-1, keepdims=True) + norm_eps)
        for t in range(n_tp):
            cols = slice(t * mod_cols, (t + 1) * mod_cols)
            shift = mod_all[t, which : which + 1, :]
            scale = mod_all[t, which + 2 : which + 3, :]
            hidden[at, cols] = (
                (x[:, cols] * factor) * (1.0 + scale) + shift
            ).astype(bf16)

    half = 2 * own
    lane = lax.broadcasted_iota(jnp.int32, (half, LANES), 1)
    first_quarter = lane % HEAD_DIM < HEAD_DIM // 2
    low_half = lane < HEAD_DIM
    ctx_half = lax.broadcasted_iota(jnp.int32, (ctx_rows, LANES), 1) < HEAD_DIM

    def rope(u, rows):
        swapped = jnp.where(
            first_quarter,
            pltpu.roll(u, LANES - HEAD_DIM // 2, 1),
            pltpu.roll(u, HEAD_DIM // 2, 1),
        )
        return u * cos_t[rows, :] + swapped * sin_t[rows, :]

    def pair_up(a, b, low):
        return (
            jnp.where(low, a, pltpu.roll(b, HEAD_DIM, 1)).astype(bf16),
            jnp.where(low, pltpu.roll(a, HEAD_DIM, 1), b).astype(bf16),
        )

    def lat_slot(s, chip=None):
        if chip is None:
            return kv_buf.at[pl.ds(pl.multiple_of(s * tok, 16), tok)]
        return kv_buf.at[pl.ds(pl.multiple_of(s * tok + chip * half, 16), half)]

    def ctx_slot(s):
        return kv_buf.at[pl.ds(pl.multiple_of(n_sp * tok + s * ctx_rows, 16), ctx_rows)]

    order = list(range(1, groups))
    for c in range(chips):
        chip = (chip_i + c) % chips
        rows = pl.ds(pl.multiple_of(chip * half, 16), half)
        if c == 0:
            modulate(ctx[...].astype(f32), 1, half)
            modulate(raw[tp_i].astype(f32), 0, core_i * own)
            arrived(raw.at[partner], fwd_s.at[0, 0], fwd_r.at[chip_i, 0], tp=partner)
            modulate(raw[partner].astype(f32), 0, (1 - core_i) * own)
            for i in range(early, pieces):
                relay_raw(i)
            count = half + ctx_rows
        else:
            slot = chip * 2 + core_i
            modulate(raw[slot].astype(f32), 0, core_i * own)
            slot = chip * 2 + (1 - core_i)
            for i in range(pieces):
                arrived(
                    raw_piece(slot, i), fwd_s.at[chips - c, i], fwd_r.at[chip, i], tp=partner
                )
            modulate(raw[slot].astype(f32), 0, (1 - core_i) * own)
            count = half
        if c == 0:
            loads[0].wait()
        keys = [jnp.dot(hidden[:count, :], wk[m], preferred_element_type=f32) for m in (0, 1)]
        for p in range(groups // 2):
            slab = slice(p * LANES, (p + 1) * LANES)
            a, b = pair_up(
                rope(keys[0][:half, slab], rows), rope(keys[1][:half, slab], rows), low_half
            )
            kv_send[2 * p, rows, :LANES] = a
            kv_send[2 * p + 1, rows, :LANES] = b
            if c == 0:
                a, b = pair_up(keys[0][half:, slab], keys[1][half:, slab], ctx_half)
                kvc_send[2 * p, :, :LANES] = a
                kvc_send[2 * p + 1, :, :LANES] = b
        if c == 0:
            loads[1].wait()
        vals = jnp.dot(hidden[:count, :], wv[...], preferred_element_type=f32).astype(bf16)
        for j in range(groups):
            slab = slice(j * LANES, (j + 1) * LANES)
            kv_send[j, rows, LANES:] = vals[:half, slab]
            if c == 0:
                kvc_send[j, :, LANES:] = vals[half:, slab]
        for k in order:
            g = (g_i + k) % groups
            to = g * ranks + r_i
            send(
                kv_send.at[g, rows], lat_slot(sp_i, chip), kv_s.at[k, c], kv_r.at[g_i, c], sp=to
            )
            if c == 0:
                send(kvc_send.at[g], ctx_slot(sp_i), kvc_s.at[k], kvc_r.at[g_i], sp=to)
        for e in range(1, ranks):
            to = g_i * ranks + (r_i + e) % ranks
            send(
                kv_send.at[g_i, rows], lat_slot(sp_i, chip), rel_s.at[0, c, e],
                rel_r.at[g_i, c, r_i], sp=to,
            )
            if c == 0:
                send(
                    kvc_send.at[g_i], ctx_slot(sp_i), relc_s.at[0, e], relc_r.at[g_i, r_i], sp=to
                )
        if c == 0:
            loads[2].wait()
        queries = [
            jnp.dot(hidden[:half, :], wq[m], preferred_element_type=f32) for m in (0, 1)
        ]
        for p in range(groups // 2):
            slab = slice(p * LANES, (p + 1) * LANES)
            a, b = pair_up(
                rope(queries[0][:, slab], rows), rope(queries[1][:, slab], rows), low_half
            )
            q_send[2 * p, rows, :] = a
            q_send[2 * p + 1, rows, :] = b
    for k in order:
        g = (g_i + k) % groups
        send(q_send.at[g], q_buf.at[g_i], q_s.at[k], q_r.at[g_i], sp=g * ranks + r_i)
    local = [
        pltpu.make_async_copy(kv_send.at[g_i], lat_slot(sp_i), loc_sem.at[0]),
        pltpu.make_async_copy(kvc_send.at[g_i], ctx_slot(sp_i), loc_sem.at[1]),
        pltpu.make_async_copy(q_send.at[g_i], q_buf.at[g_i], loc_sem.at[2]),
    ]
    for copy in local:
        copy.start()

    for c in range(chips):
        chip = (chip_i + c) % chips
        for k in order:
            g = (g_i + groups - k) % groups
            s = g * ranks + r_i
            arrived(lat_slot(s, chip), kv_s.at[k, c], kv_r.at[g, c], sp=s)
            for e in range(1, ranks):
                to = g_i * ranks + (r_i + e) % ranks
                send(
                    lat_slot(s, chip), lat_slot(s, chip), rel_s.at[k, c, e],
                    rel_r.at[g, c, r_i], sp=to,
                )
            if c == 0:
                arrived(ctx_slot(s), kvc_s.at[k], kvc_r.at[g], sp=s)
                for e in range(1, ranks):
                    to = g_i * ranks + (r_i + e) % ranks
                    send(
                        ctx_slot(s), ctx_slot(s), relc_s.at[k, e], relc_r.at[g, r_i], sp=to
                    )
    for copy in local:
        copy.wait()
    for e in range(1, ranks):
        r = (r_i + ranks - e) % ranks
        to = g_i * ranks + r
        for k in range(groups):
            g = (g_i + groups - k) % groups
            s = g * ranks + r
            for c in range(chips):
                chip = (chip_i + c) % chips
                arrived(lat_slot(s, chip), rel_s.at[k, c, e], rel_r.at[g, c, r], sp=to)
            arrived(ctx_slot(s), relc_s.at[k, e], relc_r.at[g, r], sp=to)

    key_total = kv_buf.shape[0]
    q_tile = scores.shape[0] // 2
    block = pick(key_total, 512, LANES)
    coef = HEAD_DIM ** (-0.5) * 1.4426950408889634
    q_low = lax.broadcasted_iota(jnp.int32, (q_tile, LANES), 1) < HEAD_DIM
    head_lam = lam[g_i]
    tiles = tok // q_tile
    head_gain = gain[g_i]

    def attend(g, start):
        q = q_buf[g, pl.ds(start, q_tile), :]
        zero = jnp.zeros_like(q)
        q2 = jnp.concatenate([jnp.where(q_low, q, zero), jnp.where(q_low, zero, q)], axis=0)
        peak = None
        for b in range(key_total // block):
            rows = slice(b * block, (b + 1) * block)
            s = lax.dot_general(
                q2, kv_buf[rows, :LANES], (((1,), (1,)), ((), ())), preferred_element_type=f32
            )
            scores[:, rows] = s
            for c in range(block // LANES):
                piece = s[:, c * LANES : (c + 1) * LANES]
                peak = piece if peak is None else jnp.maximum(peak, piece)
        top = jnp.max(peak, axis=-1, keepdims=True) * coef
        sums = None
        acc = None
        for b in range(key_total // block):
            rows = slice(b * block, (b + 1) * block)
            w = jnp.exp2(scores[:, rows] * coef - top)
            for c in range(block // LANES):
                piece = w[:, c * LANES : (c + 1) * LANES]
                sums = piece if sums is None else sums + piece
            part = jnp.dot(w.astype(bf16), kv_buf[rows, LANES:], preferred_element_type=f32)
            acc = part if acc is None else acc + part
        mean_v = acc / jnp.sum(sums, axis=-1, keepdims=True)
        mixed = mean_v[:q_tile] - head_lam * mean_v[q_tile:]
        factor = lax.rsqrt(jnp.mean(mixed * mixed, axis=-1, keepdims=True) + norm_eps)
        o_send[g, pl.ds(start, q_tile), :] = (mixed * factor * head_gain).astype(bf16)

    def o_copy(k, i):
        g = (g_i + groups - k) % groups
        rows = pl.ds(pl.multiple_of(i * q_tile, 16), q_tile)
        return pltpu.make_async_remote_copy(
            src_ref=o_send.at[g, rows], dst_ref=heads.at[g_i, rows], send_sem=o_s.at[k, i],
            recv_sem=o_r.at[g_i, i], device_id={"sp": g * ranks + r_i}, device_id_type=MESH,
        )

    @pl.loop(0, groups)
    def _(k):
        g = (g_i + groups - k) % groups

        @pl.when(k > 0)
        def _():
            arrived(q_buf.at[g], q_s.at[k], q_r.at[g], sp=g * ranks + r_i)

        @pl.loop(0, tiles)
        def _(i):
            attend(g, pl.multiple_of(i * q_tile, q_tile))

            @pl.when(k > 0)
            def _():
                o_copy(k, i).start()

    heads[g_i] = o_send[g_i]
    loads[3].wait()
    for k in order:
        src = (g_i + k) % groups
        for i in range(tiles):
            rows = pl.ds(i * q_tile, q_tile)
            arrived(heads.at[src, rows], o_s.at[k, i], o_r.at[src, i], sp=src * ranks + r_i)

    parts = pair_send.shape[1]
    part_cols = width // parts

    def head_rows(chunk):
        start = pl.multiple_of(chunk * own, 16)
        return jnp.concatenate(
            [heads[h, pl.ds(start, own), :] for h in range(groups)], axis=-1
        )

    def term(left, p):
        cols = slice(p * part_cols, (p + 1) * part_cols)
        return jnp.dot(left, wo[:, cols], preferred_element_type=f32).astype(bf16)

    def to_partner(k):
        chip = (chip_i + 1 + k) % chips
        left = head_rows(chip * 2 + (1 - core_i))
        for p in range(parts):
            pair_send[k, p] = term(left, p)
            send(
                pair_send.at[k, p], pair_recv.at[k, p], pair_s.at[k, p], pair_r.at[k, p],
                tp=partner,
            )

    def with_partner(k):
        chip = (chip_i + 1 + k) % chips
        left = head_rows(chip * 2 + core_i)
        for p in range(parts):
            mine = term(left, p).astype(f32)
            arrived(pair_recv.at[k, p], pair_s.at[k, p], pair_r.at[k, p], tp=partner)
            both = mine + pair_recv[k, p].astype(f32)
            if k < chips - 1:
                fin_send[k, p] = both.astype(bf16)
                send(
                    fin_send.at[k, p], fin_recv.at[k, p], fin_s.at[k, p], fin_r.at[k, p],
                    tp=chip * 2 + core_i,
                )
            else:
                own_sum[p] = both

    for k in range(chips - 1):
        to_partner(k)
    for k in range(chips - 1):
        with_partner(k)
    to_partner(chips - 1)
    with_partner(chips - 1)
    for p in range(parts):
        summed = own_sum[p]
        for k in range(chips - 1):
            src_chip = (chip_i + chips - 1 - k) % chips
            arrived(
                fin_recv.at[k, p], fin_s.at[k, p], fin_r.at[k, p], tp=src_chip * 2 + core_i
            )
            summed = summed + fin_recv[k, p].astype(f32)
        cols = slice(p * part_cols, (p + 1) * part_cols)
        per = mod_cols // part_cols
        if per >= 1:
            low = (p % per) * part_cols
            gate = mod_all[p // per, 4:5, low : low + part_cols]
        else:
            span = part_cols // mod_cols
            gate = jnp.concatenate(
                [mod_all[p * span + q, 4:5, :] for q in range(span)], axis=-1
            )
        out[:, cols] = (lat[:, cols].astype(f32) + gate * summed).astype(bf16)
    for copy in pending:
        copy.wait_send()
    for k in order:
        for i in range(tiles):
            o_copy(k, i).wait_send()


def split_body(
    n_sp,
    n_tp,
    lat_hbm,
    ctx_hbm,
    cond_l_hbm,
    cond_c_hbm,
    shift_hbm,
    scale_hbm,
    gate_hbm,
    lane_table_hbm,
    lam,
    gain_hbm,
    wq_hbm,
    wk_hbm,
    wv_hbm,
    wo_hbm,
    out,
    lat,
    ctx,
    cond_l,
    cond_c,
    shift_w,
    scale_w,
    gate_w,
    lane_table,
    gain,
    w,
    wo,
    mod_part,
    mod_recv,
    mod_all,
    gate_part,
    gate_recv,
    gate_all,
    par_own,
    par_recv,
    raw,
    far_ctx,
    hidden,
    cos_t,
    sin_t,
    kv_send,
    kvc_send,
    q_send,
    kv_buf,
    q_buf,
    vals_t,
    gain_t,
    peak_s,
    sum_s,
    acc_s,
    o_send,
    heads,
    mine,
    pair_send,
    pair_recv,
    fin_send,
    fin_recv,
    own_sum,
    in_sem,
    w_sem,
    par_sem,
    mod_sem,
    gate_sem,
    raw_s,
    z_r,
    x_r,
    d_r,
    kv_s,
    kv_r,
    rel_r,
    q_s,
    q_r,
    o_s,
    o_r,
    pair_s,
    pair_r,
    fin_s,
    fin_r,
):
    own, width = lat.shape
    ctx_rows = ctx.shape[0]
    tok = own * n_tp
    mod_cols = shift_w.shape[1]
    pieces = z_r.shape[0] - 1
    rows_p = own // pieces
    ctx_p = ctx_rows // n_tp
    pair_rows = 2 * rows_p
    chunk_rows = 2 * pair_rows
    set_rows = tok + ctx_rows
    keys = 4 * set_rows
    q_tile = 4 * pair_rows
    sp_i = lax.axis_index("sp")
    tp_i = lax.axis_index("tp")
    z_i = sp_i // 2
    y_i = sp_i % 2
    half_i = z_i // 2
    zl_i = z_i % 2
    src_i = zl_i * 2 + y_i
    x_i = tp_i // 2
    c_i = tp_i % 2
    slot_i = c_i * 2 + x_i
    mirror = (sp_i + 4) % n_sp
    partner = x_i * 2 + (1 - c_i)
    across = (1 - x_i) * 2 + c_i
    owns_head = c_i == y_i

    def remote(src, dst, s_sem, r_sem, **where):
        return pltpu.make_async_remote_copy(
            src_ref=src, dst_ref=dst, send_sem=s_sem, recv_sem=r_sem,
            device_id=where, device_id_type=MESH,
        )

    def send(src, dst, s_sem, r_sem, **where):
        remote(src, dst, s_sem, r_sem, **where).start()

    def send_or_keep(src, dst, s_sem, r_sem, **where):
        copy = remote(src, dst, s_sem, r_sem, **where)

        @pl.when(owns_head)
        def _():
            pltpu.make_async_copy(src, dst, r_sem).start()

        @pl.when(jnp.logical_not(owns_head))
        def _():
            copy.start()

    def arrived(ref, r_sem):
        pltpu.make_async_copy(ref, ref, r_sem).wait()

    def sp_at(half, zl, y):
        return (half * 2 + zl) * 2 + y

    staged = [
        pltpu.make_async_copy(a, b, in_sem.at[i])
        for i, (a, b) in enumerate(
            (
                (cond_l_hbm, cond_l), (cond_c_hbm, cond_c), (shift_hbm, shift_w),
                (scale_hbm, scale_w), (gain_hbm, gain), (lat_hbm, lat), (ctx_hbm, ctx),
                (gate_hbm, gate_w), (lane_table_hbm, lane_table),
            )
        )
    ]
    for copy in staged:
        copy.start()

    head_cols = 2 * HEAD_DIM
    val_cols = 2 * VALUE_DIM

    def part_cols_of(start, size):
        return pl.ds(pl.multiple_of(start, LANES), size)

    loads = []
    for m in (0, 1):
        loads.append(
            (wk_hbm.at[m, :, part_cols_of(half_i * head_cols, head_cols)],
             w.at[:, pl.ds(m * head_cols, head_cols)])
        )
    loads.append(
        (wv_hbm.at[:, part_cols_of(half_i * val_cols, val_cols)],
         w.at[:, pl.ds(2 * head_cols, val_cols)])
    )
    for m in (0, 1):
        loads.append(
            (wq_hbm.at[m, :, part_cols_of(half_i * head_cols, head_cols)],
             w.at[:, pl.ds(2 * head_cols + val_cols + m * head_cols, head_cols)])
        )
    loads = [pltpu.make_async_copy(a, b, w_sem.at[0]) for a, b in loads]
    loads.append(pltpu.make_async_copy(wo_hbm, wo, w_sem.at[1]))

    barrier = pltpu.get_barrier_semaphore()
    for k in range(1, n_sp):
        for tp in (tp_i, partner):
            pl.semaphore_signal(
                barrier, inc=1, device_id={"sp": (sp_i + k) % n_sp, "tp": tp},
                device_id_type=MESH,
            )
    for k in range(1, n_tp):
        pl.semaphore_signal(
            barrier, inc=1, device_id={"tp": (tp_i + k) % n_tp}, device_id_type=MESH
        )

    for load in loads:
        load.start()
    for copy in staged[:5]:
        copy.wait()

    def silu(v):
        return (v / (1.0 + jnp.exp(-v))).astype(bf16).astype(f32)

    c0 = silu(cond_l[sp_i])
    c1 = silu(cond_c[sp_i])
    row = lax.broadcasted_iota(jnp.int32, (8, c0.shape[-1]), 0)

    def placed_rows(at0, at1):
        zero = jnp.zeros(row.shape, f32)
        rows = jnp.where(row == at0, jnp.broadcast_to(c0, row.shape), zero)
        if at1 is not None:
            rows = jnp.where(row == at1, jnp.broadcast_to(c1, row.shape), rows)
        return rows.astype(bf16)

    half_cols = mod_cols // 2
    mod_total = None
    for k in (0, 1):
        at = slice(k * half_cols, (k + 1) * half_cols)
        for first, weight in ((4 * k, shift_w), (4 * k + 2, scale_w)):
            term = jnp.dot(
                placed_rows(first, first + 1), weight[:, at], preferred_element_type=f32
            )
            mod_total = term if mod_total is None else mod_total + term
    mod_part[...] = mod_total
    par_own[0:1, :] = gain[z_i]
    par_own[1:2, :] = jnp.full((1, VALUE_DIM), lam[z_i], f32)
    for copy in staged[5:]:
        copy.wait()
    pl.semaphore_wait(barrier, 2 * (n_sp - 1) + n_tp - 1)

    def to_all_sp(src, dst, sems):
        for k in range(1, n_sp):
            send(src, dst.at[sp_i], sems.at[0], sems.at[1], sp=(sp_i + k) % n_sp)

    def to_all_tp(ref, sems):
        for k in range(1, n_tp):
            send(ref.at[tp_i], ref.at[tp_i], sems.at[2], sems.at[3], tp=(tp_i + k) % n_tp)

    def sum_sp(ref, sems):
        arrived(ref.at[pl.ds(0, n_sp - 1)], sems.at[1])
        total = ref[0]
        for k in range(1, n_sp):
            total = total + ref[k]
        return total

    mates = [(0, 1), (1, 0), (1, 1)]
    to_all_sp(mod_part, mod_recv, mod_sem)

    def piece(s, slot, p):
        if p == pieces:
            return far_ctx.at[pl.ds(pl.multiple_of(slot * ctx_p, 16), ctx_p)]
        start = ((s * pieces + p) * 4 + slot) * rows_p
        return raw.at[pl.ds(pl.multiple_of(start, 16), rows_p)]

    def piece_pair(s, core, p):
        if p == pieces:
            return far_ctx.at[pl.ds(pl.multiple_of(core * 2 * ctx_p, 16), 2 * ctx_p)]
        start = ((s * pieces + p) * 4 + core * 2) * rows_p
        return raw.at[pl.ds(pl.multiple_of(start, 16), pair_rows)]

    def send_far(p):
        src = (
            ctx.at[pl.ds(pl.multiple_of(tp_i * ctx_p, ctx_p), ctx_p)]
            if p == pieces
            else lat.at[pl.ds(p * rows_p, rows_p)]
        )
        send(src, piece(1, slot_i, p), raw_s.at[0], z_r.at[p], sp=mirror)

    def spread_x(s, p):
        src = piece(s, slot_i, p)
        if s == 0:
            src = lat.at[pl.ds(p * rows_p, rows_p)]
        send(src, piece(s, slot_i, p), raw_s.at[0], x_r.at[s, p], tp=across)

    def spread_d(s, p):
        src = piece(s, slot_i, p)
        if s == 0:
            src = lat.at[pl.ds(p * rows_p, rows_p)]
        send(src, piece(s, slot_i, p), raw_s.at[0], d_r.at[s, p], tp=partner)

    def from_far(p):
        arrived(piece(1, slot_i, p), z_r.at[p])
        spread_x(1, p)
        spread_d(1, p)

    def from_across(s, p):
        slot = c_i * 2 + (1 - x_i)
        arrived(piece(s, slot, p), x_r.at[s, p])
        send(piece(s, slot, p), piece(s, slot, p), raw_s.at[0], d_r.at[s, p], tp=partner)

    def from_across_far(p):
        from_across(1, p)

    def from_partner(s, p):
        arrived(piece_pair(s, 1 - c_i, p), d_r.at[s, p])

    spread_x(0, 0)
    for p in range(pieces):
        spread_d(0, p)
    send(par_own, par_recv, par_sem.at[0], par_sem.at[1], tp=partner)
    for p in range(pieces):
        piece(0, slot_i, p)[...] = lat[p * rows_p : (p + 1) * rows_p, :]
    mod_recv[sp_i] = mod_part[...]

    def fill_rope(s):
        place = lax.broadcasted_iota(jnp.int32, (chunk_rows, LANES), 0)
        core = place // pair_rows
        chip = (place // rows_p) % 2
        home = sp_i if s == 0 else mirror
        for p in range(pieces):
            tok_row = home * tok + (chip * 2 + core) * own + p * rows_p + place % rows_p
            grid_row = (tok_row // GRID_W).astype(f32)
            grid_col = (tok_row % GRID_W).astype(f32)
            angles = grid_row * lane_table[0:1, :] + grid_col * lane_table[1:2, :]
            cos_t[s, p] = jnp.cos(angles)
            sin_t[s, p] = jnp.sin(angles) * lane_table[2:3, :]

    fill_rope(0)
    fill_rope(1)
    gate_total = None
    gate_cols = mod_cols // 4
    for k in range(4):
        term = jnp.dot(
            placed_rows(k, None), gate_w[:, k * gate_cols : (k + 1) * gate_cols],
            preferred_element_type=f32,
        )
        gate_total = term if gate_total is None else gate_total + term
    gate_part[...] = gate_total
    gate_recv[sp_i] = gate_total

    mod_all[tp_i] = sum_sp(mod_recv, mod_sem)
    to_all_tp(mod_all, mod_sem)
    inner = zl_i != half_i
    outer = jnp.logical_not(inner)

    def at(condition, action, *ps):
        @pl.when(condition)
        def _():
            for p in ps:
                action(p)

    at(inner, send_far, pieces, *range(pieces))
    for p in range(1, pieces):
        spread_x(0, p)
    to_all_sp(gate_part, gate_recv, gate_sem)
    from_across(0, 0)
    arrived(mod_all.at[pl.ds(0, n_tp - 1)], mod_sem.at[3])

    def modulate(x, which, start):
        at = pl.ds(start, x.shape[0])
        factor = lax.rsqrt(jnp.mean(x * x, axis=-1, keepdims=True) + norm_eps)
        for t in range(n_tp):
            for k in (0, 1):
                start = t * mod_cols + k * half_cols
                cols = slice(start, start + half_cols)
                shift = mod_all[t, 4 * k + which : 4 * k + which + 1, :]
                scale = mod_all[t, 4 * k + which + 2 : 4 * k + which + 3, :]
                hidden[at, cols] = (
                    (x[:, cols] * factor) * (1.0 + scale) + shift
                ).astype(bf16)

    lane = lax.broadcasted_iota(jnp.int32, (chunk_rows, LANES), 1)
    first_quarter = lane % HEAD_DIM < HEAD_DIM // 2
    low_half = lane < HEAD_DIM
    ctx_half = lax.broadcasted_iota(jnp.int32, (ctx_rows, LANES), 1) < HEAD_DIM

    def rope(u, s, p):
        swapped = jnp.where(
            first_quarter,
            pltpu.roll(u, LANES - HEAD_DIM // 2, 1),
            pltpu.roll(u, HEAD_DIM // 2, 1),
        )
        return u * cos_t[s, p] + swapped * sin_t[s, p]

    def pair_up(a, b, low):
        return (
            jnp.where(low, a, pltpu.roll(b, HEAD_DIM, 1)).astype(bf16),
            jnp.where(low, pltpu.roll(a, HEAD_DIM, 1), b).astype(bf16),
        )

    core_keys = keys // 2

    def kv_at(s, src, core, p):
        start = s * keys + core * core_keys + (p * 4 + src) * pair_rows
        return kv_buf.at[pl.ds(pl.multiple_of(start, 16), pair_rows)]

    def kvc_at(s, src, core):
        start = s * keys + core * core_keys + 2 * tok + src * (ctx_rows // 2)
        return kv_buf.at[pl.ds(pl.multiple_of(start, 16), ctx_rows // 2)]

    def kv_block(s, core, p):
        start = s * keys + core * core_keys + p * 4 * pair_rows
        size = 2 * ctx_rows if p == pieces else 4 * pair_rows
        return kv_buf.at[pl.ds(pl.multiple_of(start, 16), size)]

    def q_at(s, src, p):
        start = ((s * pieces + p) * 4 + src) * pair_rows
        return pl.ds(pl.multiple_of(start, 16), pair_rows)

    kv_cols = 2 * head_cols + val_cols

    def chunk(s, ps, with_ctx):
        for i, p in enumerate(ps):
            from_partner(s, p)
            start = (s * pieces + p) * chunk_rows
            modulate(raw[start : start + chunk_rows, :].astype(f32), 0, i * chunk_rows)
        lat_count = len(ps) * chunk_rows
        count = lat_count
        if with_ctx:
            if s == 1:
                from_partner(1, pieces)
                modulate(far_ctx[...].astype(f32), 1, lat_count)
            else:
                modulate(ctx[...].astype(f32), 1, lat_count)
            count = lat_count + ctx_rows
        if s == 0 and ps[0] == 0:
            arrived(w, w_sem.at[0])
        kv = jnp.dot(hidden[:count, :], w[:, :kv_cols], preferred_element_type=f32)
        slabs = [kv[:, m * LANES : (m + 1) * LANES] for m in (0, 1)]
        vals = [kv[:, (2 + j) * LANES : (3 + j) * LANES].astype(bf16) for j in (0, 1)]
        for i, p in enumerate(ps):
            at = slice(i * chunk_rows, (i + 1) * chunk_rows)
            pair = pair_up(rope(slabs[0][at], s, p), rope(slabs[1][at], s, p), low_half)
            for j in (0, 1):
                for core in (0, 1):
                    rows = slice(core * pair_rows, (core + 1) * pair_rows)
                    kv_send[s, j, core, p, :, :LANES] = pair[j][rows]
                    kv_send[s, j, core, p, :, LANES:] = vals[j][at][rows]
        if with_ctx:
            pair = pair_up(slabs[0][lat_count:], slabs[1][lat_count:], ctx_half)
            for j in (0, 1):
                kvc_send[s, j, :, :LANES] = pair[j]
                kvc_send[s, j, :, LANES:] = vals[j][lat_count:]
        for dj in (1, 0):
            j = (zl_i + dj) % 2
            for dc in (0, 1):
                core = (c_i + dc) % 2
                put = send if dj or dc else send_or_keep
                s_sem = kv_s.at[0] if dj or dc else kv_s.at[1]
                where = dict(sp=sp_at(half_i, j, c_i), tp=x_i * 2 + core)
                for p in ps:
                    put(
                        kv_send.at[s, j, core, p], kv_at(s, src_i, core, p),
                        s_sem, kv_r.at[s, p], **where,
                    )
                if with_ctx:
                    half = pl.ds(pl.multiple_of(core * (ctx_rows // 2), 16), ctx_rows // 2)
                    put(
                        kvc_send.at[s, j, half], kvc_at(s, src_i, core),
                        s_sem, kv_r.at[s, pieces], **where,
                    )
        q = jnp.dot(hidden[:lat_count, :], w[:, kv_cols:], preferred_element_type=f32)
        for i, p in enumerate(ps):
            at = slice(i * chunk_rows, (i + 1) * chunk_rows)
            pair = pair_up(rope(q[at, :LANES], s, p), rope(q[at, LANES:], s, p), low_half)
            for j in (0, 1):
                for core in (0, 1):
                    q_send[s, j, core, p] = pair[j][core * pair_rows : (core + 1) * pair_rows]
        for dj in (1, 0):
            j = (zl_i + dj) % 2
            for dc in (0, 1):
                core = (c_i + dc) % 2
                put = send if dj or dc else send_or_keep
                s_sem = q_s.at[0] if dj or dc else q_s.at[1]
                for p in ps:
                    put(
                        q_send.at[s, j, core, p], q_buf.at[q_at(s, src_i, p)],
                        s_sem, q_r.at[s, p],
                        sp=sp_at(half_i, j, c_i), tp=x_i * 2 + core,
                    )

    def relay(s, p):
        block = kv_block(s, c_i, p)
        arrived(block, kv_r.at[s, p])
        send(block, block, kv_s.at[0], rel_r.at[s], tp=partner)

    def wait_keys(s):
        start = s * keys + (1 - c_i) * core_keys
        arrived(kv_buf.at[pl.ds(pl.multiple_of(start, 16), core_keys)], rel_r.at[s])
        step = 2 * LANES
        for b in range(keys // step):
            at = s * keys + b * step
            vals_t[s, :, b * step : (b + 1) * step] = kv_buf[at : at + step, LANES:].T

    def wait_queries(s, p):
        arrived(
            q_buf.at[pl.ds((s * pieces + p) * 4 * pair_rows, 4 * pair_rows)], q_r.at[s, p]
        )

    coef = HEAD_DIM ** (-0.5) * 1.4426950408889634
    q_low = lax.broadcasted_iota(jnp.int32, (q_tile, LANES), 1) < HEAD_DIM
    cols = 2 * q_tile

    def item(tile, s, first, last):
        q = q_buf[tile * q_tile : (tile + 1) * q_tile, :]
        zero = jnp.zeros_like(q)
        q2 = jnp.concatenate([jnp.where(q_low, q, zero), jnp.where(q_low, zero, q)], axis=0)
        scores = lax.dot_general(
            kv_buf[s * keys : (s + 1) * keys, :LANES], q2, (((1,), (1,)), ((), ())),
            preferred_element_type=f32,
        )
        peak = jnp.max(scores, axis=0, keepdims=True)
        if not first:
            old = peak_s[tile]
            peak = jnp.maximum(old, peak)
        weights = jnp.exp2(scores * coef - peak * coef)
        sums = jnp.sum(weights.reshape(keys // 8, 8, cols), axis=0)
        acc = jnp.dot(vals_t[s], weights.astype(bf16), preferred_element_type=f32)
        if not first:
            fade = jnp.exp2((old - peak) * coef)
            sums = sums + sum_s[tile] * fade
            acc = acc + acc_s[tile] * fade
        if not last:
            peak_s[tile] = peak
            sum_s[tile] = sums
            acc_s[tile] = acc
            return
        mean_v = acc / jnp.sum(sums, axis=0, keepdims=True)
        mixed = mean_v[:, :q_tile] - gain_t[VALUE_DIM : VALUE_DIM + 1, :] * mean_v[:, q_tile:]
        factor = lax.rsqrt(jnp.mean(mixed * mixed, axis=0, keepdims=True) + norm_eps)
        o_send[tile * q_tile : (tile + 1) * q_tile, :] = (
            mixed * factor * gain_t[:VALUE_DIM, :]
        ).T.astype(bf16)

    def head_row(p, core, h):
        return ((p * 2 + core) * 4 + h) * pair_rows

    def give_back(s, p):
        half = half_i if s == 0 else 1 - half_i
        for dz, dy in mates + [(0, 0)]:
            zl = (zl_i + dz) % 2
            y = (y_i + dy) % 2
            put = send if s or dz or dy else send_or_keep
            put(
                o_send.at[q_at(s, zl * 2 + y, p)],
                heads.at[pl.ds(pl.multiple_of(head_row(p, c_i, z_i), 16), pair_rows)],
                o_s.at[0] if s or dz or dy else o_s.at[1], o_r.at[p],
                sp=sp_at(half, zl, y), tp=x_i * 2 + y_i,
            )

    parts = pair_send.shape[1]
    part_cols = width // parts

    def project(p):
        arrived(heads.at[pl.ds(head_row(p, 0, 0), 8 * pair_rows)], o_r.at[p])
        left = jnp.concatenate(
            [
                jnp.concatenate(
                    [
                        heads[pl.ds(pl.multiple_of(head_row(p, core, h), 16), pair_rows), :]
                        for h in range(4)
                    ],
                    axis=-1,
                )
                for core in (1 - c_i, c_i)
            ],
            axis=0,
        )
        for k in range(parts):
            if k % 2 == 0:
                at = slice(k * part_cols, (k + 2) * part_cols)
                both = jnp.dot(left, wo[:, at], preferred_element_type=f32).astype(bf16)
            terms = both[:, k % 2 * part_cols : (k % 2 + 1) * part_cols]
            pair_send[p, k] = terms[:pair_rows]
            mine[p, k] = terms[pair_rows:]
            send(
                pair_send.at[p, k], pair_recv.at[p, k], pair_s.at[0], pair_r.at[p, k],
                tp=partner,
            )

    def combine(p):
        here = pl.ds(pl.multiple_of(x_i * rows_p, rows_p), rows_p)
        there = pl.ds(pl.multiple_of((1 - x_i) * rows_p, rows_p), rows_p)
        for k in range(parts):
            arrived(pair_recv.at[p, k], pair_r.at[p, k])
            both = mine[p, k, there, :].astype(f32) + pair_recv[p, k, there, :].astype(f32)
            fin_send[p, k] = both.astype(bf16)
            send(
                fin_send.at[p, k], fin_recv.at[p, k], fin_s.at[0], fin_r.at[p, k], tp=across
            )
            own_sum[p, k] = mine[p, k, here, :].astype(f32) + pair_recv[p, k, here, :].astype(f32)

    def finish(p):
        rows = slice(p * rows_p, (p + 1) * rows_p)
        for k in range(parts):
            arrived(fin_recv.at[p, k], fin_r.at[p, k])
            summed = own_sum[p, k] + fin_recv[p, k].astype(f32)
            for col in range(0, part_cols, gate_cols):
                at = slice(k * part_cols + col, k * part_cols + col + gate_cols)
                block = (k * part_cols + col) // gate_cols
                gate = gate_all[block // 4, block % 4 : block % 4 + 1, :]
                out[rows, at] = (
                    lat[rows, at].astype(f32) + gate * summed[:, col : col + gate_cols]
                ).astype(bf16)

    last = pieces - 1
    chunk(0, [0], True)
    at(outer, send_far, pieces, 0)
    for p in range(1, pieces):
        from_across(0, p)
    at(outer, from_far, pieces, 0)
    chunk(0, list(range(1, pieces)), False)
    at(outer, send_far, *range(1, pieces))
    arrived(par_recv, par_sem.at[1])
    params = jnp.where(owns_head, par_own[...], par_recv[...])
    gain_row = jnp.broadcast_to(params[0:1, :], (VALUE_DIM, VALUE_DIM)).T
    lam_row = jnp.broadcast_to(params[1:2, :], (8, VALUE_DIM))
    for k in range(q_tile // VALUE_DIM):
        gain_t[:VALUE_DIM, k * VALUE_DIM : (k + 1) * VALUE_DIM] = gain_row
        gain_t[VALUE_DIM:, k * VALUE_DIM : (k + 1) * VALUE_DIM] = lam_row
    at(outer, from_far, 1)
    relay(0, 0)
    relay(0, pieces)
    at(inner, from_far, pieces, 0)
    for p in range(1, pieces):
        relay(0, p)
    from_across(1, pieces)
    wait_keys(0)
    for p in range(pieces):
        wait_queries(0, p)
    item(0, 0, True, False)
    at(outer, from_across_far, 0)
    item(1, 0, True, False)
    at(inner, from_across_far, 0)
    at(inner, from_far, 1)
    at(outer, from_far, *range(2, pieces))
    chunk(1, [0], True)
    at(inner, from_far, *range(2, pieces))
    from_across(1, 1)
    chunk(1, [1], False)
    for p in range(2, pieces):
        from_across(1, p)
    item(2, 0, True, False)
    for p in range(2, pieces):
        chunk(1, [p], False)
    relay(1, 0)
    relay(1, pieces)
    for p in range(1, last):
        relay(1, p)
    gate_all[tp_i] = sum_sp(gate_recv, gate_sem)
    to_all_tp(gate_all, gate_sem)
    for p in range(last):
        wait_queries(1, p)
        item(pieces + p, 0, True, False)
    relay(1, last)
    wait_queries(1, last)
    item(pieces + last, 0, True, False)
    wait_keys(1)
    arrived(wo, w_sem.at[1])
    for p in range(pieces):
        item(pieces + p, 1, False, True)
        give_back(1, p)
        if p == last:
            project(p - 1)
        item(p, 1, False, True)
        give_back(0, p)
        if p == last:
            combine(p - 1)
        elif p > 0:
            project(p - 1)
            combine(p - 1)
    project(last)
    combine(last)
    arrived(gate_all.at[pl.ds(0, n_tp - 1)], gate_sem.at[3])
    for p in range(pieces):
        finish(p)
    def sent(ref, s_sem):
        pltpu.make_async_copy(ref, ref, s_sem).wait()

    far_rows = own + ctx_p
    sent(raw.at[pl.ds(0, 3 * own + 4 * far_rows)], raw_s.at[0])
    for sems, ref, tp_ref in (
        (mod_sem, mod_recv, mod_all), (gate_sem, gate_recv, gate_all),
    ):
        sent(ref.at[pl.ds(0, n_sp - 1)], sems.at[0])
        sent(tp_ref.at[pl.ds(0, n_tp - 1)], sems.at[2])
    sent(par_own, par_sem.at[0])
    sent(kv_buf.at[pl.ds(0, 3 * set_rows + 2 * core_keys)], kv_s.at[0])
    sent(q_buf.at[pl.ds(0, 3 * tok)], q_s.at[0])
    sent(o_send.at[pl.ds(0, 7 * pieces * pair_rows)], o_s.at[0])
    sent(pair_send, pair_s.at[0])
    sent(fin_send, fin_s.at[0])

    @pl.when(jnp.logical_not(owns_head))
    def _():
        sent(kv_buf.at[pl.ds(0, set_rows)], kv_s.at[1])
        sent(q_buf.at[pl.ds(0, tok)], q_s.at[1])
        sent(o_send.at[pl.ds(0, pieces * pair_rows)], o_s.at[1])


def split_scratch(n_sp, n_tp, own, width, ctx_rows, mod_rows, mod_cols, groups):
    tok = own * n_tp
    pieces = 3
    rows_p = own // pieces
    pair_rows = 2 * rows_p
    q_tile = 4 * pair_rows
    keys = 4 * (tok + ctx_rows)
    parts = 4
    part_cols = width // parts
    dma = pltpu.SemaphoreType.DMA
    return [
        pltpu.VMEM((own, width), bf16),
        pltpu.VMEM((ctx_rows, width), bf16),
        pltpu.VMEM((n_sp, 1, mod_rows), f32),
        pltpu.VMEM((n_sp, 1, mod_rows), f32),
        pltpu.VMEM((mod_rows, mod_cols), bf16),
        pltpu.VMEM((mod_rows, mod_cols), bf16),
        pltpu.VMEM((mod_rows, mod_cols), bf16),
        pltpu.VMEM((8, LANES), f32),
        pltpu.VMEM((groups, 1, VALUE_DIM), f32),
        pltpu.VMEM((width, 4 * 2 * HEAD_DIM + 2 * VALUE_DIM), bf16),
        pltpu.VMEM((groups * VALUE_DIM, width), bf16),
        pltpu.VMEM((8, mod_cols // 2), f32),
        pltpu.VMEM((n_sp, 8, mod_cols // 2), f32),
        pltpu.VMEM((n_tp, 8, mod_cols // 2), f32),
        pltpu.VMEM((8, mod_cols // 4), f32),
        pltpu.VMEM((n_sp, 8, mod_cols // 4), f32),
        pltpu.VMEM((n_tp, 8, mod_cols // 4), f32),
        pltpu.VMEM((8, VALUE_DIM), f32),
        pltpu.VMEM((8, VALUE_DIM), f32),
        pltpu.VMEM((8 * own, width), bf16),
        pltpu.VMEM((ctx_rows, width), bf16),
        pltpu.VMEM((4 * pair_rows + ctx_rows, width), bf16),
        pltpu.VMEM((2, pieces, 2 * pair_rows, LANES), f32),
        pltpu.VMEM((2, pieces, 2 * pair_rows, LANES), f32),
        pltpu.VMEM((2, 2, 2, pieces, pair_rows, 2 * LANES), bf16),
        pltpu.VMEM((2, 2, ctx_rows, 2 * LANES), bf16),
        pltpu.VMEM((2, 2, 2, pieces, pair_rows, LANES), bf16),
        pltpu.VMEM((2 * keys, 2 * LANES), bf16),
        pltpu.VMEM((2 * pieces * q_tile, LANES), bf16),
        pltpu.VMEM((2, VALUE_DIM, keys), bf16),
        pltpu.VMEM((VALUE_DIM + 8, q_tile), f32),
        pltpu.VMEM((2 * pieces, 1, 2 * q_tile), f32),
        pltpu.VMEM((2 * pieces, 8, 2 * q_tile), f32),
        pltpu.VMEM((2 * pieces, VALUE_DIM, 2 * q_tile), f32),
        pltpu.VMEM((2 * pieces * q_tile, LANES), bf16),
        pltpu.VMEM((8 * pieces * pair_rows, LANES), bf16),
        pltpu.VMEM((pieces, parts, pair_rows, part_cols), bf16),
        pltpu.VMEM((pieces, parts, pair_rows, part_cols), bf16),
        pltpu.VMEM((pieces, parts, pair_rows, part_cols), bf16),
        pltpu.VMEM((pieces, parts, rows_p, part_cols), bf16),
        pltpu.VMEM((pieces, parts, rows_p, part_cols), bf16),
        pltpu.VMEM((pieces, parts, rows_p, part_cols), f32),
        dma((9,)),
        dma((2,)),
        dma((2,)),
        dma((4,)),
        dma((4,)),
        dma((1,)),
        dma((pieces + 1,)),
        dma((2, pieces + 1)),
        dma((2, pieces + 1)),
        dma((2,)),
        dma((2, pieces + 1)),
        dma((2,)),
        dma((2,)),
        dma((2, pieces)),
        dma((2,)),
        dma((pieces,)),
        dma((1,)),
        dma((pieces, parts)),
        dma((1,)),
        dma((pieces, parts)),
    ]


def local(
    n_sp,
    n_tp,
    latent,
    context,
    cond_latent,
    cond_context,
    shift_weight,
    scale_weight,
    gate_weight,
    query_weight,
    key_weight,
    value_weight,
    out_weight,
    lambda_heads,
    out_gain,
):
    own, width = latent.shape
    ctx_rows = context.shape[0]
    tok = own * n_tp
    groups = lambda_heads.shape[0]
    ranks = n_sp // groups
    chips = n_tp // 2
    mod_rows, mod_cols = shift_weight.shape
    keys = n_sp * (tok + ctx_rows)
    q_tile = pick(tok, 128, 16)
    pieces = 3 if own % 48 == 0 else 1
    parts = 4 if width % (4 * LANES) == 0 else 1

    quarter = HEAD_DIM // 4
    inverse = np.float32(rope_theta) ** (-np.arange(quarter, dtype=np.float32) / quarter)
    zeros = np.zeros((quarter,), np.float32)
    repeat = LANES // (2 * quarter)
    half = np.ones((2 * quarter,), np.float32)
    lane_table = np.zeros((8, LANES), np.float32)
    lane_table[0] = np.tile(np.concatenate([inverse, zeros]), repeat)
    lane_table[1] = np.tile(np.concatenate([zeros, inverse]), repeat)
    lane_table[2] = np.tile(np.concatenate([-half, half]), repeat // 2)
    gain = out_gain.reshape(groups, 1, VALUE_DIM)
    vmem = pl.BlockSpec(memory_space=pltpu.VMEM)
    hbm = pl.BlockSpec(memory_space=pl.ANY)
    dma = pltpu.SemaphoreType.DMA
    scratch = [
        pltpu.VMEM(query_weight.shape, bf16),
        pltpu.VMEM(key_weight.shape, bf16),
        pltpu.VMEM(value_weight.shape, bf16),
        pltpu.VMEM(out_weight.shape, bf16),
        pltpu.VMEM((8, mod_cols), f32),
        pltpu.VMEM((n_sp, 8, mod_cols), f32),
        pltpu.VMEM((n_tp, 8, mod_cols), f32),
        pltpu.VMEM((n_tp, own, width), bf16),
        pltpu.VMEM((2 * own + ctx_rows, width), bf16),
        pltpu.VMEM((tok, LANES), f32),
        pltpu.VMEM((tok, LANES), f32),
        pltpu.VMEM((groups, tok, LANES), bf16),
        pltpu.VMEM((groups, tok, 2 * LANES), bf16),
        pltpu.VMEM((groups, ctx_rows, 2 * LANES), bf16),
        pltpu.VMEM((groups, tok, LANES), bf16),
        pltpu.VMEM((keys, 2 * LANES), bf16),
        pltpu.VMEM((2 * q_tile, keys), f32),
        pltpu.VMEM((groups, tok, LANES), bf16),
        pltpu.VMEM((groups, tok, LANES), bf16),
        pltpu.VMEM((chips, parts, own, width // parts), bf16),
        pltpu.VMEM((chips, parts, own, width // parts), bf16),
        pltpu.VMEM((max(chips - 1, 1), parts, own, width // parts), bf16),
        pltpu.VMEM((max(chips - 1, 1), parts, own, width // parts), bf16),
        pltpu.VMEM((parts, own, width // parts), f32),
        dma((4,)),
        dma((3,)),
        dma((n_sp,)),
        dma((n_sp,)),
        dma((n_tp,)),
        dma((n_tp,)),
        dma((chips, pieces)),
        dma((chips, pieces)),
        dma((chips, pieces)),
        dma((chips, pieces)),
        dma((groups,)),
        dma((groups,)),
        dma((groups, chips)),
        dma((groups, chips)),
        dma((groups,)),
        dma((groups,)),
        dma((groups, chips, ranks)),
        dma((groups, chips, ranks)),
        dma((groups, ranks)),
        dma((groups, ranks)),
        dma((groups, tok // q_tile)),
        dma((groups, tok // q_tile)),
        dma((chips, parts)),
        dma((chips, parts)),
        dma((chips, parts)),
        dma((chips, parts)),
    ]
    kernel, staged = body, vmem
    fits = own % 48 == 0 and ctx_rows % (16 * n_tp) == 0 and own * 8 // 3 % LANES == 0
    if (n_sp, n_tp, groups) == (8, 4, 4) and fits and (tok + ctx_rows) % 64 == 0:
        kernel = split_body
        scratch = split_scratch(n_sp, n_tp, own, width, ctx_rows, mod_rows, mod_cols, groups)
        staged = hbm
    return pl.pallas_call(
        functools.partial(kernel, n_sp, n_tp),
        out_shape=jax.ShapeDtypeStruct((own, width), bf16),
        in_specs=[staged] * 8 + [pl.BlockSpec(memory_space=pltpu.SMEM), staged] + [hbm] * 4,
        out_specs=vmem,
        scratch_shapes=scratch,
        compiler_params=pltpu.CompilerParams(
            collective_id=0, has_side_effects=True, vmem_limit_bytes=60 * 1024 * 1024
        ),
        name="diff_attention",
    )(
        latent,
        context,
        cond_latent.reshape(n_sp, 1, mod_rows),
        cond_context.reshape(n_sp, 1, mod_rows),
        shift_weight,
        scale_weight,
        gate_weight,
        jnp.asarray(lane_table),
        lambda_heads,
        gain,
        query_weight,
        key_weight,
        value_weight,
        out_weight,
    )


def solution(mesh):
    placed = (
        P(("sp", "tp"), None),
        P("sp", None),
        P(),
        P(),
        P("sp", "tp"),
        P("sp", "tp"),
        P("sp", "tp"),
        P(None, None, "tp"),
        P(None, None, "tp"),
        P(None, "tp"),
        P("tp", None),
        P("tp"),
        P("tp"),
    )
    return jax.shard_map(
        functools.partial(local, mesh.shape["sp"], mesh.shape["tp"]),
        mesh=mesh,
        in_specs=placed,
        out_specs=P(("sp", "tp"), None),
        check_vma=False,
    )
```

```python
import functools

import jax
import jax.numpy as jnp
import numpy as np
from jax import lax
from jax.experimental import pallas as pl
from jax.experimental.pallas import tpu as pltpu
from jax.sharding import PartitionSpec as P

HEAD_DIM = 64
GRID_W = 64
VALUE_DIM = 128
LANES = 128

norm_eps = 1e-06
rope_theta = 10000.0
f32 = jnp.float32
bf16 = jnp.bfloat16
MESH = pl.DeviceIdType.MESH


def pick(total, limit, unit):
    best = unit
    for size in range(unit, limit + 1, unit):
        if total % size == 0:
            best = size
    return best


def body(
    n_sp,
    n_tp,
    lat,
    ctx,
    cond_l,
    cond_c,
    shift_w,
    scale_w,
    gate_w,
    lane_table,
    lam,
    gain,
    wq_hbm,
    wk_hbm,
    wv_hbm,
    wo_hbm,
    out,
    wq,
    wk,
    wv,
    wo,
    mod_part,
    mod_recv,
    mod_all,
    raw,
    hidden,
    cos_t,
    sin_t,
    q_send,
    kv_send,
    kvc_send,
    q_buf,
    kv_buf,
    scores,
    o_send,
    heads,
    pair_send,
    pair_recv,
    fin_send,
    fin_recv,
    own_sum,
    w_sem,
    loc_sem,
    mod1_s,
    mod1_r,
    mod2_s,
    mod2_r,
    raw_s,
    raw_r,
    fwd_s,
    fwd_r,
    q_s,
    q_r,
    kv_s,
    kv_r,
    kvc_s,
    kvc_r,
    rel_s,
    rel_r,
    relc_s,
    relc_r,
    o_s,
    o_r,
    pair_s,
    pair_r,
    fin_s,
    fin_r,
):
    own, width = lat.shape
    ctx_rows = ctx.shape[0]
    tok = own * n_tp
    mod_cols = shift_w.shape[1]
    groups = q_send.shape[0]
    ranks = n_sp // groups
    chips = n_tp // 2
    sp_i = lax.axis_index("sp")
    tp_i = lax.axis_index("tp")
    g_i = sp_i // ranks
    r_i = sp_i % ranks
    chip_i = tp_i // 2
    core_i = tp_i % 2
    partner = chip_i * 2 + (1 - core_i)
    pending = []

    def send(src, dst, s_sem, r_sem, **where):
        copy = pltpu.make_async_remote_copy(
            src_ref=src, dst_ref=dst, send_sem=s_sem, recv_sem=r_sem,
            device_id=where, device_id_type=MESH,
        )
        copy.start()
        pending.append(copy)

    def arrived(ref, s_sem, r_sem, **where):
        pltpu.make_async_remote_copy(
            src_ref=ref, dst_ref=ref, send_sem=s_sem, recv_sem=r_sem,
            device_id=where, device_id_type=MESH,
        ).wait_recv()

    loads = [
        pltpu.make_async_copy(src, dst, w_sem.at[i])
        for i, (src, dst) in enumerate(
            ((wk_hbm, wk), (wv_hbm, wv), (wq_hbm, wq), (wo_hbm, wo))
        )
    ]
    for load in loads:
        load.start()

    barrier = pltpu.get_barrier_semaphore()
    for k in range(1, n_sp):
        pl.semaphore_signal(
            barrier, inc=1, device_id={"sp": (sp_i + k) % n_sp}, device_id_type=MESH
        )
    for k in range(1, n_tp):
        pl.semaphore_signal(
            barrier, inc=1, device_id={"tp": (tp_i + k) % n_tp}, device_id_type=MESH
        )

    def silu(v):
        return (v / (1.0 + jnp.exp(-v))).astype(bf16).astype(f32)

    c0 = silu(cond_l[sp_i])
    c1 = silu(cond_c[sp_i])
    row = lax.broadcasted_iota(jnp.int32, (8, c0.shape[-1]), 0)

    def placed_rows(at0, at1):
        zero = jnp.zeros(row.shape, f32)
        rows = jnp.where(row == at0, jnp.broadcast_to(c0, row.shape), zero)
        if at1 is not None:
            rows = jnp.where(row == at1, jnp.broadcast_to(c1, row.shape), rows)
        return rows.astype(bf16)

    mod_part[...] = (
        jnp.dot(placed_rows(0, 1), shift_w[...], preferred_element_type=f32)
        + jnp.dot(placed_rows(2, 3), scale_w[...], preferred_element_type=f32)
        + jnp.dot(placed_rows(4, None), gate_w[...], preferred_element_type=f32)
    )
    pl.semaphore_wait(barrier, n_sp + n_tp - 2)

    for k in range(1, n_sp):
        send(
            mod_part, mod_recv.at[sp_i], mod1_s.at[k], mod1_r.at[sp_i], sp=(sp_i + k) % n_sp
        )
    pieces = raw_s.shape[1]
    piece_rows = own // pieces

    def raw_piece(slot, i):
        return raw.at[slot, pl.ds(i * piece_rows, piece_rows)]

    def send_raw(i):
        for k in range(1, chips):
            send(
                lat.at[pl.ds(i * piece_rows, piece_rows)], raw_piece(tp_i, i),
                raw_s.at[k, i], raw_r.at[chip_i, i],
                tp=((chip_i + k) % chips) * 2 + core_i,
            )

    def relay_raw(i):
        for k in range(1, chips):
            src_chip = (chip_i + chips - k) % chips
            slot = src_chip * 2 + core_i
            arrived(raw_piece(slot, i), raw_s.at[k, i], raw_r.at[src_chip, i], tp=slot)
            send(
                raw_piece(slot, i), raw_piece(slot, i), fwd_s.at[k, i], fwd_r.at[src_chip, i],
                tp=partner,
            )

    early = max(pieces - 1, 1)
    for i in range(early):
        send_raw(i)
    send(lat, raw.at[tp_i], fwd_s.at[0, 0], fwd_r.at[chip_i, 0], tp=partner)
    raw[tp_i] = lat[...]
    mod_recv[sp_i] = mod_part[...]

    tok_row = lax.broadcasted_iota(jnp.int32, (tok, LANES), 0) + sp_i * tok
    grid_row = (tok_row // GRID_W).astype(f32)
    grid_col = (tok_row % GRID_W).astype(f32)
    angles = grid_row * lane_table[0:1, :] + grid_col * lane_table[1:2, :]
    cos_t[...] = jnp.cos(angles)
    sin_t[...] = jnp.sin(angles) * lane_table[2:3, :]

    for k in range(1, n_sp):
        src = (sp_i + n_sp - k) % n_sp
        arrived(mod_recv.at[src], mod1_s.at[k], mod1_r.at[src], sp=src)
    total = mod_recv[0]
    for s in range(1, n_sp):
        total = total + mod_recv[s]
    mod_part2 = mod_all.at[tp_i]
    mod_part2[...] = total
    for k in range(1, n_tp):
        send(
            mod_part2, mod_all.at[tp_i], mod2_s.at[k], mod2_r.at[tp_i], tp=(tp_i + k) % n_tp
        )
    for i in range(early, pieces):
        send_raw(i)
    for i in range(early):
        relay_raw(i)
    for k in range(1, n_tp):
        src = (tp_i + n_tp - k) % n_tp
        arrived(mod_all.at[src], mod2_s.at[k], mod2_r.at[src], tp=src)

    def modulate(x, which, start):
        at = pl.ds(start if isinstance(start, int) else pl.multiple_of(start, 16), x.shape[0])
        factor = lax.rsqrt(jnp.mean(x * x, axis=-1, keepdims=True) + norm_eps)
        for t in range(n_tp):
            cols = slice(t * mod_cols, (t + 1) * mod_cols)
            shift = mod_all[t, which : which + 1, :]
            scale = mod_all[t, which + 2 : which + 3, :]
            hidden[at, cols] = (
                (x[:, cols] * factor) * (1.0 + scale) + shift
            ).astype(bf16)

    half = 2 * own
    lane = lax.broadcasted_iota(jnp.int32, (half, LANES), 1)
    first_quarter = lane % HEAD_DIM < HEAD_DIM // 2
    low_half = lane < HEAD_DIM
    ctx_half = lax.broadcasted_iota(jnp.int32, (ctx_rows, LANES), 1) < HEAD_DIM

    def rope(u, rows):
        swapped = jnp.where(
            first_quarter,
            pltpu.roll(u, LANES - HEAD_DIM // 2, 1),
            pltpu.roll(u, HEAD_DIM // 2, 1),
        )
        return u * cos_t[rows, :] + swapped * sin_t[rows, :]

    def pair_up(a, b, low):
        return (
            jnp.where(low, a, pltpu.roll(b, HEAD_DIM, 1)).astype(bf16),
            jnp.where(low, pltpu.roll(a, HEAD_DIM, 1), b).astype(bf16),
        )

    def lat_slot(s, chip=None):
        if chip is None:
            return kv_buf.at[pl.ds(pl.multiple_of(s * tok, 16), tok)]
        return kv_buf.at[pl.ds(pl.multiple_of(s * tok + chip * half, 16), half)]

    def ctx_slot(s):
        return kv_buf.at[pl.ds(pl.multiple_of(n_sp * tok + s * ctx_rows, 16), ctx_rows)]

    order = list(range(1, groups))
    for c in range(chips):
        chip = (chip_i + c) % chips
        rows = pl.ds(pl.multiple_of(chip * half, 16), half)
        if c == 0:
            modulate(ctx[...].astype(f32), 1, half)
            modulate(raw[tp_i].astype(f32), 0, core_i * own)
            arrived(raw.at[partner], fwd_s.at[0, 0], fwd_r.at[chip_i, 0], tp=partner)
            modulate(raw[partner].astype(f32), 0, (1 - core_i) * own)
            for i in range(early, pieces):
                relay_raw(i)
            count = half + ctx_rows
        else:
            slot = chip * 2 + core_i
            modulate(raw[slot].astype(f32), 0, core_i * own)
            slot = chip * 2 + (1 - core_i)
            for i in range(pieces):
                arrived(
                    raw_piece(slot, i), fwd_s.at[chips - c, i], fwd_r.at[chip, i], tp=partner
                )
            modulate(raw[slot].astype(f32), 0, (1 - core_i) * own)
            count = half
        if c == 0:
            loads[0].wait()
        keys = [jnp.dot(hidden[:count, :], wk[m], preferred_element_type=f32) for m in (0, 1)]
        for p in range(groups // 2):
            slab = slice(p * LANES, (p + 1) * LANES)
            a, b = pair_up(
                rope(keys[0][:half, slab], rows), rope(keys[1][:half, slab], rows), low_half
            )
            kv_send[2 * p, rows, :LANES] = a
            kv_send[2 * p + 1, rows, :LANES] = b
            if c == 0:
                a, b = pair_up(keys[0][half:, slab], keys[1][half:, slab], ctx_half)
                kvc_send[2 * p, :, :LANES] = a
                kvc_send[2 * p + 1, :, :LANES] = b
        if c == 0:
            loads[1].wait()
        vals = jnp.dot(hidden[:count, :], wv[...], preferred_element_type=f32).astype(bf16)
        for j in range(groups):
            slab = slice(j * LANES, (j + 1) * LANES)
            kv_send[j, rows, LANES:] = vals[:half, slab]
            if c == 0:
                kvc_send[j, :, LANES:] = vals[half:, slab]
        for k in order:
            g = (g_i + k) % groups
            to = g * ranks + r_i
            send(
                kv_send.at[g, rows], lat_slot(sp_i, chip), kv_s.at[k, c], kv_r.at[g_i, c], sp=to
            )
            if c == 0:
                send(kvc_send.at[g], ctx_slot(sp_i), kvc_s.at[k], kvc_r.at[g_i], sp=to)
        for e in range(1, ranks):
            to = g_i * ranks + (r_i + e) % ranks
            send(
                kv_send.at[g_i, rows], lat_slot(sp_i, chip), rel_s.at[0, c, e],
                rel_r.at[g_i, c, r_i], sp=to,
            )
            if c == 0:
                send(
                    kvc_send.at[g_i], ctx_slot(sp_i), relc_s.at[0, e], relc_r.at[g_i, r_i], sp=to
                )
        if c == 0:
            loads[2].wait()
        queries = [
            jnp.dot(hidden[:half, :], wq[m], preferred_element_type=f32) for m in (0, 1)
        ]
        for p in range(groups // 2):
            slab = slice(p * LANES, (p + 1) * LANES)
            a, b = pair_up(
                rope(queries[0][:, slab], rows), rope(queries[1][:, slab], rows), low_half
            )
            q_send[2 * p, rows, :] = a
            q_send[2 * p + 1, rows, :] = b
    for k in order:
        g = (g_i + k) % groups
        send(q_send.at[g], q_buf.at[g_i], q_s.at[k], q_r.at[g_i], sp=g * ranks + r_i)
    local = [
        pltpu.make_async_copy(kv_send.at[g_i], lat_slot(sp_i), loc_sem.at[0]),
        pltpu.make_async_copy(kvc_send.at[g_i], ctx_slot(sp_i), loc_sem.at[1]),
        pltpu.make_async_copy(q_send.at[g_i], q_buf.at[g_i], loc_sem.at[2]),
    ]
    for copy in local:
        copy.start()

    for c in range(chips):
        chip = (chip_i + c) % chips
        for k in order:
            g = (g_i + groups - k) % groups
            s = g * ranks + r_i
            arrived(lat_slot(s, chip), kv_s.at[k, c], kv_r.at[g, c], sp=s)
            for e in range(1, ranks):
                to = g_i * ranks + (r_i + e) % ranks
                send(
                    lat_slot(s, chip), lat_slot(s, chip), rel_s.at[k, c, e],
                    rel_r.at[g, c, r_i], sp=to,
                )
            if c == 0:
                arrived(ctx_slot(s), kvc_s.at[k], kvc_r.at[g], sp=s)
                for e in range(1, ranks):
                    to = g_i * ranks + (r_i + e) % ranks
                    send(
                        ctx_slot(s), ctx_slot(s), relc_s.at[k, e], relc_r.at[g, r_i], sp=to
                    )
    for copy in local:
        copy.wait()
    for e in range(1, ranks):
        r = (r_i + ranks - e) % ranks
        to = g_i * ranks + r
        for k in range(groups):
            g = (g_i + groups - k) % groups
            s = g * ranks + r
            for c in range(chips):
                chip = (chip_i + c) % chips
                arrived(lat_slot(s, chip), rel_s.at[k, c, e], rel_r.at[g, c, r], sp=to)
            arrived(ctx_slot(s), relc_s.at[k, e], relc_r.at[g, r], sp=to)

    key_total = kv_buf.shape[0]
    q_tile = scores.shape[0] // 2
    block = pick(key_total, 512, LANES)
    coef = HEAD_DIM ** (-0.5) * 1.4426950408889634
    q_low = lax.broadcasted_iota(jnp.int32, (q_tile, LANES), 1) < HEAD_DIM
    head_lam = lam[g_i]
    tiles = tok // q_tile
    head_gain = gain[g_i]

    def attend(g, start):
        q = q_buf[g, pl.ds(start, q_tile), :]
        zero = jnp.zeros_like(q)
        q2 = jnp.concatenate([jnp.where(q_low, q, zero), jnp.where(q_low, zero, q)], axis=0)
        peak = None
        for b in range(key_total // block):
            rows = slice(b * block, (b + 1) * block)
            s = lax.dot_general(
                q2, kv_buf[rows, :LANES], (((1,), (1,)), ((), ())), preferred_element_type=f32
            )
            scores[:, rows] = s
            for c in range(block // LANES):
                piece = s[:, c * LANES : (c + 1) * LANES]
                peak = piece if peak is None else jnp.maximum(peak, piece)
        top = jnp.max(peak, axis=-1, keepdims=True) * coef
        sums = None
        acc = None
        for b in range(key_total // block):
            rows = slice(b * block, (b + 1) * block)
            w = jnp.exp2(scores[:, rows] * coef - top)
            for c in range(block // LANES):
                piece = w[:, c * LANES : (c + 1) * LANES]
                sums = piece if sums is None else sums + piece
            part = jnp.dot(w.astype(bf16), kv_buf[rows, LANES:], preferred_element_type=f32)
            acc = part if acc is None else acc + part
        mean_v = acc / jnp.sum(sums, axis=-1, keepdims=True)
        mixed = mean_v[:q_tile] - head_lam * mean_v[q_tile:]
        factor = lax.rsqrt(jnp.mean(mixed * mixed, axis=-1, keepdims=True) + norm_eps)
        o_send[g, pl.ds(start, q_tile), :] = (mixed * factor * head_gain).astype(bf16)

    def o_copy(k, i):
        g = (g_i + groups - k) % groups
        rows = pl.ds(pl.multiple_of(i * q_tile, 16), q_tile)
        return pltpu.make_async_remote_copy(
            src_ref=o_send.at[g, rows], dst_ref=heads.at[g_i, rows], send_sem=o_s.at[k, i],
            recv_sem=o_r.at[g_i, i], device_id={"sp": g * ranks + r_i}, device_id_type=MESH,
        )

    @pl.loop(0, groups)
    def _(k):
        g = (g_i + groups - k) % groups

        @pl.when(k > 0)
        def _():
            arrived(q_buf.at[g], q_s.at[k], q_r.at[g], sp=g * ranks + r_i)

        @pl.loop(0, tiles)
        def _(i):
            attend(g, pl.multiple_of(i * q_tile, q_tile))

            @pl.when(k > 0)
            def _():
                o_copy(k, i).start()

    heads[g_i] = o_send[g_i]
    loads[3].wait()
    for k in order:
        src = (g_i + k) % groups
        for i in range(tiles):
            rows = pl.ds(i * q_tile, q_tile)
            arrived(heads.at[src, rows], o_s.at[k, i], o_r.at[src, i], sp=src * ranks + r_i)

    parts = pair_send.shape[1]
    part_cols = width // parts

    def head_rows(chunk):
        start = pl.multiple_of(chunk * own, 16)
        return jnp.concatenate(
            [heads[h, pl.ds(start, own), :] for h in range(groups)], axis=-1
        )

    def term(left, p):
        cols = slice(p * part_cols, (p + 1) * part_cols)
        return jnp.dot(left, wo[:, cols], preferred_element_type=f32).astype(bf16)

    def to_partner(k):
        chip = (chip_i + 1 + k) % chips
        left = head_rows(chip * 2 + (1 - core_i))
        for p in range(parts):
            pair_send[k, p] = term(left, p)
            send(
                pair_send.at[k, p], pair_recv.at[k, p], pair_s.at[k, p], pair_r.at[k, p],
                tp=partner,
            )

    def with_partner(k):
        chip = (chip_i + 1 + k) % chips
        left = head_rows(chip * 2 + core_i)
        for p in range(parts):
            mine = term(left, p).astype(f32)
            arrived(pair_recv.at[k, p], pair_s.at[k, p], pair_r.at[k, p], tp=partner)
            both = mine + pair_recv[k, p].astype(f32)
            if k < chips - 1:
                fin_send[k, p] = both.astype(bf16)
                send(
                    fin_send.at[k, p], fin_recv.at[k, p], fin_s.at[k, p], fin_r.at[k, p],
                    tp=chip * 2 + core_i,
                )
            else:
                own_sum[p] = both

    for k in range(chips - 1):
        to_partner(k)
    for k in range(chips - 1):
        with_partner(k)
    to_partner(chips - 1)
    with_partner(chips - 1)
    for p in range(parts):
        summed = own_sum[p]
        for k in range(chips - 1):
            src_chip = (chip_i + chips - 1 - k) % chips
            arrived(
                fin_recv.at[k, p], fin_s.at[k, p], fin_r.at[k, p], tp=src_chip * 2 + core_i
            )
            summed = summed + fin_recv[k, p].astype(f32)
        cols = slice(p * part_cols, (p + 1) * part_cols)
        per = mod_cols // part_cols
        if per >= 1:
            low = (p % per) * part_cols
            gate = mod_all[p // per, 4:5, low : low + part_cols]
        else:
            span = part_cols // mod_cols
            gate = jnp.concatenate(
                [mod_all[p * span + q, 4:5, :] for q in range(span)], axis=-1
            )
        out[:, cols] = (lat[:, cols].astype(f32) + gate * summed).astype(bf16)
    for copy in pending:
        copy.wait_send()
    for k in order:
        for i in range(tiles):
            o_copy(k, i).wait_send()


def split_body(
    n_sp,
    n_tp,
    lat_hbm,
    ctx_hbm,
    cond_l_hbm,
    cond_c_hbm,
    shift_hbm,
    scale_hbm,
    gate_hbm,
    lane_table_hbm,
    lam,
    gain_hbm,
    wq_hbm,
    wk_hbm,
    wv_hbm,
    wo_hbm,
    out,
    lat,
    ctx,
    cond_l,
    cond_c,
    shift_w,
    scale_w,
    gate_w,
    lane_table,
    gain,
    w,
    wo,
    mod_part,
    mod_recv,
    mod_all,
    gate_part,
    gate_recv,
    gate_all,
    par_own,
    par_recv,
    raw,
    far_ctx,
    hidden,
    cos_t,
    sin_t,
    kv_send,
    kvc_send,
    q_send,
    kv_buf,
    q_buf,
    vals_t,
    gain_t,
    peak_s,
    sum_s,
    acc_s,
    o_send,
    heads,
    mine,
    pair_send,
    pair_recv,
    fin_send,
    fin_recv,
    own_sum,
    in_sem,
    w_sem,
    par_sem,
    mod_sem,
    gate_sem,
    raw_s,
    z_r,
    x_r,
    d_r,
    kv_s,
    kv_r,
    rel_r,
    q_s,
    q_r,
    o_s,
    o_r,
    pair_s,
    pair_r,
    fin_s,
    fin_r,
):
    own, width = lat.shape
    ctx_rows = ctx.shape[0]
    tok = own * n_tp
    mod_cols = shift_w.shape[1]
    pieces = z_r.shape[0] - 1
    rows_p = own // pieces
    ctx_p = ctx_rows // n_tp
    pair_rows = 2 * rows_p
    chunk_rows = 2 * pair_rows
    set_rows = tok + ctx_rows
    keys = 4 * set_rows
    q_tile = 4 * pair_rows
    sp_i = lax.axis_index("sp")
    tp_i = lax.axis_index("tp")
    z_i = sp_i // 2
    y_i = sp_i % 2
    half_i = z_i // 2
    zl_i = z_i % 2
    src_i = zl_i * 2 + y_i
    x_i = tp_i // 2
    c_i = tp_i % 2
    slot_i = c_i * 2 + x_i
    mirror = (sp_i + 4) % n_sp
    partner = x_i * 2 + (1 - c_i)
    across = (1 - x_i) * 2 + c_i
    owns_head = c_i == y_i

    def remote(src, dst, s_sem, r_sem, **where):
        return pltpu.make_async_remote_copy(
            src_ref=src, dst_ref=dst, send_sem=s_sem, recv_sem=r_sem,
            device_id=where, device_id_type=MESH,
        )

    def send(src, dst, s_sem, r_sem, **where):
        remote(src, dst, s_sem, r_sem, **where).start()

    def send_or_keep(src, dst, s_sem, r_sem, **where):
        copy = remote(src, dst, s_sem, r_sem, **where)

        @pl.when(owns_head)
        def _():
            pltpu.make_async_copy(src, dst, r_sem).start()

        @pl.when(jnp.logical_not(owns_head))
        def _():
            copy.start()

    def arrived(ref, r_sem):
        pltpu.make_async_copy(ref, ref, r_sem).wait()

    def sp_at(half, zl, y):
        return (half * 2 + zl) * 2 + y

    staged = [
        pltpu.make_async_copy(a, b, in_sem.at[i])
        for i, (a, b) in enumerate(
            (
                (cond_l_hbm, cond_l), (cond_c_hbm, cond_c), (shift_hbm, shift_w),
                (scale_hbm, scale_w), (gain_hbm, gain), (lat_hbm, lat), (ctx_hbm, ctx),
                (gate_hbm, gate_w), (lane_table_hbm, lane_table),
            )
        )
    ]
    for copy in staged:
        copy.start()

    head_cols = 2 * HEAD_DIM
    val_cols = 2 * VALUE_DIM

    def part_cols_of(start, size):
        return pl.ds(pl.multiple_of(start, LANES), size)

    loads = []
    for m in (0, 1):
        loads.append(
            (wk_hbm.at[m, :, part_cols_of(half_i * head_cols, head_cols)],
             w.at[:, pl.ds(m * head_cols, head_cols)])
        )
    loads.append(
        (wv_hbm.at[:, part_cols_of(half_i * val_cols, val_cols)],
         w.at[:, pl.ds(2 * head_cols, val_cols)])
    )
    for m in (0, 1):
        loads.append(
            (wq_hbm.at[m, :, part_cols_of(half_i * head_cols, head_cols)],
             w.at[:, pl.ds(2 * head_cols + val_cols + m * head_cols, head_cols)])
        )
    loads = [pltpu.make_async_copy(a, b, w_sem.at[0]) for a, b in loads]
    loads.append(pltpu.make_async_copy(wo_hbm, wo, w_sem.at[1]))

    barrier = pltpu.get_barrier_semaphore()
    for k in range(1, n_sp):
        for tp in (tp_i, partner):
            pl.semaphore_signal(
                barrier, inc=1, device_id={"sp": (sp_i + k) % n_sp, "tp": tp},
                device_id_type=MESH,
            )
    for k in range(1, n_tp):
        pl.semaphore_signal(
            barrier, inc=1, device_id={"tp": (tp_i + k) % n_tp}, device_id_type=MESH
        )

    for load in loads:
        load.start()
    for copy in staged[:5]:
        copy.wait()

    def silu(v):
        return (v / (1.0 + jnp.exp(-v))).astype(bf16).astype(f32)

    c0 = silu(cond_l[sp_i])
    c1 = silu(cond_c[sp_i])
    row = lax.broadcasted_iota(jnp.int32, (8, c0.shape[-1]), 0)

    def placed_rows(at0, at1):
        zero = jnp.zeros(row.shape, f32)
        rows = jnp.where(row == at0, jnp.broadcast_to(c0, row.shape), zero)
        if at1 is not None:
            rows = jnp.where(row == at1, jnp.broadcast_to(c1, row.shape), rows)
        return rows.astype(bf16)

    half_cols = mod_cols // 2
    mod_total = None
    for k in (0, 1):
        at = slice(k * half_cols, (k + 1) * half_cols)
        for first, weight in ((4 * k, shift_w), (4 * k + 2, scale_w)):
            term = jnp.dot(
                placed_rows(first, first + 1), weight[:, at], preferred_element_type=f32
            )
            mod_total = term if mod_total is None else mod_total + term
    mod_part[...] = mod_total
    par_own[0:1, :] = gain[z_i]
    par_own[1:2, :] = jnp.full((1, VALUE_DIM), lam[z_i], f32)
    for copy in staged[5:]:
        copy.wait()
    pl.semaphore_wait(barrier, 2 * (n_sp - 1) + n_tp - 1)

    def to_all_sp(src, dst, sems):
        for k in range(1, n_sp):
            send(src, dst.at[sp_i], sems.at[0], sems.at[1], sp=(sp_i + k) % n_sp)

    def to_all_tp(ref, sems):
        for k in range(1, n_tp):
            send(ref.at[tp_i], ref.at[tp_i], sems.at[2], sems.at[3], tp=(tp_i + k) % n_tp)

    def sum_sp(ref, sems):
        arrived(ref.at[pl.ds(0, n_sp - 1)], sems.at[1])
        total = ref[0]
        for k in range(1, n_sp):
            total = total + ref[k]
        return total

    mates = [(0, 1), (1, 0), (1, 1)]
    to_all_sp(mod_part, mod_recv, mod_sem)

    def piece(s, slot, p):
        if p == pieces:
            return far_ctx.at[pl.ds(pl.multiple_of(slot * ctx_p, 16), ctx_p)]
        start = ((s * pieces + p) * 4 + slot) * rows_p
        return raw.at[pl.ds(pl.multiple_of(start, 16), rows_p)]

    def piece_pair(s, core, p):
        if p == pieces:
            return far_ctx.at[pl.ds(pl.multiple_of(core * 2 * ctx_p, 16), 2 * ctx_p)]
        start = ((s * pieces + p) * 4 + core * 2) * rows_p
        return raw.at[pl.ds(pl.multiple_of(start, 16), pair_rows)]

    def send_far(p):
        src = (
            ctx.at[pl.ds(pl.multiple_of(tp_i * ctx_p, ctx_p), ctx_p)]
            if p == pieces
            else lat.at[pl.ds(p * rows_p, rows_p)]
        )
        send(src, piece(1, slot_i, p), raw_s.at[0], z_r.at[p], sp=mirror)

    def spread_x(s, p):
        src = piece(s, slot_i, p)
        if s == 0:
            src = lat.at[pl.ds(p * rows_p, rows_p)]
        send(src, piece(s, slot_i, p), raw_s.at[0], x_r.at[s, p], tp=across)

    def spread_d(s, p):
        src = piece(s, slot_i, p)
        if s == 0:
            src = lat.at[pl.ds(p * rows_p, rows_p)]
        send(src, piece(s, slot_i, p), raw_s.at[0], d_r.at[s, p], tp=partner)

    def from_far(p):
        arrived(piece(1, slot_i, p), z_r.at[p])
        spread_x(1, p)
        spread_d(1, p)

    def from_across(s, p):
        slot = c_i * 2 + (1 - x_i)
        arrived(piece(s, slot, p), x_r.at[s, p])
        send(piece(s, slot, p), piece(s, slot, p), raw_s.at[0], d_r.at[s, p], tp=partner)

    def from_across_far(p):
        from_across(1, p)

    def from_partner(s, p):
        arrived(piece_pair(s, 1 - c_i, p), d_r.at[s, p])

    spread_x(0, 0)
    for p in range(pieces):
        spread_d(0, p)
    send(par_own, par_recv, par_sem.at[0], par_sem.at[1], tp=partner)
    for p in range(pieces):
        piece(0, slot_i, p)[...] = lat[p * rows_p : (p + 1) * rows_p, :]
    mod_recv[sp_i] = mod_part[...]

    def fill_rope(s):
        place = lax.broadcasted_iota(jnp.int32, (chunk_rows, LANES), 0)
        core = place // pair_rows
        chip = (place // rows_p) % 2
        home = sp_i if s == 0 else mirror
        for p in range(pieces):
            tok_row = home * tok + (chip * 2 + core) * own + p * rows_p + place % rows_p
            grid_row = (tok_row // GRID_W).astype(f32)
            grid_col = (tok_row % GRID_W).astype(f32)
            angles = grid_row * lane_table[0:1, :] + grid_col * lane_table[1:2, :]
            cos_t[s, p] = jnp.cos(angles)
            sin_t[s, p] = jnp.sin(angles) * lane_table[2:3, :]

    fill_rope(0)
    fill_rope(1)
    gate_total = None
    gate_cols = mod_cols // 4
    for k in range(4):
        term = jnp.dot(
            placed_rows(k, None), gate_w[:, k * gate_cols : (k + 1) * gate_cols],
            preferred_element_type=f32,
        )
        gate_total = term if gate_total is None else gate_total + term
    gate_part[...] = gate_total
    gate_recv[sp_i] = gate_total

    mod_all[tp_i] = sum_sp(mod_recv, mod_sem)
    to_all_tp(mod_all, mod_sem)
    inner = zl_i != half_i
    outer = jnp.logical_not(inner)

    def at(condition, action, *ps):
        @pl.when(condition)
        def _():
            for p in ps:
                action(p)

    at(inner, send_far, pieces, *range(pieces))
    for p in range(1, pieces):
        spread_x(0, p)
    to_all_sp(gate_part, gate_recv, gate_sem)
    from_across(0, 0)
    arrived(mod_all.at[pl.ds(0, n_tp - 1)], mod_sem.at[3])

    def modulate(x, which, start):
        at = pl.ds(start, x.shape[0])
        factor = lax.rsqrt(jnp.mean(x * x, axis=-1, keepdims=True) + norm_eps)
        for t in range(n_tp):
            for k in (0, 1):
                start = t * mod_cols + k * half_cols
                cols = slice(start, start + half_cols)
                shift = mod_all[t, 4 * k + which : 4 * k + which + 1, :]
                scale = mod_all[t, 4 * k + which + 2 : 4 * k + which + 3, :]
                hidden[at, cols] = (
                    (x[:, cols] * factor) * (1.0 + scale) + shift
                ).astype(bf16)

    lane = lax.broadcasted_iota(jnp.int32, (chunk_rows, LANES), 1)
    first_quarter = lane % HEAD_DIM < HEAD_DIM // 2
    low_half = lane < HEAD_DIM
    ctx_half = lax.broadcasted_iota(jnp.int32, (ctx_rows, LANES), 1) < HEAD_DIM

    def rope(u, s, p):
        swapped = jnp.where(
            first_quarter,
            pltpu.roll(u, LANES - HEAD_DIM // 2, 1),
            pltpu.roll(u, HEAD_DIM // 2, 1),
        )
        return u * cos_t[s, p] + swapped * sin_t[s, p]

    def pair_up(a, b, low):
        return (
            jnp.where(low, a, pltpu.roll(b, HEAD_DIM, 1)).astype(bf16),
            jnp.where(low, pltpu.roll(a, HEAD_DIM, 1), b).astype(bf16),
        )

    core_keys = keys // 2

    def kv_at(s, src, core, p):
        start = s * keys + core * core_keys + (p * 4 + src) * pair_rows
        return kv_buf.at[pl.ds(pl.multiple_of(start, 16), pair_rows)]

    def kvc_at(s, src, core):
        start = s * keys + core * core_keys + 2 * tok + src * (ctx_rows // 2)
        return kv_buf.at[pl.ds(pl.multiple_of(start, 16), ctx_rows // 2)]

    def kv_block(s, core, p):
        start = s * keys + core * core_keys + p * 4 * pair_rows
        size = 2 * ctx_rows if p == pieces else 4 * pair_rows
        return kv_buf.at[pl.ds(pl.multiple_of(start, 16), size)]

    def q_at(s, src, p):
        start = ((s * pieces + p) * 4 + src) * pair_rows
        return pl.ds(pl.multiple_of(start, 16), pair_rows)

    kv_cols = 2 * head_cols + val_cols

    def chunk(s, ps, with_ctx):
        for i, p in enumerate(ps):
            from_partner(s, p)
            start = (s * pieces + p) * chunk_rows
            modulate(raw[start : start + chunk_rows, :].astype(f32), 0, i * chunk_rows)
        lat_count = len(ps) * chunk_rows
        count = lat_count
        if with_ctx:
            if s == 1:
                from_partner(1, pieces)
                modulate(far_ctx[...].astype(f32), 1, lat_count)
            else:
                modulate(ctx[...].astype(f32), 1, lat_count)
            count = lat_count + ctx_rows
        if s == 0 and ps[0] == 0:
            arrived(w, w_sem.at[0])
        kv = jnp.dot(hidden[:count, :], w[:, :kv_cols], preferred_element_type=f32)
        slabs = [kv[:, m * LANES : (m + 1) * LANES] for m in (0, 1)]
        vals = [kv[:, (2 + j) * LANES : (3 + j) * LANES].astype(bf16) for j in (0, 1)]
        for i, p in enumerate(ps):
            at = slice(i * chunk_rows, (i + 1) * chunk_rows)
            pair = pair_up(rope(slabs[0][at], s, p), rope(slabs[1][at], s, p), low_half)
            for j in (0, 1):
                for core in (0, 1):
                    rows = slice(core * pair_rows, (core + 1) * pair_rows)
                    kv_send[s, j, core, p, :, :LANES] = pair[j][rows]
                    kv_send[s, j, core, p, :, LANES:] = vals[j][at][rows]
        if with_ctx:
            pair = pair_up(slabs[0][lat_count:], slabs[1][lat_count:], ctx_half)
            for j in (0, 1):
                kvc_send[s, j, :, :LANES] = pair[j]
                kvc_send[s, j, :, LANES:] = vals[j][lat_count:]
        for dj in (1, 0):
            j = (zl_i + dj) % 2
            for dc in (0, 1):
                core = (c_i + dc) % 2
                put = send if dj or dc else send_or_keep
                s_sem = kv_s.at[0] if dj or dc else kv_s.at[1]
                where = dict(sp=sp_at(half_i, j, c_i), tp=x_i * 2 + core)
                for p in ps:
                    put(
                        kv_send.at[s, j, core, p], kv_at(s, src_i, core, p),
                        s_sem, kv_r.at[s, p], **where,
                    )
                if with_ctx:
                    half = pl.ds(pl.multiple_of(core * (ctx_rows // 2), 16), ctx_rows // 2)
                    put(
                        kvc_send.at[s, j, half], kvc_at(s, src_i, core),
                        s_sem, kv_r.at[s, pieces], **where,
                    )
        q = jnp.dot(hidden[:lat_count, :], w[:, kv_cols:], preferred_element_type=f32)
        for i, p in enumerate(ps):
            at = slice(i * chunk_rows, (i + 1) * chunk_rows)
            pair = pair_up(rope(q[at, :LANES], s, p), rope(q[at, LANES:], s, p), low_half)
            for j in (0, 1):
                for core in (0, 1):
                    q_send[s, j, core, p] = pair[j][core * pair_rows : (core + 1) * pair_rows]
        for dj in (1, 0):
            j = (zl_i + dj) % 2
            for dc in (0, 1):
                core = (c_i + dc) % 2
                put = send if dj or dc else send_or_keep
                s_sem = q_s.at[0] if dj or dc else q_s.at[1]
                for p in ps:
                    put(
                        q_send.at[s, j, core, p], q_buf.at[q_at(s, src_i, p)],
                        s_sem, q_r.at[s, p],
                        sp=sp_at(half_i, j, c_i), tp=x_i * 2 + core,
                    )

    def relay(s, p):
        block = kv_block(s, c_i, p)
        arrived(block, kv_r.at[s, p])
        send(block, block, kv_s.at[0], rel_r.at[s], tp=partner)

    def wait_keys(s):
        start = s * keys + (1 - c_i) * core_keys
        arrived(kv_buf.at[pl.ds(pl.multiple_of(start, 16), core_keys)], rel_r.at[s])
        step = 2 * LANES
        for b in range(keys // step):
            at = s * keys + b * step
            vals_t[s, :, b * step : (b + 1) * step] = kv_buf[at : at + step, LANES:].T

    def wait_queries(s, p):
        arrived(
            q_buf.at[pl.ds((s * pieces + p) * 4 * pair_rows, 4 * pair_rows)], q_r.at[s, p]
        )

    coef = HEAD_DIM ** (-0.5) * 1.4426950408889634
    q_low = lax.broadcasted_iota(jnp.int32, (q_tile, LANES), 1) < HEAD_DIM
    cols = 2 * q_tile

    def item(tile, s, first, last):
        q = q_buf[tile * q_tile : (tile + 1) * q_tile, :]
        zero = jnp.zeros_like(q)
        q2 = jnp.concatenate([jnp.where(q_low, q, zero), jnp.where(q_low, zero, q)], axis=0)
        scores = lax.dot_general(
            kv_buf[s * keys : (s + 1) * keys, :LANES], q2, (((1,), (1,)), ((), ())),
            preferred_element_type=f32,
        )
        peak = jnp.max(scores, axis=0, keepdims=True)
        if not first:
            old = peak_s[tile]
            peak = jnp.maximum(old, peak)
        weights = jnp.exp2(scores * coef - peak * coef)
        sums = jnp.sum(weights.reshape(keys // 8, 8, cols), axis=0)
        acc = jnp.dot(vals_t[s], weights.astype(bf16), preferred_element_type=f32)
        if not first:
            fade = jnp.exp2((old - peak) * coef)
            sums = sums + sum_s[tile] * fade
            acc = acc + acc_s[tile] * fade
        if not last:
            peak_s[tile] = peak
            sum_s[tile] = sums
            acc_s[tile] = acc
            return
        mean_v = acc / jnp.sum(sums, axis=0, keepdims=True)
        mixed = mean_v[:, :q_tile] - gain_t[VALUE_DIM : VALUE_DIM + 1, :] * mean_v[:, q_tile:]
        factor = lax.rsqrt(jnp.mean(mixed * mixed, axis=0, keepdims=True) + norm_eps)
        o_send[tile * q_tile : (tile + 1) * q_tile, :] = (
            mixed * factor * gain_t[:VALUE_DIM, :]
        ).T.astype(bf16)

    def head_row(p, core, h):
        return ((p * 2 + core) * 4 + h) * pair_rows

    def give_back(s, p):
        half = half_i if s == 0 else 1 - half_i
        for dz, dy in mates + [(0, 0)]:
            zl = (zl_i + dz) % 2
            y = (y_i + dy) % 2
            put = send if s or dz or dy else send_or_keep
            put(
                o_send.at[q_at(s, zl * 2 + y, p)],
                heads.at[pl.ds(pl.multiple_of(head_row(p, c_i, z_i), 16), pair_rows)],
                o_s.at[0] if s or dz or dy else o_s.at[1], o_r.at[p],
                sp=sp_at(half, zl, y), tp=x_i * 2 + y_i,
            )

    parts = pair_send.shape[1]
    part_cols = width // parts

    def project(p):
        arrived(heads.at[pl.ds(head_row(p, 0, 0), 8 * pair_rows)], o_r.at[p])
        left = jnp.concatenate(
            [
                jnp.concatenate(
                    [
                        heads[pl.ds(pl.multiple_of(head_row(p, core, h), 16), pair_rows), :]
                        for h in range(4)
                    ],
                    axis=-1,
                )
                for core in (1 - c_i, c_i)
            ],
            axis=0,
        )
        for k in range(parts):
            if k % 2 == 0:
                at = slice(k * part_cols, (k + 2) * part_cols)
                both = jnp.dot(left, wo[:, at], preferred_element_type=f32).astype(bf16)
            terms = both[:, k % 2 * part_cols : (k % 2 + 1) * part_cols]
            pair_send[p, k] = terms[:pair_rows]
            mine[p, k] = terms[pair_rows:]
            send(
                pair_send.at[p, k], pair_recv.at[p, k], pair_s.at[0], pair_r.at[p, k],
                tp=partner,
            )

    def combine(p):
        here = pl.ds(pl.multiple_of(x_i * rows_p, rows_p), rows_p)
        there = pl.ds(pl.multiple_of((1 - x_i) * rows_p, rows_p), rows_p)
        for k in range(parts):
            arrived(pair_recv.at[p, k], pair_r.at[p, k])
            both = mine[p, k, there, :].astype(f32) + pair_recv[p, k, there, :].astype(f32)
            fin_send[p, k] = both.astype(bf16)
            send(
                fin_send.at[p, k], fin_recv.at[p, k], fin_s.at[0], fin_r.at[p, k], tp=across
            )
            own_sum[p, k] = mine[p, k, here, :].astype(f32) + pair_recv[p, k, here, :].astype(f32)

    def finish(p):
        rows = slice(p * rows_p, (p + 1) * rows_p)
        for k in range(parts):
            arrived(fin_recv.at[p, k], fin_r.at[p, k])
            summed = own_sum[p, k] + fin_recv[p, k].astype(f32)
            for col in range(0, part_cols, gate_cols):
                at = slice(k * part_cols + col, k * part_cols + col + gate_cols)
                block = (k * part_cols + col) // gate_cols
                gate = gate_all[block // 4, block % 4 : block % 4 + 1, :]
                out[rows, at] = (
                    lat[rows, at].astype(f32) + gate * summed[:, col : col + gate_cols]
                ).astype(bf16)

    last = pieces - 1
    chunk(0, [0], True)
    at(outer, send_far, pieces, 0)
    for p in range(1, pieces):
        from_across(0, p)
    at(outer, from_far, pieces, 0)
    chunk(0, list(range(1, pieces)), False)
    at(outer, send_far, *range(1, pieces))
    arrived(par_recv, par_sem.at[1])
    params = jnp.where(owns_head, par_own[...], par_recv[...])
    gain_row = jnp.broadcast_to(params[0:1, :], (VALUE_DIM, VALUE_DIM)).T
    lam_row = jnp.broadcast_to(params[1:2, :], (8, VALUE_DIM))
    for k in range(q_tile // VALUE_DIM):
        gain_t[:VALUE_DIM, k * VALUE_DIM : (k + 1) * VALUE_DIM] = gain_row
        gain_t[VALUE_DIM:, k * VALUE_DIM : (k + 1) * VALUE_DIM] = lam_row
    at(outer, from_far, 1)
    relay(0, 0)
    relay(0, pieces)
    at(inner, from_far, pieces, 0)
    for p in range(1, pieces):
        relay(0, p)
    wait_keys(0)
    for p in range(pieces):
        wait_queries(0, p)
    item(0, 0, True, False)
    from_across(1, pieces)
    at(outer, from_across_far, 0)
    item(1, 0, True, False)
    at(inner, from_across_far, 0)
    at(inner, from_far, 1)
    at(outer, from_far, *range(2, pieces))
    chunk(1, [0], True)
    at(inner, from_far, *range(2, pieces))
    from_across(1, 1)
    chunk(1, [1], False)
    for p in range(2, pieces):
        from_across(1, p)
    item(2, 0, True, False)
    for p in range(2, pieces):
        chunk(1, [p], False)
    relay(1, 0)
    relay(1, pieces)
    for p in range(1, last):
        relay(1, p)
    gate_all[tp_i] = sum_sp(gate_recv, gate_sem)
    to_all_tp(gate_all, gate_sem)
    for p in range(last):
        wait_queries(1, p)
        item(pieces + p, 0, True, False)
    relay(1, last)
    wait_queries(1, last)
    item(pieces + last, 0, True, False)
    wait_keys(1)
    arrived(wo, w_sem.at[1])
    for p in range(pieces):
        item(pieces + p, 1, False, True)
        give_back(1, p)
        if p == last:
            if p > 1:
                combine(p - 2)
            project(p - 1)
        item(p, 1, False, True)
        give_back(0, p)
        if p == last:
            combine(p - 1)
        elif p > 0:
            project(p - 1)
            if p < last - 1:
                combine(p - 1)
    project(last)
    combine(last)
    arrived(gate_all.at[pl.ds(0, n_tp - 1)], gate_sem.at[3])
    for p in range(pieces):
        finish(p)
    def sent(ref, s_sem):
        pltpu.make_async_copy(ref, ref, s_sem).wait()

    far_rows = own + ctx_p
    sent(raw.at[pl.ds(0, 3 * own + 4 * far_rows)], raw_s.at[0])
    for sems, ref, tp_ref in (
        (mod_sem, mod_recv, mod_all), (gate_sem, gate_recv, gate_all),
    ):
        sent(ref.at[pl.ds(0, n_sp - 1)], sems.at[0])
        sent(tp_ref.at[pl.ds(0, n_tp - 1)], sems.at[2])
    sent(par_own, par_sem.at[0])
    sent(kv_buf.at[pl.ds(0, 3 * set_rows + 2 * core_keys)], kv_s.at[0])
    sent(q_buf.at[pl.ds(0, 3 * tok)], q_s.at[0])
    sent(o_send.at[pl.ds(0, 7 * pieces * pair_rows)], o_s.at[0])
    sent(pair_send, pair_s.at[0])
    sent(fin_send, fin_s.at[0])

    @pl.when(jnp.logical_not(owns_head))
    def _():
        sent(kv_buf.at[pl.ds(0, set_rows)], kv_s.at[1])
        sent(q_buf.at[pl.ds(0, tok)], q_s.at[1])
        sent(o_send.at[pl.ds(0, pieces * pair_rows)], o_s.at[1])


def split_scratch(n_sp, n_tp, own, width, ctx_rows, mod_rows, mod_cols, groups):
    tok = own * n_tp
    pieces = 3
    rows_p = own // pieces
    pair_rows = 2 * rows_p
    q_tile = 4 * pair_rows
    keys = 4 * (tok + ctx_rows)
    parts = 4
    part_cols = width // parts
    dma = pltpu.SemaphoreType.DMA
    return [
        pltpu.VMEM((own, width), bf16),
        pltpu.VMEM((ctx_rows, width), bf16),
        pltpu.VMEM((n_sp, 1, mod_rows), f32),
        pltpu.VMEM((n_sp, 1, mod_rows), f32),
        pltpu.VMEM((mod_rows, mod_cols), bf16),
        pltpu.VMEM((mod_rows, mod_cols), bf16),
        pltpu.VMEM((mod_rows, mod_cols), bf16),
        pltpu.VMEM((8, LANES), f32),
        pltpu.VMEM((groups, 1, VALUE_DIM), f32),
        pltpu.VMEM((width, 4 * 2 * HEAD_DIM + 2 * VALUE_DIM), bf16),
        pltpu.VMEM((groups * VALUE_DIM, width), bf16),
        pltpu.VMEM((8, mod_cols // 2), f32),
        pltpu.VMEM((n_sp, 8, mod_cols // 2), f32),
        pltpu.VMEM((n_tp, 8, mod_cols // 2), f32),
        pltpu.VMEM((8, mod_cols // 4), f32),
        pltpu.VMEM((n_sp, 8, mod_cols // 4), f32),
        pltpu.VMEM((n_tp, 8, mod_cols // 4), f32),
        pltpu.VMEM((8, VALUE_DIM), f32),
        pltpu.VMEM((8, VALUE_DIM), f32),
        pltpu.VMEM((8 * own, width), bf16),
        pltpu.VMEM((ctx_rows, width), bf16),
        pltpu.VMEM((4 * pair_rows + ctx_rows, width), bf16),
        pltpu.VMEM((2, pieces, 2 * pair_rows, LANES), f32),
        pltpu.VMEM((2, pieces, 2 * pair_rows, LANES), f32),
        pltpu.VMEM((2, 2, 2, pieces, pair_rows, 2 * LANES), bf16),
        pltpu.VMEM((2, 2, ctx_rows, 2 * LANES), bf16),
        pltpu.VMEM((2, 2, 2, pieces, pair_rows, LANES), bf16),
        pltpu.VMEM((2 * keys, 2 * LANES), bf16),
        pltpu.VMEM((2 * pieces * q_tile, LANES), bf16),
        pltpu.VMEM((2, VALUE_DIM, keys), bf16),
        pltpu.VMEM((VALUE_DIM + 8, q_tile), f32),
        pltpu.VMEM((2 * pieces, 1, 2 * q_tile), f32),
        pltpu.VMEM((2 * pieces, 8, 2 * q_tile), f32),
        pltpu.VMEM((2 * pieces, VALUE_DIM, 2 * q_tile), f32),
        pltpu.VMEM((2 * pieces * q_tile, LANES), bf16),
        pltpu.VMEM((8 * pieces * pair_rows, LANES), bf16),
        pltpu.VMEM((pieces, parts, pair_rows, part_cols), bf16),
        pltpu.VMEM((pieces, parts, pair_rows, part_cols), bf16),
        pltpu.VMEM((pieces, parts, pair_rows, part_cols), bf16),
        pltpu.VMEM((pieces, parts, rows_p, part_cols), bf16),
        pltpu.VMEM((pieces, parts, rows_p, part_cols), bf16),
        pltpu.VMEM((pieces, parts, rows_p, part_cols), f32),
        dma((9,)),
        dma((2,)),
        dma((2,)),
        dma((4,)),
        dma((4,)),
        dma((1,)),
        dma((pieces + 1,)),
        dma((2, pieces + 1)),
        dma((2, pieces + 1)),
        dma((2,)),
        dma((2, pieces + 1)),
        dma((2,)),
        dma((2,)),
        dma((2, pieces)),
        dma((2,)),
        dma((pieces,)),
        dma((1,)),
        dma((pieces, parts)),
        dma((1,)),
        dma((pieces, parts)),
    ]


def local(
    n_sp,
    n_tp,
    latent,
    context,
    cond_latent,
    cond_context,
    shift_weight,
    scale_weight,
    gate_weight,
    query_weight,
    key_weight,
    value_weight,
    out_weight,
    lambda_heads,
    out_gain,
):
    own, width = latent.shape
    ctx_rows = context.shape[0]
    tok = own * n_tp
    groups = lambda_heads.shape[0]
    ranks = n_sp // groups
    chips = n_tp // 2
    mod_rows, mod_cols = shift_weight.shape
    keys = n_sp * (tok + ctx_rows)
    q_tile = pick(tok, 128, 16)
    pieces = 3 if own % 48 == 0 else 1
    parts = 4 if width % (4 * LANES) == 0 else 1

    quarter = HEAD_DIM // 4
    inverse = np.float32(rope_theta) ** (-np.arange(quarter, dtype=np.float32) / quarter)
    zeros = np.zeros((quarter,), np.float32)
    repeat = LANES // (2 * quarter)
    half = np.ones((2 * quarter,), np.float32)
    lane_table = np.zeros((8, LANES), np.float32)
    lane_table[0] = np.tile(np.concatenate([inverse, zeros]), repeat)
    lane_table[1] = np.tile(np.concatenate([zeros, inverse]), repeat)
    lane_table[2] = np.tile(np.concatenate([-half, half]), repeat // 2)
    gain = out_gain.reshape(groups, 1, VALUE_DIM)
    vmem = pl.BlockSpec(memory_space=pltpu.VMEM)
    hbm = pl.BlockSpec(memory_space=pl.ANY)
    dma = pltpu.SemaphoreType.DMA
    scratch = [
        pltpu.VMEM(query_weight.shape, bf16),
        pltpu.VMEM(key_weight.shape, bf16),
        pltpu.VMEM(value_weight.shape, bf16),
        pltpu.VMEM(out_weight.shape, bf16),
        pltpu.VMEM((8, mod_cols), f32),
        pltpu.VMEM((n_sp, 8, mod_cols), f32),
        pltpu.VMEM((n_tp, 8, mod_cols), f32),
        pltpu.VMEM((n_tp, own, width), bf16),
        pltpu.VMEM((2 * own + ctx_rows, width), bf16),
        pltpu.VMEM((tok, LANES), f32),
        pltpu.VMEM((tok, LANES), f32),
        pltpu.VMEM((groups, tok, LANES), bf16),
        pltpu.VMEM((groups, tok, 2 * LANES), bf16),
        pltpu.VMEM((groups, ctx_rows, 2 * LANES), bf16),
        pltpu.VMEM((groups, tok, LANES), bf16),
        pltpu.VMEM((keys, 2 * LANES), bf16),
        pltpu.VMEM((2 * q_tile, keys), f32),
        pltpu.VMEM((groups, tok, LANES), bf16),
        pltpu.VMEM((groups, tok, LANES), bf16),
        pltpu.VMEM((chips, parts, own, width // parts), bf16),
        pltpu.VMEM((chips, parts, own, width // parts), bf16),
        pltpu.VMEM((max(chips - 1, 1), parts, own, width // parts), bf16),
        pltpu.VMEM((max(chips - 1, 1), parts, own, width // parts), bf16),
        pltpu.VMEM((parts, own, width // parts), f32),
        dma((4,)),
        dma((3,)),
        dma((n_sp,)),
        dma((n_sp,)),
        dma((n_tp,)),
        dma((n_tp,)),
        dma((chips, pieces)),
        dma((chips, pieces)),
        dma((chips, pieces)),
        dma((chips, pieces)),
        dma((groups,)),
        dma((groups,)),
        dma((groups, chips)),
        dma((groups, chips)),
        dma((groups,)),
        dma((groups,)),
        dma((groups, chips, ranks)),
        dma((groups, chips, ranks)),
        dma((groups, ranks)),
        dma((groups, ranks)),
        dma((groups, tok // q_tile)),
        dma((groups, tok // q_tile)),
        dma((chips, parts)),
        dma((chips, parts)),
        dma((chips, parts)),
        dma((chips, parts)),
    ]
    kernel, staged = body, vmem
    fits = own % 48 == 0 and ctx_rows % (16 * n_tp) == 0 and own * 8 // 3 % LANES == 0
    if (n_sp, n_tp, groups) == (8, 4, 4) and fits and (tok + ctx_rows) % 64 == 0:
        kernel = split_body
        scratch = split_scratch(n_sp, n_tp, own, width, ctx_rows, mod_rows, mod_cols, groups)
        staged = hbm
    return pl.pallas_call(
        functools.partial(kernel, n_sp, n_tp),
        out_shape=jax.ShapeDtypeStruct((own, width), bf16),
        in_specs=[staged] * 8 + [pl.BlockSpec(memory_space=pltpu.SMEM), staged] + [hbm] * 4,
        out_specs=vmem,
        scratch_shapes=scratch,
        compiler_params=pltpu.CompilerParams(
            collective_id=0, has_side_effects=True, vmem_limit_bytes=60 * 1024 * 1024
        ),
        name="diff_attention",
    )(
        latent,
        context,
        cond_latent.reshape(n_sp, 1, mod_rows),
        cond_context.reshape(n_sp, 1, mod_rows),
        shift_weight,
        scale_weight,
        gate_weight,
        jnp.asarray(lane_table),
        lambda_heads,
        gain,
        query_weight,
        key_weight,
        value_weight,
        out_weight,
    )


def solution(mesh):
    placed = (
        P(("sp", "tp"), None),
        P("sp", None),
        P(),
        P(),
        P("sp", "tp"),
        P("sp", "tp"),
        P("sp", "tp"),
        P(None, None, "tp"),
        P(None, None, "tp"),
        P(None, "tp"),
        P("tp", None),
        P("tp"),
        P("tp"),
    )
    return jax.shard_map(
        functools.partial(local, mesh.shape["sp"], mesh.shape["tp"]),
        mesh=mesh,
        in_specs=placed,
        out_specs=P(("sp", "tp"), None),
        check_vma=False,
    )
```
